128 devices in a mesh: ra: 16 (over z, y), cb: 8 (over x, core).
Axes of the slice: x: 4, y: 4, z: 4, core: 2. Of those that a mesh axis runs over, the one named last changes fastest.
Arguments:
- tokens: bfloat16 [1024, 4096], P(None, 'ra'), may hold values from -40 to 40
- norm_gain: float32 [4096], P('ra'), may hold values from 0.1 to 1.9
- gate_weight: bfloat16 [4096, 11264], P('ra', 'cb'), may hold values from -0.09375 to 0.09375
- up_weight: bfloat16 [4096, 11264], P('ra', 'cb'), may hold values from -0.09375 to 0.09375
- down_weight: bfloat16 [11264, 4096], P('cb', 'ra'), may hold values from -0.0546875 to 0.0546875
- out_gain: float32 [4096], P('ra'), may hold values from 0.1 to 1.9
Outputs:
- normed: bfloat16 [1024, 4096], P(None, 'ra')
The draws below stay inside these ranges and needn't reach their ends.
All inputs are finite; a program needn't handle non-finite values.
Results may differ from the reference program's by a relative error of at most 0.0076.
Values may be sent and summed in bfloat16 or wider, within the bound.
A program may use at most 128 MiB of HBM per device.

```python
import jax
import jax.numpy as jnp
from jax import lax

D = 4096
FF = 11264
TOKENS = 1024


def draw_tokens(key, part):
    keys = jax.random.split(key, 4)
    base = jax.random.normal(keys[0], (TOKENS, D), jnp.float32)
    blocks = jnp.exp(jax.random.uniform(keys[1], (16,), jnp.float32, jnp.log(0.3), jnp.log(3.0)))
    columns = jnp.repeat(blocks, D // 16)[None, :]
    rows = jax.random.uniform(keys[2], (TOKENS, 1), jnp.float32, 0.5, 2.0)
    return jnp.clip(base * columns * rows, -40.0, 40.0).astype(jnp.bfloat16)


def block_scale(key, dims, cuts, smallest, high):
    factor_of = 1.0
    for dim, blocks in cuts:
        heights = jax.random.uniform(jax.random.fold_in(jax.random.fold_in(key, 6), dim), (blocks,), jnp.float32, smallest / len(cuts), high / len(cuts))
        factor_of = factor_of * jnp.repeat(jnp.exp(heights), dims[dim] // blocks).reshape((-1,) + (1,) * (len(dims) - 1 - dim))
    return factor_of


def gaussian(rng, dims, deviation, bound, cuts=(), kind=jnp.bfloat16):
    entries = deviation * jax.random.normal(rng, dims, jnp.float32)
    if cuts:
        entries = entries * block_scale(rng, dims, cuts, -0.22, 0.18)
    return jnp.clip(entries, -bound, bound).astype(kind)


def setup_inputs(seed: int = 0) -> dict:
    key_list = jax.random.split(jax.random.key(seed), 7)
    return {
        "tokens": draw_tokens(jax.random.fold_in(key_list[6], 71), 0),
        "norm_gain": jnp.clip(1.0 + 0.18 * jax.random.normal(key_list[1], (D,), jnp.float32), 0.1, 1.9),
        "gate_weight": gaussian(key_list[2], (D, FF), D ** -0.5, 0.09375, ((0, 16), (1, 8))),
        "up_weight": gaussian(key_list[3], (D, FF), D ** -0.5, 0.09375, ((0, 16), (1, 8))),
        "down_weight": gaussian(key_list[4], (FF, D), FF ** -0.5, 0.0546875, ((0, 8), (1, 16))),
        "out_gain": jnp.clip(1.0 + 0.18 * jax.random.normal(key_list[5], (D,), jnp.float32), 0.1, 1.9),
    }


def reference(tokens, norm_gain, gate_weight, up_weight, down_weight, out_gain):
    stream_in = tokens.astype(jnp.float32)
    inv_rms = jax.lax.rsqrt(lax.optimization_barrier(jnp.sum(stream_in * stream_in, axis=1)) / D + 1e-06)[:, None]
    scaled = (stream_in * norm_gain[None, :]).astype(jnp.bfloat16)
    gate = jnp.dot(scaled, gate_weight, preferred_element_type=jnp.float32) * inv_rms
    up = jnp.dot(scaled, up_weight, preferred_element_type=jnp.float32) * inv_rms
    hidden = (jax.nn.silu(gate) * up).astype(jnp.bfloat16)
    branch = jnp.dot(hidden, down_weight, preferred_element_type=jnp.float32)
    stream = 0.5 * stream_in + branch
    factor = jax.lax.rsqrt(lax.optimization_barrier(jnp.sum(stream * stream, axis=1)) / D + 1e-06)[:, None]
    return (stream * factor * out_gain[None, :]).astype(jnp.bfloat16)
```

```python
import functools

import jax
import jax.numpy as jnp
from jax import lax
from jax.experimental import pallas as pl
from jax.experimental.pallas import tpu as pltpu
from jax.sharding import PartitionSpec as P

D = 4096
EPS = 1e-06
MESH = pl.DeviceIdType.MESH
F32 = jnp.float32
BF16 = jnp.bfloat16
T = 1024
H = 512
B = 128
W = 256
L = 128
K = 3

RA = [(dz, dy) for dz in range(4) for dy in range(4) if (dz, dy) != (0, 0)]
PLANE = [(dx, dy) for dx in range(4) for dy in range(4) if (dx, dy) != (0, 0)]


def far_first(pairs):
    return sorted(pairs, key=lambda p: -(min(p[0], 4 - p[0]) + min(p[1], 4 - p[1])))


def mod4(v):
    return lax.rem(v + 4, 4)


def row_sums(v):
    sq = v * v
    hi = sq.astype(BF16)
    lo = (sq - hi.astype(F32)).astype(BF16)
    ones = jnp.ones((8, v.shape[1]), BF16)
    dims = (((1,), (1,)), ((), ()))
    out = lax.dot_general(ones, hi, dims, preferred_element_type=F32)
    return out + lax.dot_general(ones, lo, dims, preferred_element_type=F32)


def as_columns(row):
    return jnp.transpose(jnp.broadcast_to(row[:1], (L, L)), (1, 0))


def kernel(
    tok, gain, wg, wu, wd, ogain, out,
    xg, wb, wdb, part, rbuf, hall, psend, precv, sq_s, sq_r, st_s, st_r,
    loc, x_ss, x_rs, w_ss, w_rs, f_ss, f_rs, d_ss, d_rs, df_ss, df_rs,
    r_ss, r_rs, h_ss, h_rs, p_ss, p_rs, q_ss, q_rs, t_ss, t_rs, o_ss, o_rs, of_ss, of_rs,
):
    ra, cb = lax.axis_index("ra"), lax.axis_index("cb")
    z, y, x, c = ra // 4, lax.rem(ra, 4), cb // 2, lax.rem(cb, 2)

    def dev(dz=0, dy=0, dx=0, dc=0):
        return (mod4(z + dz) * 4 + mod4(y + dy), mod4(x + dx) * 2 + lax.rem(c + dc, 2))

    sends = []

    def send(src, dst, ss, rs, to):
        cp = pltpu.make_async_remote_copy(
            src_ref=src, dst_ref=dst, send_sem=ss, recv_sem=rs, device_id=to, device_id_type=MESH
        )
        cp.start()
        sends.append(cp)
        return cp

    def local(src, dst, sem):
        cp = pltpu.make_async_copy(src, dst, sem)
        cp.start()
        return cp

    partners = [dev(dz, dy) for dz, dy in RA] + [dev(0, dy, dx) for dx, dy in PLANE if dx] + [dev(dc=1)]
    bar = pltpu.get_barrier_semaphore()
    for p in partners:
        pl.semaphore_signal(bar, inc=1, device_id=p, device_id_type=MESH)

    def tile0(yy):
        return jnp.minimum(3 * yy, 8)

    def cols(yy, k):
        return pl.ds(pl.multiple_of((tile0(yy) + k) * L, L), L)

    mine = pl.ds(pl.multiple_of(c * H, H), H)
    locals_w = []
    for k in range(K):
        locals_w.append(local(wg.at[:, cols(y, k)], wb.at[k, c, 0, :, :L], loc.at[2 * k]))
        locals_w.append(local(wu.at[:, cols(y, k)], wb.at[k, c, 0, :, L:], loc.at[2 * k + 1]))
    local_d = local(wd.at[pl.ds(tile0(y), K)], wdb.at[y, :, c], loc.at[2 * K])

    t32 = tok[mine, :].astype(F32)
    xg[0] = (t32 * gain[...]).astype(BF16)
    sq = row_sums(t32)
    for b in range(4):
        sq_s[b] = sq[:, b * L : (b + 1) * L]

    pl.semaphore_wait(bar, len(partners))

    near = (2, 1, 3)
    xs = {d: send(xg.at[0], xg.at[d], x_ss.at[d], x_rs.at[d], dev(dy=d)) for d in near}
    ws = {}
    for k in range(K):
        for d in near:
            yy = mod4(y + d)
            ws[k, d, 0] = send(wg.at[:, cols(yy, k)], wb.at[k, c, d, :, :L], w_ss.at[k, d, 0], w_rs.at[k, d, 0], dev(dy=d))
            ws[k, d, 1] = send(wu.at[:, cols(yy, k)], wb.at[k, c, d, :, L:], w_ss.at[k, d, 1], w_rs.at[k, d, 1], dev(dy=d))
        if k == 0:
            qs = [
                send(sq_s.at[mod4(z + dz)], sq_r.at[i], q_ss.at[i], q_rs.at[i], dev(dz, dy))
                for i, (dz, dy) in enumerate(RA)
            ]
    ds_ = {
        d: send(wd.at[pl.ds(tile0(mod4(y + d)), K)], wdb.at[y, :, c], d_ss.at[d], d_rs.at[d], dev(dy=d))
        for d in near
    }

    inv = None
    hs = {}
    rs = {}

    def hidden_of(k):
        for d in near:
            rs[k, d].wait_recv()
        own = part[k, pl.ds(pl.multiple_of(z * B, B), B), :].astype(F32)
        total = own
        for d in range(3):
            total = total + rbuf[k, d].astype(F32)
        for cc in range(2):
            gate = total[:, 2 * cc * L : (2 * cc + 1) * L] * inv
            up = total[:, (2 * cc + 1) * L : (2 * cc + 2) * L] * inv
            hid = gate / (1.0 + jnp.exp(-gate)) * up
            if k == 0:
                hid = jnp.where(y == 3, jnp.zeros_like(hid), hid)
            hall[pl.ds(pl.multiple_of(z * B, B), B), (2 * k + cc) * L : (2 * k + cc + 1) * L] = hid.astype(BF16)
        block = hall.at[pl.ds(pl.multiple_of(z * B, B), B), 2 * k * L : (2 * k + 2) * L]
        for d in near:
            hs[k, d] = send(block, block, h_ss.at[k, d], h_rs.at[k, d], dev(dz=d))

    for d in near:
        xs[d].wait_recv()
    for k in range(K):
        fs = []
        for d in (0,) + near:
            if d == 0:
                locals_w[2 * k].wait()
                locals_w[2 * k + 1].wait()
            else:
                ws[k, d, 0].wait_recv()
                ws[k, d, 1].wait_recv()
            fs.append(send(wb.at[k, c, d], wb.at[k, c, d], f_ss.at[k, d], f_rs.at[k, d], dev(dc=1)))
        for turn in range(2):
            cc = lax.rem(c + turn, 2)
            if turn == 1:
                for f in fs:
                    f.wait_recv()
            acc = jnp.zeros((H, 2 * L), F32)
            for d in range(4):
                acc = acc + jnp.dot(xg[d], wb[k, cc, d], preferred_element_type=F32)
            lanes = pl.ds(pl.multiple_of(cc * 2 * L, 2 * L), 2 * L)
            part[k, :, lanes] = acc.astype(BF16)
        for d in near:
            zz = pl.ds(pl.multiple_of(mod4(z + d) * B, B), B)
            rs[k, d] = send(part.at[k, zz, :], rbuf.at[k, d - 1], r_ss.at[k, d], r_rs.at[k, d], dev(dz=d))
        if k == 0:
            total = sq_s[z]
            for i, q in enumerate(qs):
                q.wait_recv()
                total = total + sq_r[i]
            inv = as_columns(lax.rsqrt(total / D + EPS))
        else:
            hidden_of(k - 1)

    dfs = []
    for d in (0,) + near:
        if d == 0:
            local_d.wait()
        else:
            ds_[d].wait_recv()
        block = wdb.at[mod4(y - d), :, c]
        dfs.append(send(block, block, df_ss.at[d], df_rs.at[d], dev(dc=1)))
    hidden_of(K - 1)
    for f in dfs:
        f.wait_recv()
    for k in range(K):
        for d in near:
            hs[k, d].wait_recv()

    ps = {}
    for dy in (2, 1, 3, 0):
        yy = mod4(y + dy)
        acc = jnp.dot(hall[...], wdb[yy].reshape(2 * K * L, W), preferred_element_type=F32)
        psend[yy] = acc.astype(BF16)
        for i, (dx, dyy) in enumerate(PLANE):
            if dyy == dy:
                xx = pl.ds(pl.multiple_of(mod4(x + dx) * B, B), B)
                ps[i] = send(psend.at[yy, xx, :], precv.at[i], p_ss.at[i], p_rs.at[i], dev(dy=dy, dx=dx))
    piece = pl.ds(pl.multiple_of(c * H + x * B, B), B)
    stream = 0.5 * tok[piece, :].astype(F32) + psend[y, pl.ds(pl.multiple_of(x * B, B), B), :].astype(F32)
    for i in range(len(PLANE)):
        ps[i].wait_recv()
        stream = stream + precv[i].astype(F32)
    st_s[...] = row_sums(stream)
    ts = [
        send(st_s, st_r.at[i], t_ss.at[i], t_rs.at[i], dev(dz, dy)) for i, (dz, dy) in enumerate(RA)
    ]
    total = st_s[...]
    for i, t in enumerate(ts):
        t.wait_recv()
        total = total + st_r[i]
    factor = as_columns(lax.rsqrt(total / D + EPS))
    for h in range(2):
        lanes = slice(h * L, (h + 1) * L)
        out[piece, lanes] = (stream[:, lanes] * factor * ogain[:, lanes]).astype(BF16)

    os_ = {d: send(out.at[piece, :], out.at[piece, :], o_ss.at[d], o_rs.at[d], dev(dx=d)) for d in near}
    ofs = []
    for d in (0,) + near:
        if d:
            os_[d].wait_recv()
        rows = pl.ds(pl.multiple_of(c * H + mod4(x - d) * B, B), B)
        ofs.append(send(out.at[rows, :], out.at[rows, :], of_ss.at[d], of_rs.at[d], dev(dc=1)))
    for f in ofs:
        f.wait_recv()
    for s in sends:
        s.wait_send()


def body(tokens, norm_gain, gate_weight, up_weight, down_weight, out_gain):
    dma = pltpu.SemaphoreType.DMA
    vmem = pl.BlockSpec(memory_space=pltpu.VMEM)
    hbm = pl.BlockSpec(memory_space=pl.ANY)
    n = len(RA)
    return pl.pallas_call(
        kernel,
        out_shape=jax.ShapeDtypeStruct((T, W), BF16),
        in_specs=[vmem, vmem, hbm, hbm, hbm, vmem],
        out_specs=vmem,
        scratch_shapes=[
            pltpu.VMEM((4, H, W), BF16),
            pltpu.VMEM((K, 2, 4, W, 2 * L), BF16),
            pltpu.VMEM((4, K, 2, L, W), BF16),
            pltpu.VMEM((K, H, 4 * L), BF16),
            pltpu.VMEM((K, 3, B, 4 * L), BF16),
            pltpu.VMEM((H, 2 * K * L), BF16),
            pltpu.VMEM((4, H, W), BF16),
            pltpu.VMEM((n, B, W), BF16),
            pltpu.VMEM((4, 8, L), F32),
            pltpu.VMEM((n, 8, L), F32),
            pltpu.VMEM((8, L), F32),
            pltpu.VMEM((n, 8, L), F32),
            dma((2 * K + 1,)),
            dma((4,)), dma((4,)),
            dma((K, 4, 2)), dma((K, 4, 2)),
            dma((K, 4)), dma((K, 4)),
            dma((4,)), dma((4,)),
            dma((4,)), dma((4,)),
            dma((K, 4)), dma((K, 4)),
            dma((K, 4)), dma((K, 4)),
            dma((n,)), dma((n,)),
            dma((n,)), dma((n,)),
            dma((n,)), dma((n,)),
            dma((4,)), dma((4,)),
            dma((4,)), dma((4,)),
        ],
        compiler_params=pltpu.CompilerParams(
            collective_id=0, has_side_effects=True, vmem_limit_bytes=40 * 1024 * 1024
        ),
    )(
        tokens,
        norm_gain.reshape(1, W),
        gate_weight,
        up_weight,
        down_weight.reshape(11, L, W),
        out_gain.reshape(1, W),
    )


def solution(mesh):
    placed = (P(None, "ra"), P("ra"), P("ra", "cb"), P("ra", "cb"), P("cb", "ra"), P("ra"))
    return jax.shard_map(body, mesh=mesh, in_specs=placed, out_specs=P(None, "ra"), check_vma=False)
```

```python
import functools

import jax
import jax.numpy as jnp
from jax import lax
from jax.experimental import pallas as pl
from jax.experimental.pallas import tpu as pltpu
from jax.sharding import PartitionSpec as P

D = 4096
EPS = 1e-06
MESH = pl.DeviceIdType.MESH
scope = jax.named_scope
F32 = jnp.float32
BF16 = jnp.bfloat16
T = 1024
H = 512
B = 128
W = 256
L = 128
K = 3

R = 96

NEAR = (2, 1, 3)
ROW = [(d, e) for d in (2, 1, 3) for e in range(2)] + [(0, 1)]


def mod4(v):
    return lax.rem(v + 4, 4)


def row_sums(v):
    sq = v * v
    hi = sq.astype(BF16)
    lo = (sq - hi.astype(F32)).astype(BF16)
    ones = jnp.ones((8, v.shape[1]), BF16)
    dims = (((1,), (1,)), ((), ()))
    out = lax.dot_general(ones, hi, dims, preferred_element_type=F32)
    return out + lax.dot_general(ones, lo, dims, preferred_element_type=F32)


def as_columns(row):
    return jnp.transpose(jnp.broadcast_to(row[:1], (L, L)), (1, 0))


def kernel(
    tok_h, gain_h, wg_h, wu_h, wd_h, ogain_h, out,
    tok, gain, wg, wu, wd, ogain, xg, wb, wdb, part, rbuf, hall, psend, p1, p2, s1, s2, p3, p4,
    sq_s, sq_r, sq2_r, st_s, st_r, st2_s, st2_r, st3_r,
    head, loc, xa_ss, xa_rs, xb_ss, xb_rs, xc_ss, xc_rs, w_ss, w_rs, f_ss, f_rs, d_ss, d_rs, df_ss, df_rs,
    r_ss, r_rs, h_ss, h_rs, p1_ss, p1_rs, p2_ss, p2_rs, p3_ss, p3_rs, p4_ss, p4_rs,
    q_ss, q_rs, q2_ss, q2_rs, t_ss, t_rs, t2_ss, t2_rs, t3_ss, t3_rs, o_ss, o_rs, of_ss, of_rs,
):
    ra, cb = lax.axis_index("ra"), lax.axis_index("cb")
    z, y, x, c = ra // 4, lax.rem(ra, 4), cb // 2, lax.rem(cb, 2)

    def dev(dz=0, dy=0, dx=0, dc=0):
        return (mod4(z + dz) * 4 + mod4(y + dy), mod4(x + dx) * 2 + lax.rem(c + dc, 2))

    sends = []

    def send(src, dst, ss, rs, to):
        cp = pltpu.make_async_remote_copy(
            src_ref=src, dst_ref=dst, send_sem=ss, recv_sem=rs, device_id=to, device_id_type=MESH
        )
        cp.start()
        sends.append(cp)
        return cp

    def local(src, dst, sem):
        cp = pltpu.make_async_copy(src, dst, sem)
        cp.start()
        return cp

    partners = [dev(dy=d) for d in NEAR] + [dev(dz=d) for d in NEAR] + [dev(dx=d, dc=e) for d, e in ROW]
    bar = pltpu.get_barrier_semaphore()
    for p in partners:
        pl.semaphore_signal(bar, inc=1, device_id=p, device_id_type=MESH)

    heads = [
        local(src, dst, head.at[i])
        for i, (src, dst) in enumerate(
            ((tok_h, tok), (gain_h, gain), (wg_h, wg), (wu_h, wu), (wd_h, wd), (ogain_h, ogain))
        )
    ]

    def tile0(yy):
        return jnp.minimum(3 * yy, 8)

    def cols(yy, k):
        return pl.ds(pl.multiple_of((tile0(yy) + k) * L, L), L)

    def rows(start, size):
        return pl.ds(pl.multiple_of(start, 16), size)

    locals_w = []
    for k in range(K):
        locals_w.append(local(wg_h.at[:, cols(y, k)], wb.at[k, c, 0, :, :L], loc.at[2 * k]))
        locals_w.append(local(wu_h.at[:, cols(y, k)], wb.at[k, c, 0, :, L:], loc.at[2 * k + 1]))
    local_d = local(wd_h.at[pl.ds(tile0(y), K)], wdb.at[y, :, c], loc.at[2 * K])

    heads[0].wait()
    heads[1].wait()
    t32 = tok[rows(c * H, H), :].astype(F32)
    xg[0] = (t32 * gain[...]).astype(BF16)
    sq = row_sums(t32)
    for b in range(4):
        sq_s[b] = sq[:, b * L : (b + 1) * L]
    for h in heads[2:]:
        h.wait()
    with scope("barrier"):
        pl.semaphore_wait(bar, len(partners))

    quarter = rows(x * R, R)
    rest = slice(4 * R, H)
    xa = {d: send(xg.at[0, quarter], xg.at[d, quarter], xa_ss.at[d], xa_rs.at[d], dev(dy=d)) for d in NEAR}
    xb = {d: send(xg.at[0, rest], xg.at[d, rest], xb_ss.at[d], xb_rs.at[d], dev(dy=d)) for d in NEAR}
    qs = {d: send(sq_s, sq_r.at[d - 1], q_ss.at[d], q_rs.at[d], dev(dy=d)) for d in NEAR}
    ws = {}
    for k in range(K):
        for d in NEAR:
            yy = mod4(y + d)
            ws[k, d, 0] = send(wg.at[:, cols(yy, k)], wb.at[k, c, d, :, :L], w_ss.at[k, d, 0], w_rs.at[k, d, 0], dev(dy=d))
            ws[k, d, 1] = send(wu.at[:, cols(yy, k)], wb.at[k, c, d, :, L:], w_ss.at[k, d, 1], w_rs.at[k, d, 1], dev(dy=d))
    ds_ = {
        d: send(wd.at[pl.ds(tile0(mod4(y + d)), K)], wdb.at[y, :, c], d_ss.at[d], d_rs.at[d], dev(dy=d))
        for d in NEAR
    }
    xc = {}
    for d in (1, 3, 2):
        with scope(f"wait_xa#d={d}"):
            xa[d].wait_recv()
        for e in NEAR:
            xc[d, e] = send(xg.at[d, quarter], xg.at[d, quarter], xc_ss.at[d, e], xc_rs.at[d, e], dev(dx=e))
    with scope("wait_xb"):
        for d in NEAR:
            xb[d].wait_recv()
    with scope("wait_sq"):
        for d in NEAR:
            qs[d].wait_recv()
    for b in range(4):
        sq_s2 = sq_s[b] + sq_r[0, b] + sq_r[1, b] + sq_r[2, b]
        st2_s[b] = sq_s2
    q2 = {d: send(st2_s.at[mod4(z + d)], sq2_r.at[d - 1], q2_ss.at[d], q2_rs.at[d], dev(dz=d)) for d in NEAR}

    inv = None
    hs = {}
    rs = {}
    fs = {}
    own_rows = rows(z * B, B)

    def columns_of(k):
        with scope(f"wait_w#k={k}"):
            for d in (0,) + NEAR:
                if d == 0:
                    locals_w[2 * k].wait()
                    locals_w[2 * k + 1].wait()
                else:
                    ws[k, d, 0].wait_recv()
                    ws[k, d, 1].wait_recv()
                fs[k, d] = send(wb.at[k, c, d], wb.at[k, c, d], f_ss.at[k, d], f_rs.at[k, d], dev(dc=1))

    def hidden_of(k):
        with scope(f"wait_rs#k={k}"):
            for d in NEAR:
                rs[k, d].wait_recv()
        total = part[k, own_rows, :].astype(F32)
        for d in range(3):
            total = total + rbuf[k, d].astype(F32)
        for cc in range(2):
            gate = total[:, 2 * cc * L : (2 * cc + 1) * L] * inv
            up = total[:, (2 * cc + 1) * L : (2 * cc + 2) * L] * inv
            hid = gate / (1.0 + jnp.exp(-gate)) * up
            if k == 0:
                hid = jnp.where(y == 3, jnp.zeros_like(hid), hid)
            hall[own_rows, (2 * k + cc) * L : (2 * k + cc + 1) * L] = hid.astype(BF16)
        block = hall.at[own_rows, 2 * k * L : (2 * k + 2) * L]
        for d in NEAR:
            hs[k, d] = send(block, block, h_ss.at[k, d], h_rs.at[k, d], dev(dz=d))

    columns_of(0)
    with scope("wait_xc"):
        for d in NEAR:
            for e in NEAR:
                xc[d, e].wait_recv()
    for k in range(K):
        if k:
            columns_of(k)
        for turn in range(2):
            cc = lax.rem(c + turn, 2)
            if turn == 1:
                with scope(f"wait_f#k={k}"):
                    for d in (0,) + NEAR:
                        fs[k, d].wait_recv()
            acc = jnp.zeros((H, 2 * L), F32)
            for d in range(4):
                acc = acc + jnp.dot(xg[d], wb[k, cc, d], preferred_element_type=F32)
            lanes = pl.ds(pl.multiple_of(cc * 2 * L, 2 * L), 2 * L)
            part[k, :, lanes] = acc.astype(BF16)
        for d in NEAR:
            zz = rows(mod4(z + d) * B, B)
            rs[k, d] = send(part.at[k, zz, :], rbuf.at[k, d - 1], r_ss.at[k, d], r_rs.at[k, d], dev(dz=d))
        if k == 0:
            with scope("wait_sq2"):
                for d in NEAR:
                    q2[d].wait_recv()
            total = st2_s[z] + sq2_r[0] + sq2_r[1] + sq2_r[2]
            inv = as_columns(lax.rsqrt(total / D + EPS))
        else:
            hidden_of(k - 1)

    dfs = []
    with scope("wait_d"):
        for d in (0,) + NEAR:
            if d == 0:
                local_d.wait()
            else:
                ds_[d].wait_recv()
            block = wdb.at[mod4(y - d), :, c]
            dfs.append(send(block, block, df_ss.at[d], df_rs.at[d], dev(dc=1)))
    hidden_of(K - 1)
    with scope("wait_df"):
        for f in dfs:
            f.wait_recv()
    with scope("wait_h"):
        for k in range(K):
            for d in NEAR:
                hs[k, d].wait_recv()

    a1, a2, a3, a4 = {}, {}, {}, {}
    for dy in (2, 1, 3, 0):
        yy = mod4(y + dy)
        acc = jnp.dot(hall[...], wdb[yy].reshape(2 * K * L, W), preferred_element_type=F32)
        psend[yy] = acc.astype(BF16).reshape(4, 2, B // 2, W)
        if dy:
            a1[dy] = send(psend.at[yy, :, 0], p1.at[dy - 1], p1_ss.at[dy], p1_rs.at[dy], dev(dy=dy))
        for dx in NEAR:
            a2[dx, dy] = send(psend.at[yy, mod4(x + dx), 1], p2.at[dx - 1, yy], p2_ss.at[dx, dy], p2_rs.at[dx, dy], dev(dx=dx))
    with scope("wait_p1"):
        for d in NEAR:
            a1[d].wait_recv()
    for xx in range(4):
        v = psend[y, xx, 0].astype(F32)
        for d in range(3):
            v = v + p1[d, xx].astype(F32)
        s1[xx] = v.astype(BF16)
    for d in NEAR:
        a3[d] = send(s1.at[mod4(x + d)], p3.at[d - 1], p3_ss.at[d], p3_rs.at[d], dev(dx=d))
    with scope("wait_p2"):
        for dx in NEAR:
            for dy in range(4):
                a2[dx, dy].wait_recv()
    for yy in range(4):
        v = psend[yy, x, 1].astype(F32)
        for d in range(3):
            v = v + p2[d, yy].astype(F32)
        s2[yy] = v.astype(BF16)
    for d in NEAR:
        a4[d] = send(s2.at[mod4(y + d)], p4.at[d - 1], p4_ss.at[d], p4_rs.at[d], dev(dy=d))
    piece = c * H + x * B
    with scope("wait_p3"):
        for d in NEAR:
            a3[d].wait_recv()
    v1 = s1[x].astype(F32)
    for d in range(3):
        v1 = v1 + p3[d].astype(F32)
    with scope("wait_p4"):
        for d in NEAR:
            a4[d].wait_recv()
    v2 = s2[y].astype(F32)
    for d in range(3):
        v2 = v2 + p4[d].astype(F32)
    stream = 0.5 * tok[rows(piece, B), :].astype(F32) + jnp.concatenate([v1, v2], axis=0)
    out[rows(piece, B), :] = stream.astype(BF16)

    ag = {d: send(out.at[rows(piece, B), :], out.at[rows(piece, B), :], o_ss.at[d], o_rs.at[d], dev(dx=d)) for d in NEAR}
    st_s[...] = row_sums(stream)
    ts = {d: send(st_s, st_r.at[d - 1], t_ss.at[d], t_rs.at[d], dev(dz=d)) for d in NEAR}
    with scope("wait_st"):
        for d in NEAR:
            ts[d].wait_recv()
    st3_r[8] = st_s[...] + st_r[0] + st_r[1] + st_r[2]
    t2 = {d: send(st3_r.at[8], st2_r.at[d - 1], t2_ss.at[d], t2_rs.at[d], dev(dy=d)) for d in NEAR}
    with scope("wait_st2"):
        for d in NEAR:
            t2[d].wait_recv()
    st3_r[2 * x + c] = st3_r[8] + st2_r[0] + st2_r[1] + st2_r[2]
    me = st3_r.at[2 * x + c]
    t3 = [send(me, me, t3_ss.at[i], t3_rs.at[i], dev(dx=d, dc=e)) for i, (d, e) in enumerate(ROW)]
    ofs = []
    with scope("wait_o"):
        for d in (0,) + NEAR:
            if d:
                ag[d].wait_recv()
            block = out.at[rows(c * H + mod4(x - d) * B, B), :]
            ofs.append(send(block, block, of_ss.at[d], of_rs.at[d], dev(dc=1)))
    with scope("wait_of"):
        for f in ofs:
            f.wait_recv()
    with scope("wait_st3"):
        for t in t3:
            t.wait_recv()
    with scope("wait_sends"):
        for s in sends:
            s.wait_send()
    for xx in range(4):
        for cc in range(2):
            factor = as_columns(lax.rsqrt(st3_r[2 * xx + cc] / D + EPS))
            r = slice(cc * H + xx * B, cc * H + (xx + 1) * B)
            for h in range(2):
                lanes = slice(h * L, (h + 1) * L)
                out[r, lanes] = (out[r, lanes].astype(F32) * factor * ogain[:, lanes]).astype(BF16)


def body(tokens, norm_gain, gate_weight, up_weight, down_weight, out_gain):
    dma = pltpu.SemaphoreType.DMA
    hbm = pl.BlockSpec(memory_space=pltpu.HBM)
    operands = (
        tokens,
        norm_gain.reshape(1, W),
        gate_weight,
        up_weight,
        down_weight.reshape(11, L, W),
        out_gain.reshape(1, W),
    )
    pair = lambda *shape: (dma(shape), dma(shape))
    return pl.pallas_call(
        kernel,
        out_shape=jax.ShapeDtypeStruct((T, W), BF16),
        in_specs=[hbm] * 6,
        out_specs=pl.BlockSpec(memory_space=pltpu.VMEM),
        scratch_shapes=[
            pltpu.VMEM((T, W), BF16),
            pltpu.VMEM((1, W), F32),
            pltpu.VMEM((W, 11 * L), BF16),
            pltpu.VMEM((W, 11 * L), BF16),
            pltpu.VMEM((11, L, W), BF16),
            pltpu.VMEM((1, W), F32),
            pltpu.VMEM((4, H, W), BF16),
            pltpu.VMEM((K, 2, 4, W, 2 * L), BF16),
            pltpu.VMEM((4, K, 2, L, W), BF16),
            pltpu.VMEM((K, H, 4 * L), BF16),
            pltpu.VMEM((K, 3, B, 4 * L), BF16),
            pltpu.VMEM((H, 2 * K * L), BF16),
            pltpu.VMEM((4, 4, 2, B // 2, W), BF16),
            pltpu.VMEM((3, 4, B // 2, W), BF16),
            pltpu.VMEM((3, 4, B // 2, W), BF16),
            pltpu.VMEM((4, B // 2, W), BF16),
            pltpu.VMEM((4, B // 2, W), BF16),
            pltpu.VMEM((3, B // 2, W), BF16),
            pltpu.VMEM((3, B // 2, W), BF16),
            pltpu.VMEM((4, 8, L), F32),
            pltpu.VMEM((3, 4, 8, L), F32),
            pltpu.VMEM((3, 8, L), F32),
            pltpu.VMEM((8, L), F32),
            pltpu.VMEM((3, 8, L), F32),
            pltpu.VMEM((4, 8, L), F32),
            pltpu.VMEM((3, 8, L), F32),
            pltpu.VMEM((9, 8, L), F32),
            dma((6,)),
            dma((2 * K + 1,)),
            *pair(4), *pair(4), *pair(4, 4),
            *pair(K, 4, 2), *pair(K, 4), *pair(4), *pair(4),
            *pair(K, 4), *pair(K, 4),
            *pair(4), *pair(4, 4), *pair(4), *pair(4),
            *pair(4), *pair(4),
            *pair(4), *pair(4), *pair(7),
            *pair(4), *pair(4),
        ],
        compiler_params=pltpu.CompilerParams(
            collective_id=0, has_side_effects=True, vmem_limit_bytes=40 * 1024 * 1024
        ),
    )(*[pltpu.with_memory_space_constraint(a, pltpu.HBM) for a in operands])


def solution(mesh):
    placed = (P(None, "ra"), P("ra"), P("ra", "cb"), P("ra", "cb"), P("cb", "ra"), P("ra"))
    return jax.shard_map(body, mesh=mesh, in_specs=placed, out_specs=P(None, "ra"), check_vma=False)
```

```python
import functools

import jax
import jax.numpy as jnp
from jax import lax
from jax.experimental import pallas as pl
from jax.experimental.pallas import tpu as pltpu
from jax.sharding import PartitionSpec as P

D = 4096
EPS = 1e-06
MESH = pl.DeviceIdType.MESH
scope = jax.named_scope
F32 = jnp.float32
BF16 = jnp.bfloat16
T = 1024
H = 512
B = 128
W = 256
L = 128
K = 3

R = 96

DIRECT = 4

SHORT = 2

NEAR = (2, 1, 3)
ROW = [(d, e) for d in (2, 1, 3) for e in range(2)] + [(0, 1)]


def mod4(v):
    return lax.rem(v + 4, 4)


def row_sums(v):
    sq = v * v
    hi = sq.astype(BF16)
    lo = (sq - hi.astype(F32)).astype(BF16)
    ones = jnp.ones((8, v.shape[1]), BF16)
    dims = (((1,), (1,)), ((), ()))
    out = lax.dot_general(ones, hi, dims, preferred_element_type=F32)
    return out + lax.dot_general(ones, lo, dims, preferred_element_type=F32)


def as_columns(row):
    return jnp.transpose(jnp.broadcast_to(row[:1], (L, L)), (1, 0))


def kernel(
    tok_h, gain_h, wg_h, wu_h, wd_h, ogain_h, out,
    tok, gain, wg, wu, wd, ogain, xg, wb, wdb, part, zr, zs, rbuf, rdir, hall, begun, psend, p1, p2, s1, s2, p3, p4,
    sq_s, sq_r, sq2_r, st_s, st_r, st2_s, st2_r, st3_r,
    sent, head, loc, xa_rs, xb_rs, xc_rs, w_rs, f_rs, d_rs, df_rs, relay_rs, sum_rs, shown_rs, h_rs,
    p_rs, q_rs, t_rs, o_rs, of_rs,
):
    ra, cb = lax.axis_index("ra"), lax.axis_index("cb")
    z, y, x, c = ra // 4, lax.rem(ra, 4), cb // 2, lax.rem(cb, 2)

    def dev(dz=0, dy=0, dx=0, dc=0):
        return (mod4(z + dz) * 4 + mod4(y + dy), mod4(x + dx) * 2 + lax.rem(c + dc, 2))

    sends = []

    def send(src, dst, rs, to):
        cp = pltpu.make_async_remote_copy(
            src_ref=src, dst_ref=dst, send_sem=sent, recv_sem=rs, device_id=to, device_id_type=MESH
        )
        cp.start()
        sends.append(cp)
        return cp

    def arrived(ref, sem):
        pltpu.make_async_copy(ref, ref, sem).wait()

    def local(src, dst, sem):
        cp = pltpu.make_async_copy(src, dst, sem)
        cp.start()
        return cp

    partners = [dev(dy=d) for d in NEAR] + [dev(dz=d) for d in NEAR] + [dev(dx=d, dc=e) for d, e in ROW]
    bar = pltpu.get_barrier_semaphore()
    for p in partners:
        pl.semaphore_signal(bar, inc=1, device_id=p, device_id_type=MESH)

    heads = [
        local(src, dst, head.at[i])
        for i, (src, dst) in enumerate(
            ((tok_h, tok), (gain_h, gain), (wg_h, wg), (wu_h, wu), (wd_h, wd), (ogain_h, ogain))
        )
    ]

    def tile0(yy):
        return jnp.minimum(3 * yy, 8)

    def cols(yy, k):
        return pl.ds(pl.multiple_of((tile0(yy) + k) * L, L), L)

    def rows(start, size):
        return pl.ds(pl.multiple_of(start, 16), size)

    for k in range(K):
        local(wg_h.at[:, cols(y, k)], wb.at[k, c, 0, :, :L], loc.at[k])
        local(wu_h.at[:, cols(y, k)], wb.at[k, c, 0, :, L:], loc.at[k])
    local_d = local(wd_h.at[pl.ds(tile0(y), K)], wdb.at[y, :, c], loc.at[K])

    heads[0].wait()
    heads[1].wait()
    t32 = tok[rows(c * H, H), :].astype(F32)
    xg[0] = (t32 * gain[...]).astype(BF16)
    sq = row_sums(t32)
    for b in range(4):
        sq_s[b] = sq[:, b * L : (b + 1) * L]
    for h in heads[2:]:
        h.wait()
    with scope("barrier"):
        pl.semaphore_wait(bar, len(partners))

    quarter = rows(x * R, R)
    rest = slice(4 * R, H)
    xa = {d: send(xg.at[0, quarter], xg.at[d, quarter], xa_rs.at[d - 1], dev(dy=d)) for d in NEAR}
    for d in NEAR:
        send(xg.at[0, rest], xg.at[d, rest], xb_rs, dev(dy=d))
    for d in NEAR:
        send(sq_s, sq_r.at[d - 1], q_rs.at[0], dev(dy=d))
    for k in range(K):
        for d in NEAR:
            yy = mod4(y + d)
            send(wg.at[:, cols(yy, k)], wb.at[k, c, d, :, :L], w_rs.at[k, d - 1], dev(dy=d))
            send(wu.at[:, cols(yy, k)], wb.at[k, c, d, :, L:], w_rs.at[k, d - 1], dev(dy=d))
    for d in NEAR:
        send(wd.at[pl.ds(tile0(mod4(y + d)), K)], wdb.at[y, :, c], d_rs, dev(dy=d))
    for d in (1, 3, 2):
        with scope(f"wait_xa#d={d}"):
            xa[d].wait_recv()
        for e in NEAR:
            send(xg.at[d, quarter], xg.at[d, quarter], xc_rs, dev(dx=e))
    with scope("wait_xb"):
        arrived(xg.at[1:, rest], xb_rs)
    with scope("wait_sq"):
        arrived(sq_r, q_rs.at[0])
    for b in range(4):
        st2_s[b] = sq_s[b] + sq_r[0, b] + sq_r[1, b] + sq_r[2, b]
    for d in NEAR:
        send(st2_s.at[mod4(z + d)], sq2_r.at[d - 1], q_rs.at[1], dev(dz=d))

    own_rows = rows(z * B, B)
    h = B // 2
    up1, dn1 = dev(dz=1), dev(dz=3)

    def half(zz, i):
        return rows(mod4(z + zz) * B + i * h, h)

    def columns_of(k):
        with scope(f"wait_w#k={k}"):
            for d in (0,) + NEAR:
                arrived(wb.at[k, c, d], w_rs.at[k, d - 1] if d else loc.at[k])
                send(wb.at[k, c, d], wb.at[k, c, d], f_rs.at[k], dev(dc=1))

    relay, shown = {}, {}

    def multiply(u):
        k, cc = u // 2, lax.rem(c + u % 2, 2)
        if u % 2:
            with scope(f"wait_f#k={k}"):
                arrived(wb.at[k, cc], f_rs.at[k])
        acc = jnp.zeros((H, 2 * L), F32)
        for d in range(4):
            acc = acc + jnp.dot(xg[d], wb[k, cc, d], preferred_element_type=F32)
        part[u] = acc.astype(BF16)
        if u >= DIRECT:
            for d in NEAR:
                zz = rows(mod4(z + d) * B, B)
                send(part.at[u, zz], rdir.at[u - DIRECT, d - 1], sum_rs.at[u], dev(dz=d))
            return
        relay[u, 0] = send(part.at[u, half(2, 0)], zr.at[u, 0], relay_rs.at[u, 0], up1)
        relay[u, 1] = send(part.at[u, half(2, 1)], zr.at[u, 1], relay_rs.at[u, 1], dn1)
        send(part.at[u, half(1, 1)], rbuf.at[u, 0, h:], sum_rs.at[u], up1)
        send(part.at[u, half(3, 0)], rbuf.at[u, 1, :h], sum_rs.at[u], dn1)

    def add(u):
        with scope(f"wait_relay#u={u}"):
            relay[u, 0].wait_recv()
        zs[u, 0] = (part[u, half(1, 0), :].astype(F32) + zr[u, 0].astype(F32)).astype(BF16)
        send(zs.at[u, 0], rbuf.at[u, 0, :h], sum_rs.at[u], up1)
        relay[u, 1].wait_recv()
        zs[u, 1] = (part[u, half(3, 1), :].astype(F32) + zr[u, 1].astype(F32)).astype(BF16)
        send(zs.at[u, 1], rbuf.at[u, 1, h:], sum_rs.at[u], dn1)

    def lanes_of(u):
        return pl.ds(pl.multiple_of((u // 2 * 2 + lax.rem(c + u % 2, 2)) * L, L), L)

    def finish(u):
        with scope(f"wait_sum#u={u}"):
            arrived(rdir.at[u - DIRECT] if u >= DIRECT else rbuf.at[u], sum_rs.at[u])
        total = part[u, own_rows, :].astype(F32)
        for v in [rdir[u - DIRECT, d] for d in range(3)] if u >= DIRECT else [rbuf[u, d] for d in range(2)]:
            total = total + v.astype(F32)
        gate, up = total[:, :L] * inv, total[:, L:] * inv
        hid = gate / (1.0 + jnp.exp(-gate)) * up
        if u < 2:
            hid = jnp.where(y == 3, jnp.zeros_like(hid), hid)
        hall[own_rows, lanes_of(u)] = hid.astype(BF16)
        block = hall.at[own_rows, lanes_of(u)]
        if u >= SHORT:
            for d in NEAR:
                send(block, block, h_rs.at[u // DIRECT], dev(dz=d))
            return
        shown[u, 0] = send(block, block, shown_rs.at[u, 0], up1)
        shown[u, 1] = send(block, block, shown_rs.at[u, 1], dn1)

    def pass_on(u):
        with scope(f"wait_shown#u={u}"):
            shown[u, 0].wait_recv()
            block = hall.at[half(3, 0), lanes_of(u)]
            send(block, block, h_rs.at[0], up1)
            shown[u, 1].wait_recv()
            block = hall.at[half(1, 1), lanes_of(u)]
            send(block, block, h_rs.at[0], dn1)

    columns_of(0)
    with scope("wait_xc"):
        arrived(xg.at[1:, : 3 * R], xc_rs)
    multiply(0)
    with scope("wait_sq2"):
        arrived(sq2_r, q_rs.at[1])
    total = st2_s[z] + sq2_r[0] + sq2_r[1] + sq2_r[2]
    inv = as_columns(lax.rsqrt(total / D + EPS))
    multiply(1)
    add(0)
    add(1)
    columns_of(1)
    multiply(2)
    multiply(3)
    finish(0)
    finish(1)
    add(2)
    add(3)
    columns_of(2)
    multiply(4)
    multiply(5)
    pass_on(0)
    pass_on(1)
    finish(2)
    finish(3)
    finish(4)
    finish(5)
    with scope("wait_d"):
        local_d.wait()
        arrived(wdb.at[:3, :, c], d_rs)
        send(wdb.at[:, :, c], wdb.at[:, :, c], df_rs, dev(dc=1))
    with scope("wait_df"):
        arrived(wdb.at[:, :, c], df_rs)
    with scope("wait_h03"):
        arrived(hall.at[:, : 2 * L], h_rs.at[0])
    for yy in range(4):
        w = wdb[yy, :2].reshape(4 * L, W)
        begun[yy] = jnp.dot(hall[:, : 4 * L], w, preferred_element_type=F32)
    with scope("wait_h45"):
        arrived(hall.at[: 3 * B, 4 * L :], h_rs.at[1])

    for dy in (2, 1, 3, 0):
        yy = mod4(y + dy)
        acc = begun[yy] + jnp.dot(hall[:, 4 * L :], wdb[yy, 2].reshape(2 * L, W), preferred_element_type=F32)
        psend[yy] = acc.astype(BF16).reshape(4, 2, B // 2, W)
        if dy:
            send(psend.at[yy, :, 0], p1.at[dy - 1], p_rs.at[0], dev(dy=dy))
        for dx in NEAR:
            send(psend.at[yy, mod4(x + dx), 1], p2.at[dx - 1, yy], p_rs.at[1], dev(dx=dx))
    with scope("wait_p1"):
        arrived(p1, p_rs.at[0])
    for xx in range(4):
        v = psend[y, xx, 0].astype(F32)
        for d in range(3):
            v = v + p1[d, xx].astype(F32)
        s1[xx] = v.astype(BF16)
    for d in NEAR:
        send(s1.at[mod4(x + d)], p3.at[d - 1], p_rs.at[2], dev(dx=d))
    with scope("wait_p2"):
        arrived(p2, p_rs.at[1])
    for yy in range(4):
        v = psend[yy, x, 1].astype(F32)
        for d in range(3):
            v = v + p2[d, yy].astype(F32)
        s2[yy] = v.astype(BF16)
    for d in NEAR:
        send(s2.at[mod4(y + d)], p4.at[d - 1], p_rs.at[3], dev(dy=d))
    piece = c * H + x * B
    with scope("wait_p3"):
        arrived(p3, p_rs.at[2])
    v1 = s1[x].astype(F32)
    for d in range(3):
        v1 = v1 + p3[d].astype(F32)
    with scope("wait_p4"):
        arrived(p4, p_rs.at[3])
    v2 = s2[y].astype(F32)
    for d in range(3):
        v2 = v2 + p4[d].astype(F32)
    stream = 0.5 * tok[rows(piece, B), :].astype(F32) + jnp.concatenate([v1, v2], axis=0)
    out[rows(piece, B), :] = stream.astype(BF16)

    ag = {d: send(out.at[rows(piece, B), :], out.at[rows(piece, B), :], o_rs.at[d - 1], dev(dx=d)) for d in NEAR}
    st_s[...] = row_sums(stream)
    for d in NEAR:
        send(st_s, st_r.at[d - 1], t_rs.at[0], dev(dz=d))
    with scope("wait_st"):
        arrived(st_r, t_rs.at[0])
    st3_r[8] = st_s[...] + st_r[0] + st_r[1] + st_r[2]
    for d in NEAR:
        send(st3_r.at[8], st2_r.at[d - 1], t_rs.at[1], dev(dy=d))
    with scope("wait_o"):
        for d in (0,) + NEAR:
            if d:
                ag[d].wait_recv()
            block = out.at[rows(c * H + mod4(x - d) * B, B), :]
            send(block, block, of_rs, dev(dc=1))
    with scope("wait_st2"):
        arrived(st2_r, t_rs.at[1])
    st3_r[2 * x + c] = st3_r[8] + st2_r[0] + st2_r[1] + st2_r[2]
    me = st3_r.at[2 * x + c]
    for d, e in ROW:
        send(me, me, t_rs.at[2], dev(dx=d, dc=e))
    with scope("wait_of"):
        arrived(out.at[:H], of_rs)
    with scope("wait_st3"):
        arrived(st3_r.at[:7], t_rs.at[2])
    with scope("wait_sends"):
        for s in sends:
            s.wait_send()
    _n = scope("norm")
    _n.__enter__()
    for xx in range(4):
        for cc in range(2):
            factor = as_columns(lax.rsqrt(st3_r[2 * xx + cc] / D + EPS))
            r = slice(cc * H + xx * B, cc * H + (xx + 1) * B)
            for h in range(2):
                lanes = slice(h * L, (h + 1) * L)
                out[r, lanes] = (out[r, lanes].astype(F32) * factor * ogain[:, lanes]).astype(BF16)
    _n.__exit__(None, None, None)


def body(tokens, norm_gain, gate_weight, up_weight, down_weight, out_gain):
    dma = pltpu.SemaphoreType.DMA
    hbm = pl.BlockSpec(memory_space=pltpu.HBM)
    operands = (
        tokens,
        norm_gain.reshape(1, W),
        gate_weight,
        up_weight,
        down_weight.reshape(11, L, W),
        out_gain.reshape(1, W),
    )
    return pl.pallas_call(
        kernel,
        out_shape=jax.ShapeDtypeStruct((T, W), BF16),
        in_specs=[hbm] * 6,
        out_specs=pl.BlockSpec(memory_space=pltpu.VMEM),
        scratch_shapes=[
            pltpu.VMEM((T, W), BF16),
            pltpu.VMEM((1, W), F32),
            pltpu.VMEM((W, 11 * L), BF16),
            pltpu.VMEM((W, 11 * L), BF16),
            pltpu.VMEM((11, L, W), BF16),
            pltpu.VMEM((1, W), F32),
            pltpu.VMEM((4, H, W), BF16),
            pltpu.VMEM((K, 2, 4, W, 2 * L), BF16),
            pltpu.VMEM((4, K, 2, L, W), BF16),
            pltpu.VMEM((2 * K, H, 2 * L), BF16),
            pltpu.VMEM((2 * K, 2, B // 2, 2 * L), BF16),
            pltpu.VMEM((2 * K, 2, B // 2, 2 * L), BF16),
            pltpu.VMEM((2 * K, 2, B, 2 * L), BF16),
            pltpu.VMEM((2 * K - DIRECT, 3, B, 2 * L), BF16),
            pltpu.VMEM((H, 2 * K * L), BF16),
            pltpu.VMEM((4, H, W), F32),
            pltpu.VMEM((4, 4, 2, B // 2, W), BF16),
            pltpu.VMEM((3, 4, B // 2, W), BF16),
            pltpu.VMEM((3, 4, B // 2, W), BF16),
            pltpu.VMEM((4, B // 2, W), BF16),
            pltpu.VMEM((4, B // 2, W), BF16),
            pltpu.VMEM((3, B // 2, W), BF16),
            pltpu.VMEM((3, B // 2, W), BF16),
            pltpu.VMEM((4, 8, L), F32),
            pltpu.VMEM((3, 4, 8, L), F32),
            pltpu.VMEM((3, 8, L), F32),
            pltpu.VMEM((8, L), F32),
            pltpu.VMEM((3, 8, L), F32),
            pltpu.VMEM((4, 8, L), F32),
            pltpu.VMEM((3, 8, L), F32),
            pltpu.VMEM((9, 8, L), F32),
            dma,
            dma((6,)),
            dma((K + 1,)),
            dma((3,)), dma, dma,
            dma((K, 3)), dma((K,)), dma, dma,
            dma((DIRECT, 2)), dma((2 * K,)),
            dma((SHORT, 2)), dma((2,)),
            dma((4,)), dma((2,)), dma((3,)),
            dma((3,)), dma,
        ],
        compiler_params=pltpu.CompilerParams(
            collective_id=0, has_side_effects=True, vmem_limit_bytes=40 * 1024 * 1024
        ),
    )(*[pltpu.with_memory_space_constraint(a, pltpu.HBM) for a in operands])


def solution(mesh):
    placed = (P(None, "ra"), P("ra"), P("ra", "cb"), P("ra", "cb"), P("cb", "ra"), P("ra"))
    return jax.shard_map(body, mesh=mesh, in_specs=placed, out_specs=P(None, "ra"), check_vma=False)
```

```python
import functools

import jax
import jax.numpy as jnp
from jax import lax
from jax.experimental import pallas as pl
from jax.experimental.pallas import tpu as pltpu
from jax.sharding import PartitionSpec as P

D = 4096
EPS = 1e-06
MESH = pl.DeviceIdType.MESH
scope = jax.named_scope
F32 = jnp.float32
BF16 = jnp.bfloat16
T = 1024
H = 512
B = 128
W = 256
L = 128
K = 3

R = 96

S0 = 64
HALVES = ((0, S0), (S0, B))

JOBS = (
    (0, 1, 0, B, True, True, 0),
    (1, 1, 0, B, True, True, 0),
    (2, 1, 0, B, True, False, 0),
    (3, 1, 0, B, True, False, 0),
    (4, 1, *HALVES[0], False, False, 1),
    (5, 1, *HALVES[0], False, False, 1),
    (4, 2, *HALVES[1], False, False, 2),
)

NEAR = (2, 1, 3)
PLANE = [(f, d, e) for f in (2, 1, 3, 0) for d in (2, 1, 3, 0) for e in (1, 0) if (f, d, e) != (0, 0, 0)]


def mod4(v):
    return lax.rem(v + 4, 4)


def row_sums(v):
    sq = v * v
    hi = sq.astype(BF16)
    lo = (sq - hi.astype(F32)).astype(BF16)
    ones = jnp.ones((8, v.shape[1]), BF16)
    dims = (((1,), (1,)), ((), ()))
    out = lax.dot_general(ones, hi, dims, preferred_element_type=F32)
    return (out + lax.dot_general(ones, lo, dims, preferred_element_type=F32))[:1]


def as_columns(row):
    return jnp.transpose(jnp.broadcast_to(row, (L, L)), (1, 0))


def kernel(
    tok_h, gain_h, wg_h, wu_h, wd_h, ogain_h, out,
    tok, gain, wg, wu, wd, ogain, xg, wb, wdb, part, zr, zs, rbuf, rdir, hall, begun, psend, p1, p2, s1, s2, p3, p4,
    sq_s, sq_r, sq2_r, st2_s, st_s, st_r, st_all, sq_n,
    sent, head, loc, xa_rs, xb_rs, xc_rs, w_rs, f_rs, d_rs, df_rs, relay_rs, sum_rs, shown_rs, h_rs,
    p_rs, q_rs, t_rs, o_rs, of_rs,
):
    ra, cb = lax.axis_index("ra"), lax.axis_index("cb")
    z, y, x, c = ra // 4, lax.rem(ra, 4), cb // 2, lax.rem(cb, 2)

    def dev(dz=0, dy=0, dx=0, dc=0):
        return (mod4(z + dz) * 4 + mod4(y + dy), mod4(x + dx) * 2 + lax.rem(c + dc, 2))

    sends = []

    def send(src, dst, rs, to):
        cp = pltpu.make_async_remote_copy(
            src_ref=src, dst_ref=dst, send_sem=sent, recv_sem=rs, device_id=to, device_id_type=MESH
        )
        cp.start()
        sends.append(cp)
        return cp

    def arrived(ref, sem):
        pltpu.make_async_copy(ref, ref, sem).wait()

    def local(src, dst, sem):
        cp = pltpu.make_async_copy(src, dst, sem)
        cp.start()
        return cp

    partners = [dev(dz=d) for d in NEAR] + [dev(dy=d) for d in NEAR] + [dev(dx=d) for d in NEAR] + [dev(dc=1)]
    bar = pltpu.get_barrier_semaphore()
    for p in partners:
        pl.semaphore_signal(bar, inc=1, device_id=p, device_id_type=MESH)

    heads = [
        local(src, dst, head.at[i])
        for i, (src, dst) in enumerate(
            ((tok_h, tok), (gain_h, gain), (wg_h, wg), (wu_h, wu), (wd_h, wd), (ogain_h, ogain))
        )
    ]

    def tile0(yy):
        return jnp.minimum(3 * yy, 8)

    def cols(yy, k):
        return pl.ds(pl.multiple_of((tile0(yy) + k) * L, L), L)

    def rows(start, size):
        return pl.ds(pl.multiple_of(start, 16), size)

    for k in range(K):
        local(wg_h.at[:, cols(y, k)], wb.at[k, c, 0, :, :L], loc.at[k])
        local(wu_h.at[:, cols(y, k)], wb.at[k, c, 0, :, L:], loc.at[k])
    local_d = local(wd_h.at[pl.ds(tile0(y), K)], wdb.at[y, :, c], loc.at[K])

    heads[0].wait()
    heads[1].wait()
    t32 = tok[rows(c * H, H), :].astype(F32)
    xg[0] = (t32 * gain[...]).astype(BF16)
    sq = row_sums(t32)
    for b in range(4):
        sq_s[b] = sq[:, b * L : (b + 1) * L]
    for h in heads[2:]:
        h.wait()
    with scope("barrier"):
        pl.semaphore_wait(bar, len(partners))

    quarter = rows(x * R, R)
    rest = slice(4 * R, H)
    xa = {d: send(xg.at[0, quarter], xg.at[d, quarter], xa_rs.at[d - 1], dev(dy=d)) for d in NEAR}
    for d in NEAR:
        send(xg.at[0, rest], xg.at[d, rest], xb_rs, dev(dy=d))
    for d in NEAR:
        send(sq_s, sq_r.at[d - 1], q_rs.at[0], dev(dy=d))
    for k in range(K):
        for d in NEAR:
            yy = mod4(y + d)
            send(wg.at[:, cols(yy, k)], wb.at[k, c, d, :, :L], w_rs.at[k, d - 1], dev(dy=d))
            send(wu.at[:, cols(yy, k)], wb.at[k, c, d, :, L:], w_rs.at[k, d - 1], dev(dy=d))
    for d in NEAR:
        send(wd.at[pl.ds(tile0(mod4(y + d)), K)], wdb.at[y, :, c], d_rs, dev(dy=d))
    for d in (1, 3, 2):
        with scope(f"wait_xa#d={d}"):
            xa[d].wait_recv()
        for e in NEAR:
            send(xg.at[d, quarter], xg.at[d, quarter], xc_rs, dev(dx=e))
    with scope("wait_xb"):
        arrived(xg.at[1:, rest], xb_rs)
    with scope("wait_sq"):
        arrived(sq_r, q_rs.at[0])
    for b in range(4):
        st2_s[b] = sq_s[b] + sq_r[0, b] + sq_r[1, b] + sq_r[2, b]
    for d in NEAR:
        send(st2_s.at[mod4(z + d)], sq2_r.at[d - 1], q_rs.at[1], dev(dz=d))

    up1, dn1 = dev(dz=1), dev(dz=3)

    def columns_of(k):
        with scope(f"wait_w#k={k}"):
            for d in (0,) + NEAR:
                arrived(wb.at[k, c, d], w_rs.at[k, d - 1] if d else loc.at[k])
                send(wb.at[k, c, d], wb.at[k, c, d], f_rs.at[k], dev(dc=1))

    def block_of(dz, r0, r1):
        return rows(mod4(z + dz) * B + r0, r1 - r0)

    def multiply(u):
        k, cc = u // 2, lax.rem(c + u % 2, 2)
        if u % 2:
            with scope(f"wait_f#k={k}"):
                arrived(wb.at[k, cc], f_rs.at[k])
        acc = jnp.zeros((H, 2 * L), F32)
        for d in range(4):
            acc = acc + jnp.dot(xg[d], wb[k, cc, d], preferred_element_type=F32)
        part[u] = acc.astype(BF16)

    def start(j):
        u, n, r0, r1, through, _, _ = JOBS[j]
        us, mid = slice(u, u + n), (r0 + r1) // 2
        if not through:
            for d in NEAR:
                send(part.at[us, block_of(d, r0, r1)], rdir.at[us, d - 1, r0:r1], sum_rs.at[j], dev(dz=d))
            return
        send(part.at[us, block_of(2, r0, mid)], zr.at[us, 0, r0:mid], relay_rs.at[j, 0], up1)
        send(part.at[us, block_of(2, mid, r1)], zr.at[us, 1, mid:r1], relay_rs.at[j, 1], dn1)
        send(part.at[us, block_of(1, mid, r1)], rbuf.at[us, 0, mid:r1], sum_rs.at[j], up1)
        send(part.at[us, block_of(3, r0, mid)], rbuf.at[us, 1, r0:mid], sum_rs.at[j], dn1)

    def add(j):
        u, n, r0, r1, _, _, _ = JOBS[j]
        us, mid = slice(u, u + n), (r0 + r1) // 2
        for side, to, dz, a, b in ((0, up1, 1, r0, mid), (1, dn1, 3, mid, r1)):
            with scope(f"wait_relay#j={j}"):
                arrived(zr.at[us, side, a:b], relay_rs.at[j, side])
            for v in range(u, u + n):
                mine = part[v, block_of(dz, a, b), :].astype(F32)
                zs[v, side, a:b] = (mine + zr[v, side, a:b].astype(F32)).astype(BF16)
            send(zs.at[us, side, a:b], rbuf.at[us, side, a:b], sum_rs.at[j], to)

    def lanes_of(u, n=1):
        if n == 2:
            return slice(u * L, (u + 2) * L)
        return pl.ds(pl.multiple_of((u // 2 * 2 + lax.rem(c + u % 2, 2)) * L, L), L)

    def finish(j):
        u, n, r0, r1, through, passing, group = JOBS[j]
        us = slice(u, u + n)
        came = rbuf if through else rdir
        with scope(f"wait_sum#j={j}"):
            arrived(came.at[us, :, r0:r1], sum_rs.at[j])
        for v in range(u, u + n):
            total = part[v, block_of(0, r0, r1), :].astype(F32)
            for d in range(2 if through else 3):
                total = total + came[v, d, r0:r1].astype(F32)
            gate, up = total[:, :L] * inv[r0:r1], total[:, L:] * inv[r0:r1]
            hid = gate / (1.0 + jnp.exp(-gate)) * up
            if v < 2:
                hid = jnp.where(y == 3, jnp.zeros_like(hid), hid)
            hall[z, r0:r1, lanes_of(v)] = hid.astype(BF16)
        block = hall.at[z, r0:r1, lanes_of(u, n)]
        if passing:
            send(block, block, shown_rs.at[j, 0], up1)
            send(block, block, shown_rs.at[j, 1], dn1)
        else:
            for d in NEAR:
                send(block, block, h_rs.at[group], dev(dz=d))

    def pass_on(j):
        u, n, r0, r1, _, _, group = JOBS[j]
        mid = (r0 + r1) // 2
        for side, to, dz, a, b in ((0, up1, 3, r0, mid), (1, dn1, 1, mid, r1)):
            with scope(f"wait_shown#j={j}"):
                arrived(hall.at[mod4(z + dz), r0:r1, lanes_of(u, n)], shown_rs.at[j, side])
            block = hall.at[mod4(z + dz), a:b, lanes_of(u, n)]
            send(block, block, h_rs.at[group], to)

    def all_hidden(group):
        tiles = sum((r1 - r0) * n * (1 if passing else 3) for _, n, r0, r1, _, passing, g in JOBS if g == group)
        with scope(f"wait_h#g={group}"):
            arrived(xg.at[:, : tiles // 8], h_rs.at[group])

    columns_of(0)
    with scope("wait_xc"):
        arrived(xg.at[1:, : 3 * R], xc_rs)
    multiply(0)
    start(0)
    with scope("wait_sq2"):
        arrived(sq2_r, q_rs.at[1])
    total = st2_s[z] + sq2_r[0] + sq2_r[1] + sq2_r[2]
    inv = as_columns(lax.rsqrt(total / D + EPS))
    multiply(1)
    start(1)
    add(0)
    add(1)
    columns_of(1)
    multiply(2)
    start(2)
    multiply(3)
    start(3)
    finish(0)
    finish(1)
    add(2)
    add(3)
    columns_of(2)
    multiply(4)
    start(4)
    multiply(5)
    start(5)
    start(6)
    pass_on(0)
    pass_on(1)
    finish(2)
    finish(3)
    finish(4)
    finish(5)
    with scope("wait_d"):
        local_d.wait()
        arrived(wdb.at[:3, :, c], d_rs)
        send(wdb.at[:, :, c], wdb.at[:, :, c], df_rs, dev(dc=1))
    finish(6)
    with scope("wait_df"):
        arrived(wdb.at[:, :, c], df_rs)

    all_hidden(0)
    for yy in range(4):
        w = wdb[yy, :2].reshape(4 * L, W)
        begun[yy] = jnp.dot(hall[:, :, : 4 * L].reshape(H, 4 * L), w, preferred_element_type=F32).reshape(4, B, W)
    for i, (r0, r1) in enumerate(HALVES):
        all_hidden(1 + i)
        mid = (r0 + r1) // 2
        a, b = slice(r0, mid), slice(mid, r1)
        for dy in (2, 1, 3, 0):
            yy = mod4(y + dy)
            hid = hall[:, r0:r1, 4 * L :].reshape(4 * (r1 - r0), 2 * L)
            acc = jnp.dot(hid, wdb[yy, 2].reshape(2 * L, W), preferred_element_type=F32)
            psend[yy, :, r0:r1] = (begun[yy, :, r0:r1] + acc.reshape(4, r1 - r0, W)).astype(BF16)
            if dy:
                send(psend.at[yy, :, a], p1.at[dy - 1, :, a], p_rs.at[i, 0], dev(dy=dy))
            for dx in NEAR:
                send(psend.at[yy, mod4(x + dx), b], p2.at[dx - 1, yy, b], p_rs.at[i, 1], dev(dx=dx))
    for i, (r0, r1) in enumerate(HALVES):
        mid = (r0 + r1) // 2
        a, b = slice(r0, mid), slice(mid, r1)
        with scope(f"wait_p1#i={i}"):
            arrived(p1.at[:, :, a], p_rs.at[i, 0])
        for xx in range(4):
            v = psend[y, xx, a].astype(F32)
            for d in range(3):
                v = v + p1[d, xx, a].astype(F32)
            s1[xx, a] = v.astype(BF16)
        for d in NEAR:
            send(s1.at[mod4(x + d), a], p3.at[d - 1, a], p_rs.at[i, 2], dev(dx=d))
        with scope(f"wait_p2#i={i}"):
            arrived(p2.at[:, :, b], p_rs.at[i, 1])
        for yy in range(4):
            v = psend[yy, x, b].astype(F32)
            for d in range(3):
                v = v + p2[d, yy, b].astype(F32)
            s2[yy, b] = v.astype(BF16)
        for d in NEAR:
            send(s2.at[mod4(y + d), b], p4.at[d - 1, b], p_rs.at[i, 3], dev(dy=d))
    pieces = []
    for i, (r0, r1) in enumerate(HALVES):
        mid = (r0 + r1) // 2
        a, b = slice(r0, mid), slice(mid, r1)
        with scope(f"wait_p3#i={i}"):
            arrived(p3.at[:, a], p_rs.at[i, 2])
        v = s1[x, a].astype(F32)
        for d in range(3):
            v = v + p3[d, a].astype(F32)
        pieces.append(v)
        with scope(f"wait_p4#i={i}"):
            arrived(p4.at[:, b], p_rs.at[i, 3])
        v = s2[y, b].astype(F32)
        for d in range(3):
            v = v + p4[d, b].astype(F32)
        pieces.append(v)
    piece = rows(c * H + x * B, B)
    stream = 0.5 * tok[piece, :].astype(F32) + jnp.concatenate(pieces, axis=0)
    out[piece, :] = stream.astype(BF16)

    st_s[...] = row_sums(stream)
    for d in NEAR:
        send(st_s, st_r.at[d - 1], t_rs.at[0], dev(dz=d))
    ag = {d: send(out.at[piece, :], out.at[piece, :], o_rs.at[d - 1], dev(dx=d)) for d in NEAR}
    with scope("wait_st"):
        arrived(st_r, t_rs.at[0])
    mine = 2 * x + c
    st_all[mine, 0] = st_s[...] + st_r[0] + st_r[1] + st_r[2]
    for f, d, e in PLANE:
        send(st_all.at[mine, 0], st_all.at[mine, f], t_rs.at[1], dev(dy=f, dx=d, dc=e))
    with scope("wait_o"):
        for d in (0,) + NEAR:
            if d:
                ag[d].wait_recv()
            block = out.at[rows(c * H + mod4(x - d) * B, B), :]
            send(block, block, of_rs, dev(dc=1))
    with scope("wait_of"):
        arrived(out.at[:H], of_rs)
    with scope("wait_st2"):
        arrived(sq_n.at[: len(PLANE)], t_rs.at[1])
    with scope("wait_sends"):
        for s in sends:
            s.wait_send()
    for xx in range(4):
        for cc in range(2):
            total = st_all[2 * xx + cc, 0] + st_all[2 * xx + cc, 1] + st_all[2 * xx + cc, 2] + st_all[2 * xx + cc, 3]
            factor = as_columns(lax.rsqrt(total / D + EPS))
            r = slice(cc * H + xx * B, cc * H + (xx + 1) * B)
            for h in range(2):
                lanes = slice(h * L, (h + 1) * L)
                out[r, lanes] = (out[r, lanes].astype(F32) * factor * ogain[:, lanes]).astype(BF16)


def body(tokens, norm_gain, gate_weight, up_weight, down_weight, out_gain):
    dma = pltpu.SemaphoreType.DMA
    hbm = pl.BlockSpec(memory_space=pltpu.HBM)
    operands = (
        tokens,
        norm_gain.reshape(1, W),
        gate_weight,
        up_weight,
        down_weight.reshape(11, L, W),
        out_gain.reshape(1, W),
    )
    return pl.pallas_call(
        kernel,
        out_shape=jax.ShapeDtypeStruct((T, W), BF16),
        in_specs=[hbm] * 6,
        out_specs=pl.BlockSpec(memory_space=pltpu.VMEM),
        scratch_shapes=[
            pltpu.VMEM((T, W), BF16),
            pltpu.VMEM((1, W), F32),
            pltpu.VMEM((W, 11 * L), BF16),
            pltpu.VMEM((W, 11 * L), BF16),
            pltpu.VMEM((11, L, W), BF16),
            pltpu.VMEM((1, W), F32),
            pltpu.VMEM((4, H, W), BF16),
            pltpu.VMEM((K, 2, 4, W, 2 * L), BF16),
            pltpu.VMEM((4, K, 2, L, W), BF16),
            pltpu.VMEM((2 * K, H, 2 * L), BF16),
            pltpu.VMEM((2 * K, 2, B, 2 * L), BF16),
            pltpu.VMEM((2 * K, 2, B, 2 * L), BF16),
            pltpu.VMEM((2 * K, 2, B, 2 * L), BF16),
            pltpu.VMEM((2 * K, 3, B, 2 * L), BF16),
            pltpu.VMEM((4, B, 2 * K * L), BF16),
            pltpu.VMEM((4, 4, B, W), F32),
            pltpu.VMEM((4, 4, B, W), BF16),
            pltpu.VMEM((3, 4, B, W), BF16),
            pltpu.VMEM((3, 4, B, W), BF16),
            pltpu.VMEM((4, B, W), BF16),
            pltpu.VMEM((4, B, W), BF16),
            pltpu.VMEM((3, B, W), BF16),
            pltpu.VMEM((3, B, W), BF16),
            pltpu.VMEM((4, 1, L), F32),
            pltpu.VMEM((3, 4, 1, L), F32),
            pltpu.VMEM((3, 1, L), F32),
            pltpu.VMEM((4, 1, L), F32),
            pltpu.VMEM((1, L), F32),
            pltpu.VMEM((3, 1, L), F32),
            pltpu.VMEM((8, 4, 1, L), F32),
            pltpu.VMEM((32, 1, L), F32),
            dma,
            dma((6,)),
            dma((K + 1,)),
            dma((3,)), dma, dma,
            dma((K, 3)), dma((K,)), dma, dma,
            dma((len(JOBS), 2)), dma((len(JOBS),)),
            dma((len(JOBS), 2)), dma((3,)),
            dma((2, 4)), dma((2,)), dma((2,)),
            dma((3,)), dma,
        ],
        compiler_params=pltpu.CompilerParams(
            collective_id=0, has_side_effects=True, vmem_limit_bytes=40 * 1024 * 1024
        ),
    )(*[pltpu.with_memory_space_constraint(a, pltpu.HBM) for a in operands])


def solution(mesh):
    placed = (P(None, "ra"), P("ra"), P("ra", "cb"), P("ra", "cb"), P("cb", "ra"), P("ra"))
    return jax.shard_map(body, mesh=mesh, in_specs=placed, out_specs=P(None, "ra"), check_vma=False)
```

```python
import functools

import jax
import jax.numpy as jnp
from jax import lax
from jax.experimental import pallas as pl
from jax.experimental.pallas import tpu as pltpu
from jax.sharding import PartitionSpec as P

D = 4096
EPS = 1e-06
MESH = pl.DeviceIdType.MESH
scope = jax.named_scope
F32 = jnp.float32
BF16 = jnp.bfloat16
T = 1024
H = 512
B = 128
W = 256
L = 128
K = 3

R = 96

S0 = 64
HALVES = ((0, S0), (S0, B))

JOBS = ((0, "z", False), (1, "z", False), (2, "z", True), (3, "z", True), (4, "y", False), (5, "y", False))

NEAR = (2, 1, 3)
PLANE = [(f, d, e) for f in (2, 1, 3, 0) for d in (2, 1, 3, 0) for e in (1, 0) if (f, d, e) != (0, 0, 0)]


def mod4(v):
    return lax.rem(v + 4, 4)


def row_sums(v):
    sq = v * v
    hi = sq.astype(BF16)
    lo = (sq - hi.astype(F32)).astype(BF16)
    ones = jnp.ones((8, v.shape[1]), BF16)
    dims = (((1,), (1,)), ((), ()))
    out = lax.dot_general(ones, hi, dims, preferred_element_type=F32)
    return (out + lax.dot_general(ones, lo, dims, preferred_element_type=F32))[:1]


def as_columns(row):
    return jnp.transpose(jnp.broadcast_to(row, (L, L)), (1, 0))


def kernel(
    tok_h, gain_h, wg_h, wu_h, wd_h, ogain_h, out,
    tok, gain, wg, wu, wd, ogain, xg, xz, wb, wdb, part, zr, zs, rbuf, rdir, hall, hz, begun, psend, p1, p2, s1, s2, p3, p4,
    sq_s, sq_r, sq2_r, sq3_r, st2_s, st_s, st_r, st_all, sq_n,
    sent, head, loc, xa_rs, xb_rs, xc_rs, xz_rs, w_rs, f_rs, d_rs, df_rs, relay_rs, sum_rs, h_rs, hy_rs,
    p_rs, q_rs, t_rs, o_rs, of_rs,
):
    ra, cb = lax.axis_index("ra"), lax.axis_index("cb")
    z, y, x, c = ra // 4, lax.rem(ra, 4), cb // 2, lax.rem(cb, 2)

    def dev(dz=0, dy=0, dx=0, dc=0):
        return (mod4(z + dz) * 4 + mod4(y + dy), mod4(x + dx) * 2 + lax.rem(c + dc, 2))

    sends = []

    def send(src, dst, rs, to):
        cp = pltpu.make_async_remote_copy(
            src_ref=src, dst_ref=dst, send_sem=sent, recv_sem=rs, device_id=to, device_id_type=MESH
        )
        cp.start()
        sends.append(cp)
        return cp

    def arrived(ref, sem):
        pltpu.make_async_copy(ref, ref, sem).wait()

    def local(src, dst, sem):
        cp = pltpu.make_async_copy(src, dst, sem)
        cp.start()
        return cp

    partners = [dev(dz=d) for d in NEAR] + [dev(dy=d) for d in NEAR] + [dev(dx=d) for d in NEAR] + [dev(dc=1)]
    bar = pltpu.get_barrier_semaphore()
    for p in partners:
        pl.semaphore_signal(bar, inc=1, device_id=p, device_id_type=MESH)

    heads = [
        local(src, dst, head.at[i])
        for i, (src, dst) in enumerate(
            ((tok_h, tok), (gain_h, gain), (wg_h, wg), (wu_h, wu), (wd_h, wd), (ogain_h, ogain))
        )
    ]

    def tile0(yy):
        return jnp.minimum(3 * yy, 8)

    def cols(yy, k):
        return pl.ds(pl.multiple_of((tile0(yy) + k) * L, L), L)

    def rows(start, size):
        return pl.ds(pl.multiple_of(start, 16), size)

    for k in range(K):
        own = cols(y if k < 2 else z, k)
        local(wg_h.at[:, own], wb.at[k, c, 0, :, :L], loc.at[k])
        local(wu_h.at[:, own], wb.at[k, c, 0, :, L:], loc.at[k])
    local_d = local(wd_h.at[pl.ds(tile0(y), K)], wdb.at[y, :, c], loc.at[K])

    heads[0].wait()
    heads[1].wait()
    t32 = tok[rows(c * H, H), :].astype(F32)
    xg[0] = (t32 * gain[...]).astype(BF16)
    sq = row_sums(t32)
    for b in range(4):
        sq_s[b] = sq[:, b * L : (b + 1) * L]
    for h in heads[2:]:
        h.wait()
    with scope("barrier"):
        pl.semaphore_wait(bar, len(partners))

    quarter = rows(x * R, R)
    rest = slice(4 * R, H)
    xa = {d: send(xg.at[0, quarter], xg.at[d, quarter], xa_rs.at[d - 1], dev(dy=d)) for d in NEAR}
    for d in NEAR:
        send(xg.at[0, rest], xg.at[d, rest], xb_rs, dev(dy=d))
    for d in NEAR:
        send(sq_s, sq_r.at[d - 1], q_rs.at[0], dev(dy=d))
    near_z = {d: send(xg.at[0], xz.at[d - 1], xz_rs.at[d - 1], dev(dz=d)) for d in (1, 3)}
    for k in range(K):
        for d in NEAR:
            own, to = (mod4(y + d), dev(dy=d)) if k < 2 else (mod4(z + d), dev(dz=d))
            send(wg.at[:, cols(own, k)], wb.at[k, c, d, :, :L], w_rs.at[k, d - 1], to)
            send(wu.at[:, cols(own, k)], wb.at[k, c, d, :, L:], w_rs.at[k, d - 1], to)
    for d in (1, 3, 2):
        with scope(f"wait_xa#d={d}"):
            xa[d].wait_recv()
        for e in NEAR:
            send(xg.at[d, quarter], xg.at[d, quarter], xc_rs, dev(dx=e))
    with scope("wait_xb"):
        arrived(xg.at[1:, rest], xb_rs)
    with scope("wait_sq"):
        arrived(sq_r, q_rs.at[0])
    for b in range(4):
        st2_s[b] = sq_s[b] + sq_r[0, b] + sq_r[1, b] + sq_r[2, b]
    for d in NEAR:
        send(st2_s.at[mod4(z + d)], sq2_r.at[d - 1], q_rs.at[1], dev(dz=d))
        send(st2_s.at[y], sq3_r.at[d - 1], q_rs.at[2], dev(dz=d))
    with scope("wait_xz"):
        for d, to, half in ((1, 1, slice(0, H // 2)), (3, 3, slice(H // 2, H))):
            near_z[d].wait_recv()
            send(xz.at[d - 1, half], xz.at[1, half], xz_rs.at[1], dev(dz=to))

    def columns_of(k):
        with scope(f"wait_w#k={k}"):
            for d in (0,) + NEAR:
                arrived(wb.at[k, c, d], w_rs.at[k, d - 1] if d else loc.at[k])
                send(wb.at[k, c, d], wb.at[k, c, d], f_rs.at[k], dev(dc=1))

    def along(axis, d):
        return (dev(dz=d), mod4(z + d)) if axis == "z" else (dev(dy=d), mod4(y + d))

    def block_of(at, r0=0, r1=B):
        return rows(at * B + r0, r1 - r0)

    def multiply(u):
        k, cc = u // 2, lax.rem(c + u % 2, 2)
        if u % 2:
            with scope(f"wait_f#k={k}"):
                arrived(wb.at[k, cc], f_rs.at[k])
        acc = jnp.zeros((H, 2 * L), F32)
        for d in range(4):
            xs = xz[d - 1] if u >= 4 and d else xg[d]
            acc = acc + jnp.dot(xs, wb[k, cc, d], preferred_element_type=F32)
        part[u] = acc.astype(BF16)

    half = B // 2

    def start(u):
        _, axis, through = JOBS[u]
        if not through:
            for d in NEAR:
                to, at = along(axis, d)
                send(part.at[u, block_of(at)], rdir.at[u, d - 1], sum_rs.at[u], to)
            return
        far = along(axis, 2)[1]
        (up1, above), (dn1, below) = along(axis, 1), along(axis, 3)
        send(part.at[u, block_of(far, 0, half)], zr.at[u, 0], relay_rs.at[u, 0], up1)
        send(part.at[u, block_of(far, half, B)], zr.at[u, 1], relay_rs.at[u, 1], dn1)
        send(part.at[u, block_of(above, half, B)], rbuf.at[u, 0, half:], sum_rs.at[u], up1)
        send(part.at[u, block_of(below, 0, half)], rbuf.at[u, 1, :half], sum_rs.at[u], dn1)

    def add(u):
        _, axis, _ = JOBS[u]
        for side, d, a, b in ((0, 1, 0, half), (1, 3, half, B)):
            to, at = along(axis, d)
            with scope(f"wait_relay#u={u}"):
                arrived(zr.at[u, side], relay_rs.at[u, side])
            zs[u, side] = (part[u, block_of(at, a, b), :].astype(F32) + zr[u, side].astype(F32)).astype(BF16)
            send(zs.at[u, side], rbuf.at[u, side, a:b], sum_rs.at[u], to)

    def core_of(u):
        return lax.rem(c + u % 2, 2)

    def finish(u):
        _, axis, through = JOBS[u]
        came = rbuf if through else rdir
        with scope(f"wait_sum#u={u}"):
            arrived(came.at[u], sum_rs.at[u])
        total = part[u, block_of(along(axis, 0)[1]), :].astype(F32)
        for d in range(2 if through else 3):
            total = total + came[u, d].astype(F32)
        scale = inv if axis == "z" else inv_y
        gate, up = total[:, :L] * scale, total[:, L:] * scale
        hid = gate / (1.0 + jnp.exp(-gate)) * up
        if u < 2:
            hid = jnp.where(y == 3, jnp.zeros_like(hid), hid)
        if axis == "z":
            lanes = pl.ds(pl.multiple_of((u // 2 * 2 + core_of(u)) * L, L), L)
            hall[z, :, lanes] = hid.astype(BF16)
            block = hall.at[z, :, lanes]
        else:
            lanes = pl.ds(pl.multiple_of(core_of(u) * L, L), L)
            hz[z, :, lanes] = hid.astype(BF16)
            block = hz.at[z, :, lanes]
        for d in NEAR:
            send(block, block, h_rs.at[u // 4], dev(dz=d))

    columns_of(0)
    with scope("wait_xc"):
        arrived(xg.at[1:, : 3 * R], xc_rs)
    multiply(0)
    start(0)
    with scope("wait_sq2"):
        arrived(sq2_r, q_rs.at[1])
        arrived(sq3_r, q_rs.at[2])
    inv = as_columns(lax.rsqrt((st2_s[z] + sq2_r[0] + sq2_r[1] + sq2_r[2]) / D + EPS))
    inv_y = as_columns(lax.rsqrt((st2_s[y] + sq3_r[0] + sq3_r[1] + sq3_r[2]) / D + EPS))
    multiply(1)
    start(1)
    columns_of(2)
    with scope("wait_xz2"):
        arrived(xz.at[1], xz_rs.at[1])
    multiply(4)
    start(4)
    multiply(5)
    start(5)
    for d in NEAR:
        send(wd.at[pl.ds(tile0(mod4(y + d)), K)], wdb.at[y, :, c], d_rs.at[d - 1], dev(dy=d))
    columns_of(1)
    multiply(2)
    start(2)
    finish(0)
    multiply(3)
    start(3)
    finish(1)
    add(2)
    finish(4)
    add(3)
    finish(5)
    finish(2)
    finish(3)
    with scope("wait_hz"):
        arrived(hz.at[:3], h_rs.at[1])
    last = slice(4 * L, 6 * L)
    for i, (r0, r1) in enumerate(HALVES):
        for d in NEAR:
            send(hz.at[mod4(y + d), r0:r1], hall.at[y, r0:r1, last], hy_rs.at[i], dev(dy=d))
    hall[y, :, last] = hz[y]
    with scope("wait_d"):
        for d in (0, 1, 3, 2):
            if d:
                arrived(wdb.at[0, :, c], d_rs.at[d - 1])
            else:
                local_d.wait()
            block = wdb.at[mod4(y - d), :, c]
            send(block, block, df_rs, dev(dc=1))
    with scope("wait_df"):
        arrived(wdb.at[:, :, c], df_rs)

    with scope("wait_h"):
        arrived(hall.at[:3, :, : 4 * L], h_rs.at[0])
    for yy in range(4):
        w = wdb[yy, :2].reshape(4 * L, W)
        begun[yy] = jnp.dot(hall[:, :, : 4 * L].reshape(H, 4 * L), w, preferred_element_type=F32).reshape(4, B, W)
    for i, (r0, r1) in enumerate(HALVES):
        with scope(f"wait_hy#i={i}"):
            arrived(hall.at[:3, r0:r1, last], hy_rs.at[i])
        mid = (r0 + r1) // 2
        a, b = slice(r0, mid), slice(mid, r1)
        for dy in (2, 1, 3, 0):
            yy = mod4(y + dy)
            hid = hall[:, r0:r1, 4 * L :].reshape(4 * (r1 - r0), 2 * L)
            acc = jnp.dot(hid, wdb[yy, 2].reshape(2 * L, W), preferred_element_type=F32)
            psend[yy, :, r0:r1] = (begun[yy, :, r0:r1] + acc.reshape(4, r1 - r0, W)).astype(BF16)
            if dy:
                send(psend.at[yy, :, a], p1.at[dy - 1, :, a], p_rs.at[i, 0], dev(dy=dy))
            for dx in NEAR:
                send(psend.at[yy, mod4(x + dx), b], p2.at[dx - 1, yy, b], p_rs.at[i, 1], dev(dx=dx))
    for i, (r0, r1) in enumerate(HALVES):
        mid = (r0 + r1) // 2
        a, b = slice(r0, mid), slice(mid, r1)
        with scope(f"wait_p1#i={i}"):
            arrived(p1.at[:, :, a], p_rs.at[i, 0])
        for xx in range(4):
            v = psend[y, xx, a].astype(F32)
            for d in range(3):
                v = v + p1[d, xx, a].astype(F32)
            s1[xx, a] = v.astype(BF16)
        for d in NEAR:
            send(s1.at[mod4(x + d), a], p3.at[d - 1, a], p_rs.at[i, 2], dev(dx=d))
        with scope(f"wait_p2#i={i}"):
            arrived(p2.at[:, :, b], p_rs.at[i, 1])
        for yy in range(4):
            v = psend[yy, x, b].astype(F32)
            for d in range(3):
                v = v + p2[d, yy, b].astype(F32)
            s2[yy, b] = v.astype(BF16)
        for d in NEAR:
            send(s2.at[mod4(y + d), b], p4.at[d - 1, b], p_rs.at[i, 3], dev(dy=d))
    pieces = []
    for i, (r0, r1) in enumerate(HALVES):
        mid = (r0 + r1) // 2
        a, b = slice(r0, mid), slice(mid, r1)
        with scope(f"wait_p3#i={i}"):
            arrived(p3.at[:, a], p_rs.at[i, 2])
        v = s1[x, a].astype(F32)
        for d in range(3):
            v = v + p3[d, a].astype(F32)
        pieces.append(v)
        with scope(f"wait_p4#i={i}"):
            arrived(p4.at[:, b], p_rs.at[i, 3])
        v = s2[y, b].astype(F32)
        for d in range(3):
            v = v + p4[d, b].astype(F32)
        pieces.append(v)
    piece = rows(c * H + x * B, B)
    stream = 0.5 * tok[piece, :].astype(F32) + jnp.concatenate(pieces, axis=0)
    out[piece, :] = stream.astype(BF16)

    st_s[...] = row_sums(stream)
    for d in NEAR:
        send(st_s, st_r.at[d - 1], t_rs.at[0], dev(dz=d))
    ag = {d: send(out.at[piece, :], out.at[piece, :], o_rs.at[d - 1], dev(dx=d)) for d in NEAR}
    with scope("wait_st"):
        arrived(st_r, t_rs.at[0])
    mine = 2 * x + c
    st_all[mine, 0] = st_s[...] + st_r[0] + st_r[1] + st_r[2]
    for f, d, e in PLANE:
        send(st_all.at[mine, 0], st_all.at[mine, f], t_rs.at[1], dev(dy=f, dx=d, dc=e))
    with scope("wait_o"):
        for d in (0,) + NEAR:
            if d:
                ag[d].wait_recv()
            block = out.at[rows(c * H + mod4(x - d) * B, B), :]
            send(block, block, of_rs, dev(dc=1))
    with scope("wait_of"):
        arrived(out.at[:H], of_rs)
    with scope("wait_st2"):
        arrived(sq_n.at[: len(PLANE)], t_rs.at[1])
    with scope("wait_sends"):
        for s in sends:
            s.wait_send()
    for xx in range(4):
        for cc in range(2):
            total = st_all[2 * xx + cc, 0] + st_all[2 * xx + cc, 1] + st_all[2 * xx + cc, 2] + st_all[2 * xx + cc, 3]
            factor = as_columns(lax.rsqrt(total / D + EPS))
            r = slice(cc * H + xx * B, cc * H + (xx + 1) * B)
            for h in range(2):
                lanes = slice(h * L, (h + 1) * L)
                out[r, lanes] = (out[r, lanes].astype(F32) * factor * ogain[:, lanes]).astype(BF16)


def body(tokens, norm_gain, gate_weight, up_weight, down_weight, out_gain):
    dma = pltpu.SemaphoreType.DMA
    hbm = pl.BlockSpec(memory_space=pltpu.HBM)
    operands = (
        tokens,
        norm_gain.reshape(1, W),
        gate_weight,
        up_weight,
        down_weight.reshape(11, L, W),
        out_gain.reshape(1, W),
    )
    return pl.pallas_call(
        kernel,
        out_shape=jax.ShapeDtypeStruct((T, W), BF16),
        in_specs=[hbm] * 6,
        out_specs=pl.BlockSpec(memory_space=pltpu.VMEM),
        scratch_shapes=[
            pltpu.VMEM((T, W), BF16),
            pltpu.VMEM((1, W), F32),
            pltpu.VMEM((W, 11 * L), BF16),
            pltpu.VMEM((W, 11 * L), BF16),
            pltpu.VMEM((11, L, W), BF16),
            pltpu.VMEM((1, W), F32),
            pltpu.VMEM((4, H, W), BF16),
            pltpu.VMEM((3, H, W), BF16),
            pltpu.VMEM((K, 2, 4, W, 2 * L), BF16),
            pltpu.VMEM((4, K, 2, L, W), BF16),
            pltpu.VMEM((2 * K, H, 2 * L), BF16),
            pltpu.VMEM((2 * K, 2, B // 2, 2 * L), BF16),
            pltpu.VMEM((2 * K, 2, B // 2, 2 * L), BF16),
            pltpu.VMEM((2 * K, 2, B, 2 * L), BF16),
            pltpu.VMEM((2 * K, 3, B, 2 * L), BF16),
            pltpu.VMEM((4, B, 2 * K * L), BF16),
            pltpu.VMEM((4, B, 2 * L), BF16),
            pltpu.VMEM((4, 4, B, W), F32),
            pltpu.VMEM((4, 4, B, W), BF16),
            pltpu.VMEM((3, 4, B, W), BF16),
            pltpu.VMEM((3, 4, B, W), BF16),
            pltpu.VMEM((4, B, W), BF16),
            pltpu.VMEM((4, B, W), BF16),
            pltpu.VMEM((3, B, W), BF16),
            pltpu.VMEM((3, B, W), BF16),
            pltpu.VMEM((4, 1, L), F32),
            pltpu.VMEM((3, 4, 1, L), F32),
            pltpu.VMEM((3, 1, L), F32),
            pltpu.VMEM((3, 1, L), F32),
            pltpu.VMEM((4, 1, L), F32),
            pltpu.VMEM((1, L), F32),
            pltpu.VMEM((3, 1, L), F32),
            pltpu.VMEM((8, 4, 1, L), F32),
            pltpu.VMEM((32, 1, L), F32),
            dma,
            dma((6,)),
            dma((K + 1,)),
            dma((3,)), dma, dma, dma((3,)),
            dma((K, 3)), dma((K,)), dma((3,)), dma,
            dma((len(JOBS), 2)), dma((len(JOBS),)),
            dma((2,)), dma((2,)),
            dma((2, 4)), dma((3,)), dma((2,)),
            dma((3,)), dma,
        ],
        compiler_params=pltpu.CompilerParams(
            collective_id=0, has_side_effects=True, vmem_limit_bytes=40 * 1024 * 1024
        ),
    )(*[pltpu.with_memory_space_constraint(a, pltpu.HBM) for a in operands])


def solution(mesh):
    placed = (P(None, "ra"), P("ra"), P("ra", "cb"), P("ra", "cb"), P("cb", "ra"), P("ra"))
    return jax.shard_map(body, mesh=mesh, in_specs=placed, out_specs=P(None, "ra"), check_vma=False)
```

```python
import functools

import jax
import jax.numpy as jnp
from jax import lax
from jax.experimental import pallas as pl
from jax.experimental.pallas import tpu as pltpu
from jax.sharding import PartitionSpec as P

D = 4096
EPS = 1e-06
MESH = pl.DeviceIdType.MESH
scope = jax.named_scope
F32 = jnp.float32
BF16 = jnp.bfloat16
T = 1024
H = 512
B = 128
W = 256
L = 128
K = 3

R = 96

S0 = 64
HALVES = ((0, S0), (S0, B))

JOBS = ((0, "z", False), (1, "z", False), (2, "z", True), (3, "z", True), (4, "y", False), (5, "y", False))

NEAR = (2, 1, 3)
EVERYONE = [(g, f, d, e) for g in range(4) for f in range(4) for d in range(4) for e in range(2)][1:]
EVERYONE.sort(key=lambda s: -sum(min(v, 4 - v) for v in s[:3]))


def mod4(v):
    return lax.rem(v + 4, 4)


def row_sums(v):
    sq = v * v
    hi = sq.astype(BF16)
    lo = (sq - hi.astype(F32)).astype(BF16)
    ones = jnp.ones((8, v.shape[1]), BF16)
    dims = (((1,), (1,)), ((), ()))
    out = lax.dot_general(ones, hi, dims, preferred_element_type=F32)
    return (out + lax.dot_general(ones, lo, dims, preferred_element_type=F32))[:1]


def as_columns(row):
    return jnp.transpose(jnp.broadcast_to(row, (L, L)), (1, 0))


def kernel(
    tok_h, gain_h, wg_h, wu_h, wd_h, ogain_h, out,
    tok, gain, wg, wu, wd, ogain, xg, xz, wb, wdb, part, zr, zs, rbuf, rdir, hall, hz, begun, psend, p1, p2, s1, s2, p3, p4,
    sq_s, sq_r, sq2_r, sq3_r, st2_s, st_all, sq_n,
    sent, head, loc, xa_rs, xb_rs, xc_rs, xz_rs, w_rs, f_rs, d_rs, df_rs, relay_rs, sum_rs, h_rs, hy_rs,
    p_rs, q_rs, t_rs, o_rs, of_rs,
):
    ra, cb = lax.axis_index("ra"), lax.axis_index("cb")
    z, y, x, c = ra // 4, lax.rem(ra, 4), cb // 2, lax.rem(cb, 2)

    def dev(dz=0, dy=0, dx=0, dc=0):
        return (mod4(z + dz) * 4 + mod4(y + dy), mod4(x + dx) * 2 + lax.rem(c + dc, 2))

    sends = []

    def send(src, dst, rs, to):
        cp = pltpu.make_async_remote_copy(
            src_ref=src, dst_ref=dst, send_sem=sent, recv_sem=rs, device_id=to, device_id_type=MESH
        )
        cp.start()
        sends.append(cp)
        return cp

    def arrived(ref, sem):
        pltpu.make_async_copy(ref, ref, sem).wait()

    def local(src, dst, sem):
        cp = pltpu.make_async_copy(src, dst, sem)
        cp.start()
        return cp

    partners = [dev(dz=d) for d in NEAR] + [dev(dy=d) for d in NEAR] + [dev(dx=d) for d in NEAR] + [dev(dc=1)]
    bar = pltpu.get_barrier_semaphore()
    for p in partners:
        pl.semaphore_signal(bar, inc=1, device_id=p, device_id_type=MESH)

    heads = [
        local(src, dst, head.at[i])
        for i, (src, dst) in enumerate(
            ((tok_h, tok), (gain_h, gain), (wg_h, wg), (wu_h, wu), (wd_h, wd), (ogain_h, ogain))
        )
    ]

    def tile0(yy):
        return jnp.minimum(3 * yy, 8)

    def cols(yy, k):
        return pl.ds(pl.multiple_of((tile0(yy) + k) * L, L), L)

    def rows(start, size):
        return pl.ds(pl.multiple_of(start, 16), size)

    for k in range(K):
        own = cols(y if k < 2 else z, k)
        local(wg_h.at[:, own], wb.at[k, c, 0, :, :L], loc.at[k])
        local(wu_h.at[:, own], wb.at[k, c, 0, :, L:], loc.at[k])
    local_d = local(wd_h.at[pl.ds(tile0(y), K)], wdb.at[y, :, c], loc.at[K])

    heads[0].wait()
    heads[1].wait()
    t32 = tok[rows(c * H, H), :].astype(F32)
    xg[0] = (t32 * gain[...]).astype(BF16)
    sq = row_sums(t32)
    for b in range(4):
        sq_s[b] = sq[:, b * L : (b + 1) * L]
    for h in heads[2:]:
        h.wait()
    with scope("barrier"):
        pl.semaphore_wait(bar, len(partners))

    quarter = rows(x * R, R)
    rest = slice(4 * R, H)
    xa = {d: send(xg.at[0, quarter], xg.at[d, quarter], xa_rs.at[d - 1], dev(dy=d)) for d in NEAR}
    for d in NEAR:
        send(xg.at[0, rest], xg.at[d, rest], xb_rs, dev(dy=d))
    for d in NEAR:
        send(sq_s, sq_r.at[d - 1], q_rs.at[0], dev(dy=d))
    near_z = {d: send(xg.at[0], xz.at[d - 1], xz_rs.at[d - 1], dev(dz=d)) for d in (1, 3)}
    for k in range(K):
        for d in NEAR:
            own, to = (mod4(y + d), dev(dy=d)) if k < 2 else (mod4(z + d), dev(dz=d))
            send(wg.at[:, cols(own, k)], wb.at[k, c, d, :, :L], w_rs.at[k, d - 1], to)
            send(wu.at[:, cols(own, k)], wb.at[k, c, d, :, L:], w_rs.at[k, d - 1], to)
    for d in (1, 3, 2):
        with scope(f"wait_xa#d={d}"):
            xa[d].wait_recv()
        for e in NEAR:
            send(xg.at[d, quarter], xg.at[d, quarter], xc_rs, dev(dx=e))
    with scope("wait_xb"):
        arrived(xg.at[1:, rest], xb_rs)
    with scope("wait_sq"):
        arrived(sq_r, q_rs.at[0])
    for b in range(4):
        st2_s[b] = sq_s[b] + sq_r[0, b] + sq_r[1, b] + sq_r[2, b]
    for d in NEAR:
        send(st2_s.at[mod4(z + d)], sq2_r.at[d - 1], q_rs.at[1], dev(dz=d))
        send(st2_s.at[y], sq3_r.at[d - 1], q_rs.at[2], dev(dz=d))
    with scope("wait_xz"):
        for d, to, half in ((1, 1, slice(0, H // 2)), (3, 3, slice(H // 2, H))):
            near_z[d].wait_recv()
            send(xz.at[d - 1, half], xz.at[1, half], xz_rs.at[1], dev(dz=to))

    def columns_of(k):
        with scope(f"wait_w#k={k}"):
            for d in (0,) + NEAR:
                arrived(wb.at[k, c, d], w_rs.at[k, d - 1] if d else loc.at[k])
                send(wb.at[k, c, d], wb.at[k, c, d], f_rs.at[k], dev(dc=1))

    def along(axis, d):
        return (dev(dz=d), mod4(z + d)) if axis == "z" else (dev(dy=d), mod4(y + d))

    def block_of(at, r0=0, r1=B):
        return rows(at * B + r0, r1 - r0)

    def multiply(u):
        k, cc = u // 2, lax.rem(c + u % 2, 2)
        if u % 2:
            with scope(f"wait_f#k={k}"):
                arrived(wb.at[k, cc], f_rs.at[k])
        acc = jnp.zeros((H, 2 * L), F32)
        for d in range(4):
            xs = xz[d - 1] if u >= 4 and d else xg[d]
            acc = acc + jnp.dot(xs, wb[k, cc, d], preferred_element_type=F32)
        part[u] = acc.astype(BF16)

    half = B // 2

    def start(u):
        _, axis, through = JOBS[u]
        if not through:
            for d in NEAR:
                to, at = along(axis, d)
                send(part.at[u, block_of(at)], rdir.at[u, d - 1], sum_rs.at[u], to)
            return
        far = along(axis, 2)[1]
        (up1, above), (dn1, below) = along(axis, 1), along(axis, 3)
        send(part.at[u, block_of(far, 0, half)], zr.at[u, 0], relay_rs.at[u, 0], up1)
        send(part.at[u, block_of(far, half, B)], zr.at[u, 1], relay_rs.at[u, 1], dn1)
        send(part.at[u, block_of(above, half, B)], rbuf.at[u, 0, half:], sum_rs.at[u], up1)
        send(part.at[u, block_of(below, 0, half)], rbuf.at[u, 1, :half], sum_rs.at[u], dn1)

    def add(u):
        _, axis, _ = JOBS[u]
        for side, d, a, b in ((0, 1, 0, half), (1, 3, half, B)):
            to, at = along(axis, d)
            with scope(f"wait_relay#u={u}"):
                arrived(zr.at[u, side], relay_rs.at[u, side])
            zs[u, side] = (part[u, block_of(at, a, b), :].astype(F32) + zr[u, side].astype(F32)).astype(BF16)
            send(zs.at[u, side], rbuf.at[u, side, a:b], sum_rs.at[u], to)

    def core_of(u):
        return lax.rem(c + u % 2, 2)

    def finish(u):
        _, axis, through = JOBS[u]
        came = rbuf if through else rdir
        with scope(f"wait_sum#u={u}"):
            arrived(came.at[u], sum_rs.at[u])
        total = part[u, block_of(along(axis, 0)[1]), :].astype(F32)
        for d in range(2 if through else 3):
            total = total + came[u, d].astype(F32)
        scale = inv if axis == "z" else inv_y
        gate, up = total[:, :L] * scale, total[:, L:] * scale
        hid = gate / (1.0 + jnp.exp(-gate)) * up
        if u < 2:
            hid = jnp.where(y == 3, jnp.zeros_like(hid), hid)
        if axis == "z":
            lanes = pl.ds(pl.multiple_of((u // 2 * 2 + core_of(u)) * L, L), L)
            hall[z, :, lanes] = hid.astype(BF16)
            block = hall.at[z, :, lanes]
        else:
            lanes = pl.ds(pl.multiple_of(core_of(u) * L, L), L)
            hz[z, :, lanes] = hid.astype(BF16)
            block = hz.at[z, :, lanes]
        for d in NEAR:
            send(block, block, h_rs.at[u // 4], dev(dz=d))

    columns_of(0)
    with scope("wait_xc"):
        arrived(xg.at[1:, : 3 * R], xc_rs)
    multiply(0)
    start(0)
    with scope("wait_sq2"):
        arrived(sq2_r, q_rs.at[1])
        arrived(sq3_r, q_rs.at[2])
    inv = as_columns(lax.rsqrt((st2_s[z] + sq2_r[0] + sq2_r[1] + sq2_r[2]) / D + EPS))
    inv_y = as_columns(lax.rsqrt((st2_s[y] + sq3_r[0] + sq3_r[1] + sq3_r[2]) / D + EPS))
    multiply(1)
    start(1)
    columns_of(2)
    with scope("wait_xz2"):
        arrived(xz.at[1], xz_rs.at[1])
    multiply(4)
    start(4)
    multiply(5)
    start(5)
    for d in NEAR:
        send(wd.at[pl.ds(tile0(mod4(y + d)), K)], wdb.at[y, :, c], d_rs.at[d - 1], dev(dy=d))
    columns_of(1)
    multiply(2)
    start(2)
    finish(0)
    multiply(3)
    start(3)
    finish(1)
    add(2)
    finish(4)
    add(3)
    finish(5)
    finish(2)
    finish(3)
    with scope("wait_hz"):
        arrived(hz.at[:3], h_rs.at[1])
    last = slice(4 * L, 6 * L)
    for i, (r0, r1) in enumerate(HALVES):
        for d in NEAR:
            send(hz.at[mod4(y + d), r0:r1], hall.at[y, r0:r1, last], hy_rs.at[i], dev(dy=d))
    hall[y, :, last] = hz[y]
    with scope("wait_d"):
        for d in (0, 1, 3, 2):
            if d:
                arrived(wdb.at[0, :, c], d_rs.at[d - 1])
            else:
                local_d.wait()
            block = wdb.at[mod4(y - d), :, c]
            send(block, block, df_rs, dev(dc=1))
    with scope("wait_df"):
        arrived(wdb.at[:, :, c], df_rs)

    with scope("wait_h"):
        arrived(hall.at[:3, :, : 4 * L], h_rs.at[0])
    for yy in range(4):
        w = wdb[yy, :2].reshape(4 * L, W)
        begun[yy] = jnp.dot(hall[:, :, : 4 * L].reshape(H, 4 * L), w, preferred_element_type=F32).reshape(4, B, W)
    for i, (r0, r1) in enumerate(HALVES):
        with scope(f"wait_hy#i={i}"):
            arrived(hall.at[:3, r0:r1, last], hy_rs.at[i])
        mid = (r0 + r1) // 2
        a, b = slice(r0, mid), slice(mid, r1)
        for dy in (2, 1, 3, 0):
            yy = mod4(y + dy)
            hid = hall[:, r0:r1, 4 * L :].reshape(4 * (r1 - r0), 2 * L)
            acc = jnp.dot(hid, wdb[yy, 2].reshape(2 * L, W), preferred_element_type=F32)
            psend[yy, :, r0:r1] = (begun[yy, :, r0:r1] + acc.reshape(4, r1 - r0, W)).astype(BF16)
            if dy:
                send(psend.at[yy, :, a], p1.at[dy - 1, :, a], p_rs.at[i, 0], dev(dy=dy))
            for dx in NEAR:
                send(psend.at[yy, mod4(x + dx), b], p2.at[dx - 1, yy, b], p_rs.at[i, 1], dev(dx=dx))
    for i, (r0, r1) in enumerate(HALVES):
        mid = (r0 + r1) // 2
        a, b = slice(r0, mid), slice(mid, r1)
        with scope(f"wait_p1#i={i}"):
            arrived(p1.at[:, :, a], p_rs.at[i, 0])
        for xx in range(4):
            v = psend[y, xx, a].astype(F32)
            for d in range(3):
                v = v + p1[d, xx, a].astype(F32)
            s1[xx, a] = v.astype(BF16)
        for d in NEAR:
            send(s1.at[mod4(x + d), a], p3.at[d - 1, a], p_rs.at[i, 2], dev(dx=d))
        with scope(f"wait_p2#i={i}"):
            arrived(p2.at[:, :, b], p_rs.at[i, 1])
        for yy in range(4):
            v = psend[yy, x, b].astype(F32)
            for d in range(3):
                v = v + p2[d, yy, b].astype(F32)
            s2[yy, b] = v.astype(BF16)
        for d in NEAR:
            send(s2.at[mod4(y + d), b], p4.at[d - 1, b], p_rs.at[i, 3], dev(dy=d))
    pieces = []
    for i, (r0, r1) in enumerate(HALVES):
        mid = (r0 + r1) // 2
        a, b = slice(r0, mid), slice(mid, r1)
        with scope(f"wait_p3#i={i}"):
            arrived(p3.at[:, a], p_rs.at[i, 2])
        v1 = s1[x, a].astype(F32)
        for d in range(3):
            v1 = v1 + p3[d, a].astype(F32)
        with scope(f"wait_p4#i={i}"):
            arrived(p4.at[:, b], p_rs.at[i, 3])
        v2 = s2[y, b].astype(F32)
        for d in range(3):
            v2 = v2 + p4[d, b].astype(F32)
        piece = rows(c * H + x * B + r0, r1 - r0)
        pieces.append(0.5 * tok[piece, :].astype(F32) + jnp.concatenate([v1, v2], axis=0))
        out[piece, :] = pieces[i].astype(BF16)
        if i == 0:
            for d in NEAR:
                send(out.at[piece, :], out.at[piece, :], o_rs.at[i, d - 1], dev(dx=d))
    stream = jnp.concatenate(pieces, axis=0)
    mine = 2 * x + c
    st_all[mine, 0] = row_sums(stream)
    for dz, f, d, e in EVERYONE:
        send(st_all.at[mine, 0], st_all.at[mine, 4 * dz + f], t_rs, dev(dz=dz, dy=f, dx=d, dc=e))
    for d in NEAR:
        send(out.at[piece, :], out.at[piece, :], o_rs.at[1, d - 1], dev(dx=d))
    for i, (r0, r1) in enumerate(HALVES):
        with scope(f"wait_o#i={i}"):
            for d in (0, 1, 3, 2):
                block = out.at[rows(c * H + mod4(x - d) * B + r0, r1 - r0), :]
                if d:
                    arrived(block, o_rs.at[i, d - 1])
                send(block, block, of_rs, dev(dc=1))
    with scope("wait_of"):
        arrived(out.at[:H], of_rs)
    with scope("wait_st2"):
        arrived(sq_n.at[: len(EVERYONE)], t_rs)
    with scope("wait_sends"):
        for s in sends:
            s.wait_send()
    for xx in range(4):
        for cc in range(2):
            total = jnp.sum(st_all[2 * xx + cc], axis=0)
            factor = as_columns(lax.rsqrt(total / D + EPS))
            r = slice(cc * H + xx * B, cc * H + (xx + 1) * B)
            for h in range(2):
                lanes = slice(h * L, (h + 1) * L)
                out[r, lanes] = (out[r, lanes].astype(F32) * factor * ogain[:, lanes]).astype(BF16)


def body(tokens, norm_gain, gate_weight, up_weight, down_weight, out_gain):
    dma = pltpu.SemaphoreType.DMA
    hbm = pl.BlockSpec(memory_space=pltpu.HBM)
    operands = (
        tokens,
        norm_gain.reshape(1, W),
        gate_weight,
        up_weight,
        down_weight.reshape(11, L, W),
        out_gain.reshape(1, W),
    )
    return pl.pallas_call(
        kernel,
        out_shape=jax.ShapeDtypeStruct((T, W), BF16),
        in_specs=[hbm] * 6,
        out_specs=pl.BlockSpec(memory_space=pltpu.VMEM),
        scratch_shapes=[
            pltpu.VMEM((T, W), BF16),
            pltpu.VMEM((1, W), F32),
            pltpu.VMEM((W, 11 * L), BF16),
            pltpu.VMEM((W, 11 * L), BF16),
            pltpu.VMEM((11, L, W), BF16),
            pltpu.VMEM((1, W), F32),
            pltpu.VMEM((4, H, W), BF16),
            pltpu.VMEM((3, H, W), BF16),
            pltpu.VMEM((K, 2, 4, W, 2 * L), BF16),
            pltpu.VMEM((4, K, 2, L, W), BF16),
            pltpu.VMEM((2 * K, H, 2 * L), BF16),
            pltpu.VMEM((2 * K, 2, B // 2, 2 * L), BF16),
            pltpu.VMEM((2 * K, 2, B // 2, 2 * L), BF16),
            pltpu.VMEM((2 * K, 2, B, 2 * L), BF16),
            pltpu.VMEM((2 * K, 3, B, 2 * L), BF16),
            pltpu.VMEM((4, B, 2 * K * L), BF16),
            pltpu.VMEM((4, B, 2 * L), BF16),
            pltpu.VMEM((4, 4, B, W), F32),
            pltpu.VMEM((4, 4, B, W), BF16),
            pltpu.VMEM((3, 4, B, W), BF16),
            pltpu.VMEM((3, 4, B, W), BF16),
            pltpu.VMEM((4, B, W), BF16),
            pltpu.VMEM((4, B, W), BF16),
            pltpu.VMEM((3, B, W), BF16),
            pltpu.VMEM((3, B, W), BF16),
            pltpu.VMEM((4, 1, L), F32),
            pltpu.VMEM((3, 4, 1, L), F32),
            pltpu.VMEM((3, 1, L), F32),
            pltpu.VMEM((3, 1, L), F32),
            pltpu.VMEM((4, 1, L), F32),
            pltpu.VMEM((8, 16, 1, L), F32),
            pltpu.VMEM((128, 1, L), F32),
            dma,
            dma((6,)),
            dma((K + 1,)),
            dma((3,)), dma, dma, dma((3,)),
            dma((K, 3)), dma((K,)), dma((3,)), dma,
            dma((len(JOBS), 2)), dma((len(JOBS),)),
            dma((2,)), dma((2,)),
            dma((2, 4)), dma((3,)), dma,
            dma((2, 3)), dma,
        ],
        compiler_params=pltpu.CompilerParams(
            collective_id=0, has_side_effects=True, vmem_limit_bytes=40 * 1024 * 1024
        ),
    )(*[pltpu.with_memory_space_constraint(a, pltpu.HBM) for a in operands])


def solution(mesh):
    placed = (P(None, "ra"), P("ra"), P("ra", "cb"), P("ra", "cb"), P("cb", "ra"), P("ra"))
    return jax.shard_map(body, mesh=mesh, in_specs=placed, out_specs=P(None, "ra"), check_vma=False)
```

```python
import functools

import jax
import jax.numpy as jnp
from jax import lax
from jax.experimental import pallas as pl
from jax.experimental.pallas import tpu as pltpu
from jax.sharding import PartitionSpec as P

D = 4096
EPS = 1e-06
MESH = pl.DeviceIdType.MESH
scope = jax.named_scope
F32 = jnp.float32
BF16 = jnp.bfloat16
T = 1024
H = 512
B = 128
W = 256
L = 128
K = 3

R = 112

S0 = 64
HALVES = ((0, S0), (S0, B))

JOBS = ((0, "z", True), (1, "z", True), (2, "z", True), (3, "z", True), (4, "y", False), (5, "y", False))

PASSED = 2

NEAR = (2, 1, 3)
EVERYONE = [(g, f, d, e) for g in range(4) for f in range(4) for d in range(4) for e in range(2)][1:]
EVERYONE.sort(key=lambda s: -sum(min(v, 4 - v) for v in s[:3]))


def mod4(v):
    return lax.rem(v + 4, 4)


def row_sums(v):
    sq = v * v
    hi = sq.astype(BF16)
    lo = (sq - hi.astype(F32)).astype(BF16)
    ones = jnp.ones((8, v.shape[1]), BF16)
    dims = (((1,), (1,)), ((), ()))
    out = lax.dot_general(ones, hi, dims, preferred_element_type=F32)
    return (out + lax.dot_general(ones, lo, dims, preferred_element_type=F32))[:1]


def as_columns(row):
    return jnp.transpose(jnp.broadcast_to(row, (L, L)), (1, 0))


def kernel(
    tok_h, gain_h, wg_h, wu_h, wd_h, ogain_h, out,
    tok, gain, wg, wu, wd, ogain, xg, xz, wb, wdb, part, zr, zs, rbuf, rdir, hall, hz, begun, psend, p1, p2, s1, s2, p3, p4,
    sq_s, sq_r, sq2_r, sq3_r, st2_s, st_all, sq_n,
    sent, head, loc, xa_rs, xb_rs, xc_rs, xz_rs, w_rs, f_rs, d_rs, df_rs, relay_rs, sum_rs, shown_rs, h_rs, hy_rs,
    p_rs, q_rs, t_rs, o_rs, of_rs,
):
    ra, cb = lax.axis_index("ra"), lax.axis_index("cb")
    z, y, x, c = ra // 4, lax.rem(ra, 4), cb // 2, lax.rem(cb, 2)

    def dev(dz=0, dy=0, dx=0, dc=0):
        return (mod4(z + dz) * 4 + mod4(y + dy), mod4(x + dx) * 2 + lax.rem(c + dc, 2))

    def rows(start, size):
        return pl.ds(pl.multiple_of(start, 8), size)

    sends = []

    def send(src, dst, rs, to):
        cp = pltpu.make_async_remote_copy(
            src_ref=src, dst_ref=dst, send_sem=sent, recv_sem=rs, device_id=to, device_id_type=MESH
        )
        cp.start()
        sends.append(cp)
        return cp

    def arrived(ref, sem):
        pltpu.make_async_copy(ref, ref, sem).wait()

    def local(src, dst, sem):
        cp = pltpu.make_async_copy(src, dst, sem)
        cp.start()
        return cp

    partners = [dev(dz=d) for d in NEAR] + [dev(dy=d) for d in NEAR] + [dev(dx=d) for d in NEAR] + [dev(dc=1)]
    bar = pltpu.get_barrier_semaphore()
    for p in partners:
        pl.semaphore_signal(bar, inc=1, device_id=p, device_id_type=MESH)

    mine = rows(c * H, H)
    first = [local(tok_h.at[mine, :], tok, head.at[0]), local(gain_h, gain, head.at[1])]
    heads = [
        local(src, dst, head.at[2 + i]) for i, (src, dst) in enumerate(((wg_h, wg), (wu_h, wu), (wd_h, wd), (ogain_h, ogain)))
    ]

    def tile0(yy):
        return jnp.minimum(3 * yy, 8)

    def cols(yy, k):
        return pl.ds(pl.multiple_of((tile0(yy) + k) * L, L), L)

    for k in range(K):
        own = cols(y if k < 2 else z, k)
        local(wg_h.at[:, own], wb.at[k, c, 0, :, :L], loc.at[k])
        local(wu_h.at[:, own], wb.at[k, c, 0, :, L:], loc.at[k])
    local_d = local(wd_h.at[pl.ds(tile0(y), K)], wdb.at[y, :, c], loc.at[K])

    for h in first:
        h.wait()
    xg[0] = (tok[...].astype(F32) * gain[...]).astype(BF16)
    with scope("barrier"):
        pl.semaphore_wait(bar, len(partners))

    quarter = rows(x * R, R)
    for d in NEAR:
        send(xg.at[0, quarter], xg.at[d, quarter], xa_rs.at[d - 1], dev(dy=d))
    for d in (1, 3):
        send(xg.at[0, 4 * R :], xg.at[d, 4 * R :], xb_rs.at[d - 1], dev(dy=d))
    near_z = {d: send(xg.at[0], xz.at[d - 1], xz_rs.at[d - 1], dev(dz=d)) for d in (1, 3)}
    for h in heads:
        h.wait()

    def send_columns(k):
        for d in NEAR:
            own, to = (mod4(y + d), dev(dy=d)) if k < 2 else (mod4(z + d), dev(dz=d))
            send(wg.at[:, cols(own, k)], wb.at[k, c, d, :, :L], w_rs.at[k, d - 1], to)
            send(wu.at[:, cols(own, k)], wb.at[k, c, d, :, L:], w_rs.at[k, d - 1], to)

    send_columns(0)
    send_columns(2)
    sq = row_sums(tok[...].astype(F32))
    for b in range(4):
        sq_s[b] = sq[:, b * L : (b + 1) * L]
    for d in NEAR:
        send(sq_s, sq_r.at[d - 1], q_rs.at[0], dev(dy=d))
    for d in (1, 3, 2):
        with scope(f"wait_xa#d={d}"):
            arrived(xg.at[d, quarter], xa_rs.at[d - 1])
        for e in NEAR:
            send(xg.at[d, quarter], xg.at[d, quarter], xc_rs, dev(dx=e))
    cut = 4 * R + (H - 4 * R) // 2
    for d, part_of in ((1, slice(4 * R, cut)), (3, slice(cut, H))):
        with scope(f"wait_xb#d={d}"):
            arrived(xg.at[d, 4 * R :], xb_rs.at[d - 1])
        send(xg.at[d, part_of], xg.at[2, part_of], xb_rs.at[1], dev(dy=d))
    send_columns(1)

    def send_rows(d, k0, k1):
        tiles = pl.ds(tile0(mod4(y + d)) + k0, k1 - k0)
        send(wd.at[tiles], wdb.at[y, k0:k1, c], d_rs.at[d - 1], dev(dy=d))

    for d in (1, 3):
        send_rows(d, 0, 1)
    with scope("wait_xz"):
        for d, half in ((1, slice(0, H // 2)), (3, slice(H // 2, H))):
            near_z[d].wait_recv()
            send(xz.at[d - 1, half], xz.at[1, half], xz_rs.at[1], dev(dz=d))
    def columns_of(k):
        with scope(f"wait_w#k={k}"):
            for d in NEAR:
                arrived(wb.at[k, c, d], w_rs.at[k, d - 1])
                send(wb.at[k, c, d], wb.at[k, c, d], f_rs.at[k], dev(dc=1))

    def along(axis, d):
        return (dev(dz=d), mod4(z + d)) if axis == "z" else (dev(dy=d), mod4(y + d))

    def block_of(at, r0=0, r1=B):
        return rows(at * B + r0, r1 - r0)

    def multiply(u):
        k, cc = u // 2, lax.rem(c + u % 2, 2)
        if u % 2:
            with scope(f"wait_f#k={k}"):
                arrived(wb.at[k, cc], f_rs.at[k])
        acc = jnp.zeros((H, 2 * L), F32)
        for d in range(4):
            xs = xz[d - 1] if u >= 4 and d else xg[d]
            acc = acc + jnp.dot(xs, wb[k, cc, d], preferred_element_type=F32)
        part[u] = acc.astype(BF16)

    half = B // 2

    def start(u):
        _, axis, through = JOBS[u]
        if not through:
            for d in NEAR:
                to, at = along(axis, d)
                send(part.at[u, block_of(at)], rdir.at[u, d - 1], sum_rs.at[u], to)
            return
        far = along(axis, 2)[1]
        (up1, above), (dn1, below) = along(axis, 1), along(axis, 3)
        send(part.at[u, block_of(far, 0, half)], zr.at[u, 0], relay_rs.at[u, 0], up1)
        send(part.at[u, block_of(far, half, B)], zr.at[u, 1], relay_rs.at[u, 1], dn1)
        send(part.at[u, block_of(above, half, B)], rbuf.at[u, 0, half:], sum_rs.at[u], up1)
        send(part.at[u, block_of(below, 0, half)], rbuf.at[u, 1, :half], sum_rs.at[u], dn1)

    def add(u):
        _, axis, _ = JOBS[u]
        for side, d, a, b in ((0, 1, 0, half), (1, 3, half, B)):
            to, at = along(axis, d)
            with scope(f"wait_relay#u={u}"):
                arrived(zr.at[u, side], relay_rs.at[u, side])
            zs[u, side] = (part[u, block_of(at, a, b), :].astype(F32) + zr[u, side].astype(F32)).astype(BF16)
            send(zs.at[u, side], rbuf.at[u, side, a:b], sum_rs.at[u], to)

    def core_of(u):
        return lax.rem(c + u % 2, 2)

    def finish(u):
        _, axis, through = JOBS[u]
        came = rbuf if through else rdir
        with scope(f"wait_sum#u={u}"):
            arrived(came.at[u], sum_rs.at[u])
        total = part[u, block_of(along(axis, 0)[1]), :].astype(F32)
        for d in range(2 if through else 3):
            total = total + came[u, d].astype(F32)
        scale = inv if axis == "z" else inv_y
        gate, up = total[:, :L] * scale, total[:, L:] * scale
        hid = gate / (1.0 + jnp.exp(-gate)) * up
        if u < 2:
            hid = jnp.where(y == 3, jnp.zeros_like(hid), hid)
        if axis == "z":
            lanes = pl.ds(pl.multiple_of((u // 2 * 2 + core_of(u)) * L, L), L)
            hall[z, :, lanes] = hid.astype(BF16)
            block = hall.at[z, :, lanes]
        else:
            lanes = pl.ds(pl.multiple_of(core_of(u) * L, L), L)
            hz[z, :, lanes] = hid.astype(BF16)
            block = hz.at[z, :, lanes]
        if u < PASSED:
            send(block, block, shown_rs.at[u, 0], dev(dz=1))
            send(block, block, shown_rs.at[u, 1], dev(dz=3))
            return
        for d in NEAR:
            send(block, block, h_rs.at[u // 4], dev(dz=d))

    def pass_on(u):
        lanes = pl.ds(pl.multiple_of((u // 2 * 2 + core_of(u)) * L, L), L)
        for side, to, dz, a, b in ((0, 1, 3, 0, half), (1, 3, 1, half, B)):
            with scope(f"wait_shown#u={u}"):
                arrived(hall.at[mod4(z + dz), :, lanes], shown_rs.at[u, side])
            block = hall.at[mod4(z + dz), a:b, lanes]
            send(block, block, h_rs.at[0], dev(dz=to))

    for k in range(K):
        arrived(wb.at[k, c, 0], loc.at[k])
        send(wb.at[k, c, 0], wb.at[k, c, 0], f_rs.at[k], dev(dc=1))
    local_d.wait()
    send(wdb.at[y, :, c], wdb.at[y, :, c], df_rs, dev(dc=1))
    columns_of(0)
    with scope("wait_xc"):
        arrived(xg.at[1:, : 3 * R], xc_rs)
    with scope("wait_xb2"):
        arrived(xg.at[2, 4 * R :], xb_rs.at[1])
    multiply(0)
    start(0)
    columns_of(2)
    with scope("wait_sq"):
        arrived(sq_r, q_rs.at[0])
    for b in range(4):
        st2_s[b] = sq_s[b] + sq_r[0, b] + sq_r[1, b] + sq_r[2, b]
    for d in NEAR:
        send(st2_s.at[mod4(z + d)], sq2_r.at[d - 1], q_rs.at[1], dev(dz=d))
        send(st2_s.at[y], sq3_r.at[d - 1], q_rs.at[2], dev(dz=d))
    multiply(1)
    start(1)
    with scope("wait_xz2"):
        arrived(xz.at[1], xz_rs.at[1])
    multiply(4)
    start(4)
    multiply(5)
    start(5)
    for d in NEAR:
        send_rows(d, 0 if d == 2 else 1, K)
    add(0)
    columns_of(1)
    add(1)
    multiply(2)
    start(2)
    multiply(3)
    start(3)
    with scope("wait_sq2"):
        arrived(sq2_r, q_rs.at[1])
        arrived(sq3_r, q_rs.at[2])
    inv = as_columns(lax.rsqrt((st2_s[z] + sq2_r[0] + sq2_r[1] + sq2_r[2]) / D + EPS))
    inv_y = as_columns(lax.rsqrt((st2_s[y] + sq3_r[0] + sq3_r[1] + sq3_r[2]) / D + EPS))
    finish(0)
    finish(1)
    add(2)
    finish(4)
    add(3)
    finish(5)
    finish(2)
    pass_on(0)
    pass_on(1)
    with scope("wait_d2"):
        arrived(wdb.at[0, :, c], d_rs.at[1])
        send(wdb.at[mod4(y - 2), :, c], wdb.at[mod4(y - 2), :, c], df_rs, dev(dc=1))
    finish(3)
    with scope("wait_hz"):
        arrived(hz.at[:3], h_rs.at[1])
    last = slice(4 * L, 6 * L)
    for i, (r0, r1) in enumerate(HALVES):
        for d in NEAR:
            send(hz.at[mod4(y + d), r0:r1], hall.at[y, r0:r1, last], hy_rs.at[i], dev(dy=d))
    hall[y, :, last] = hz[y]
    with scope("wait_d"):
        for d in (1, 3):
            arrived(wdb.at[0, :, c], d_rs.at[d - 1])
            block = wdb.at[mod4(y - d), :, c]
            send(block, block, df_rs, dev(dc=1))
    with scope("wait_df"):
        arrived(wdb.at[:, :, c], df_rs)

    with scope("wait_h"):
        arrived(hall.at[:2, :, : 4 * L], h_rs.at[0])
    for yy in range(4):
        w = wdb[yy, :2].reshape(4 * L, W)
        begun[yy] = jnp.dot(hall[:, :, : 4 * L].reshape(H, 4 * L), w, preferred_element_type=F32).reshape(4, B, W)
    for i, (r0, r1) in enumerate(HALVES):
        with scope(f"wait_hy#i={i}"):
            arrived(hall.at[:3, r0:r1, last], hy_rs.at[i])
        mid = (r0 + r1) // 2
        a, b = slice(r0, mid), slice(mid, r1)
        for dy in (2, 1, 3, 0):
            yy = mod4(y + dy)
            hid = hall[:, r0:r1, 4 * L :].reshape(4 * (r1 - r0), 2 * L)
            acc = jnp.dot(hid, wdb[yy, 2].reshape(2 * L, W), preferred_element_type=F32)
            psend[yy, :, r0:r1] = (begun[yy, :, r0:r1] + acc.reshape(4, r1 - r0, W)).astype(BF16)
            if dy:
                send(psend.at[yy, :, a], p1.at[dy - 1, :, a], p_rs.at[i, 0], dev(dy=dy))
            for dx in NEAR:
                send(psend.at[yy, mod4(x + dx), b], p2.at[dx - 1, yy, b], p_rs.at[i, 1], dev(dx=dx))
    for i, (r0, r1) in enumerate(HALVES):
        mid = (r0 + r1) // 2
        a, b = slice(r0, mid), slice(mid, r1)
        with scope(f"wait_p1#i={i}"):
            arrived(p1.at[:, :, a], p_rs.at[i, 0])
        for xx in range(4):
            v = psend[y, xx, a].astype(F32)
            for d in range(3):
                v = v + p1[d, xx, a].astype(F32)
            s1[xx, a] = v.astype(BF16)
        for d in NEAR:
            send(s1.at[mod4(x + d), a], p3.at[d - 1, a], p_rs.at[i, 2], dev(dx=d))
        with scope(f"wait_p2#i={i}"):
            arrived(p2.at[:, :, b], p_rs.at[i, 1])
        for yy in range(4):
            v = psend[yy, x, b].astype(F32)
            for d in range(3):
                v = v + p2[d, yy, b].astype(F32)
            s2[yy, b] = v.astype(BF16)
        for d in NEAR:
            send(s2.at[mod4(y + d), b], p4.at[d - 1, b], p_rs.at[i, 3], dev(dy=d))
    pieces = []
    for i, (r0, r1) in enumerate(HALVES):
        mid = (r0 + r1) // 2
        a, b = slice(r0, mid), slice(mid, r1)
        with scope(f"wait_p3#i={i}"):
            arrived(p3.at[:, a], p_rs.at[i, 2])
        v1 = s1[x, a].astype(F32)
        for d in range(3):
            v1 = v1 + p3[d, a].astype(F32)
        with scope(f"wait_p4#i={i}"):
            arrived(p4.at[:, b], p_rs.at[i, 3])
        v2 = s2[y, b].astype(F32)
        for d in range(3):
            v2 = v2 + p4[d, b].astype(F32)
        piece = rows(c * H + x * B + r0, r1 - r0)
        pieces.append(0.5 * tok[rows(x * B + r0, r1 - r0), :].astype(F32) + jnp.concatenate([v1, v2], axis=0))
        out[piece, :] = pieces[i].astype(BF16)
        if i == 0:
            for d in NEAR:
                send(out.at[piece, :], out.at[piece, :], o_rs.at[i, d - 1], dev(dx=d))
    stream = jnp.concatenate(pieces, axis=0)
    mine = 2 * x + c
    st_all[mine, 0] = row_sums(stream)
    for dz, f, d, e in EVERYONE:
        send(st_all.at[mine, 0], st_all.at[mine, 4 * dz + f], t_rs, dev(dz=dz, dy=f, dx=d, dc=e))
    for d in NEAR:
        send(out.at[piece, :], out.at[piece, :], o_rs.at[1, d - 1], dev(dx=d))
    for i, (r0, r1) in enumerate(HALVES):
        with scope(f"wait_o#i={i}"):
            for d in (0, 1, 3, 2):
                block = out.at[rows(c * H + mod4(x - d) * B + r0, r1 - r0), :]
                if d:
                    arrived(block, o_rs.at[i, d - 1])
                send(block, block, of_rs, dev(dc=1))
    with scope("wait_of"):
        arrived(out.at[:H], of_rs)
    with scope("wait_st2"):
        arrived(sq_n.at[: len(EVERYONE)], t_rs)
    with scope("wait_sends"):
        for s in sends:
            s.wait_send()
    for xx in range(4):
        for cc in range(2):
            total = jnp.sum(st_all[2 * xx + cc], axis=0)
            factor = as_columns(lax.rsqrt(total / D + EPS))
            r = slice(cc * H + xx * B, cc * H + (xx + 1) * B)
            for h in range(2):
                lanes = slice(h * L, (h + 1) * L)
                out[r, lanes] = (out[r, lanes].astype(F32) * factor * ogain[:, lanes]).astype(BF16)


def body(tokens, norm_gain, gate_weight, up_weight, down_weight, out_gain):
    dma = pltpu.SemaphoreType.DMA
    hbm = pl.BlockSpec(memory_space=pltpu.HBM)
    operands = (
        tokens,
        norm_gain.reshape(1, W),
        gate_weight,
        up_weight,
        down_weight.reshape(11, L, W),
        out_gain.reshape(1, W),
    )
    return pl.pallas_call(
        kernel,
        out_shape=jax.ShapeDtypeStruct((T, W), BF16),
        in_specs=[hbm] * 6,
        out_specs=pl.BlockSpec(memory_space=pltpu.VMEM),
        scratch_shapes=[
            pltpu.VMEM((H, W), BF16),
            pltpu.VMEM((1, W), F32),
            pltpu.VMEM((W, 11 * L), BF16),
            pltpu.VMEM((W, 11 * L), BF16),
            pltpu.VMEM((11, L, W), BF16),
            pltpu.VMEM((1, W), F32),
            pltpu.VMEM((4, H, W), BF16),
            pltpu.VMEM((3, H, W), BF16),
            pltpu.VMEM((K, 2, 4, W, 2 * L), BF16),
            pltpu.VMEM((4, K, 2, L, W), BF16),
            pltpu.VMEM((2 * K, H, 2 * L), BF16),
            pltpu.VMEM((2 * K, 2, B // 2, 2 * L), BF16),
            pltpu.VMEM((2 * K, 2, B // 2, 2 * L), BF16),
            pltpu.VMEM((2 * K, 2, B, 2 * L), BF16),
            pltpu.VMEM((2 * K, 3, B, 2 * L), BF16),
            pltpu.VMEM((4, B, 2 * K * L), BF16),
            pltpu.VMEM((4, B, 2 * L), BF16),
            pltpu.VMEM((4, 4, B, W), F32),
            pltpu.VMEM((4, 4, B, W), BF16),
            pltpu.VMEM((3, 4, B, W), BF16),
            pltpu.VMEM((3, 4, B, W), BF16),
            pltpu.VMEM((4, B, W), BF16),
            pltpu.VMEM((4, B, W), BF16),
            pltpu.VMEM((3, B, W), BF16),
            pltpu.VMEM((3, B, W), BF16),
            pltpu.VMEM((4, 1, L), F32),
            pltpu.VMEM((3, 4, 1, L), F32),
            pltpu.VMEM((3, 1, L), F32),
            pltpu.VMEM((3, 1, L), F32),
            pltpu.VMEM((4, 1, L), F32),
            pltpu.VMEM((8, 16, 1, L), F32),
            pltpu.VMEM((128, 1, L), F32),
            dma,
            dma((6,)),
            dma((K + 1,)),
            dma((3,)), dma((3,)), dma, dma((3,)),
            dma((K, 3)), dma((K,)), dma((3,)), dma,
            dma((len(JOBS), 2)), dma((len(JOBS),)),
            dma((PASSED, 2)), dma((2,)), dma((2,)),
            dma((2, 4)), dma((3,)), dma,
            dma((2, 3)), dma,
        ],
        compiler_params=pltpu.CompilerParams(
            collective_id=0, has_side_effects=True, vmem_limit_bytes=40 * 1024 * 1024
        ),
    )(*[pltpu.with_memory_space_constraint(a, pltpu.HBM) for a in operands])


def solution(mesh):
    placed = (P(None, "ra"), P("ra"), P("ra", "cb"), P("ra", "cb"), P("cb", "ra"), P("ra"))
    return jax.shard_map(body, mesh=mesh, in_specs=placed, out_specs=P(None, "ra"), check_vma=False)
```

```python
import functools

import jax
import jax.numpy as jnp
from jax import lax
from jax.experimental import pallas as pl
from jax.experimental.pallas import tpu as pltpu
from jax.sharding import PartitionSpec as P

D = 4096
EPS = 1e-06
MESH = pl.DeviceIdType.MESH
scope = jax.named_scope
F32 = jnp.float32
BF16 = jnp.bfloat16
T = 1024
H = 512
B = 128
W = 256
L = 128
K = 3

R = 112
RZ = 32

S0 = 64
HALVES = ((0, S0), (S0, B))

JOBS = ((0, "z", True), (1, "z", True), (2, "z", True), (3, "z", True), (4, "y", False), (5, "y", False))

PASSED = 2

NEAR = (2, 1, 3)
EVERYONE = [(g, f, d, e) for g in range(4) for f in range(4) for d in range(4) for e in range(2)][1:]
EVERYONE.sort(key=lambda s: -sum(min(v, 4 - v) for v in s[:3]))


def mod4(v):
    return lax.rem(v + 4, 4)


def row_sums(v):
    sq = v * v
    hi = sq.astype(BF16)
    lo = (sq - hi.astype(F32)).astype(BF16)
    ones = jnp.ones((8, v.shape[1]), BF16)
    dims = (((1,), (1,)), ((), ()))
    out = lax.dot_general(ones, hi, dims, preferred_element_type=F32)
    return (out + lax.dot_general(ones, lo, dims, preferred_element_type=F32))[:1]


def as_columns(row):
    return jnp.transpose(jnp.broadcast_to(row, (L, L)), (1, 0))


def kernel(
    tok_h, gain_h, wg_h, wu_h, wd_h, ogain_h, out,
    tok, gain, wg, wu, wd, ogain, xg, xz, wb, wdb, part, zr, zs, rbuf, rdir, hall, hz, begun, psend, p1, p2, s1, s2, p3, p4,
    sq_s, sq_r, sq2_r, sq3_r, st2_s, st_all, sq_n,
    sent, head, loc, xa_rs, xb_rs, xc_rs, xz_rs, xza_rs, xzc_rs, w_rs, f_rs, d_rs, df_rs, relay_rs, sum_rs, shown_rs, h_rs, hy_rs,
    p_rs, q_rs, t_rs, o_rs, of_rs,
):
    ra, cb = lax.axis_index("ra"), lax.axis_index("cb")
    z, y, x, c = ra // 4, lax.rem(ra, 4), cb // 2, lax.rem(cb, 2)

    def dev(dz=0, dy=0, dx=0, dc=0):
        return (mod4(z + dz) * 4 + mod4(y + dy), mod4(x + dx) * 2 + lax.rem(c + dc, 2))

    def rows(start, size):
        return pl.ds(pl.multiple_of(start, 8), size)

    sends = []

    def send(src, dst, rs, to):
        cp = pltpu.make_async_remote_copy(
            src_ref=src, dst_ref=dst, send_sem=sent, recv_sem=rs, device_id=to, device_id_type=MESH
        )
        cp.start()
        sends.append(cp)
        return cp

    def arrived(ref, sem):
        pltpu.make_async_copy(ref, ref, sem).wait()

    def local(src, dst, sem):
        cp = pltpu.make_async_copy(src, dst, sem)
        cp.start()
        return cp

    partners = [dev(dz=d) for d in NEAR] + [dev(dy=d) for d in NEAR] + [dev(dx=d) for d in NEAR] + [dev(dc=1)]
    bar = pltpu.get_barrier_semaphore()
    for p in partners:
        pl.semaphore_signal(bar, inc=1, device_id=p, device_id_type=MESH)

    mine = rows(c * H, H)
    first = [local(tok_h.at[mine, :], tok, head.at[0]), local(gain_h, gain, head.at[1])]
    heads = [
        local(src, dst, head.at[2 + i]) for i, (src, dst) in enumerate(((wg_h, wg), (wu_h, wu), (wd_h, wd), (ogain_h, ogain)))
    ]

    def tile0(yy):
        return jnp.minimum(3 * yy, 8)

    def cols(yy, k):
        return pl.ds(pl.multiple_of((tile0(yy) + k) * L, L), L)

    for k in range(K):
        own = cols(y if k < 2 else z, k)
        local(wg_h.at[:, own], wb.at[k, c, 0, :, :L], loc.at[k])
        local(wu_h.at[:, own], wb.at[k, c, 0, :, L:], loc.at[k])
    local_d = local(wd_h.at[pl.ds(tile0(y), K)], wdb.at[y, :, c], loc.at[K])

    for h in first:
        h.wait()
    xg[0] = (tok[...].astype(F32) * gain[...]).astype(BF16)
    with scope("barrier"):
        pl.semaphore_wait(bar, len(partners))

    quarter = rows(x * R, R)
    for d in NEAR:
        send(xg.at[0, quarter], xg.at[d, quarter], xa_rs.at[d - 1], dev(dy=d))
    for d in (1, 3):
        send(xg.at[0, 4 * R :], xg.at[d, 4 * R :], xb_rs.at[d - 1], dev(dy=d))
    quarter_z = rows(x * RZ, RZ)
    for d in NEAR:
        send(xg.at[0, quarter_z], xz.at[d - 1, quarter_z], xza_rs.at[d - 1], dev(dz=d))
    near_z = {d: send(xg.at[0, 4 * RZ :], xz.at[d - 1, 4 * RZ :], xz_rs.at[d - 1], dev(dz=d)) for d in (1, 3)}
    for h in heads:
        h.wait()

    def send_columns(k):
        for d in NEAR:
            own, to = (mod4(y + d), dev(dy=d)) if k < 2 else (mod4(z + d), dev(dz=d))
            send(wg.at[:, cols(own, k)], wb.at[k, c, d, :, :L], w_rs.at[k, d - 1], to)
            send(wu.at[:, cols(own, k)], wb.at[k, c, d, :, L:], w_rs.at[k, d - 1], to)

    send_columns(0)
    send_columns(2)
    sq = row_sums(tok[...].astype(F32))
    for b in range(4):
        sq_s[b] = sq[:, b * L : (b + 1) * L]
    for d in NEAR:
        send(sq_s, sq_r.at[d - 1], q_rs.at[0], dev(dy=d))
    for d in (1, 3, 2):
        with scope(f"wait_xa#d={d}"):
            arrived(xg.at[d, quarter], xa_rs.at[d - 1])
        for e in NEAR:
            send(xg.at[d, quarter], xg.at[d, quarter], xc_rs, dev(dx=e))
    cut = 4 * R + (H - 4 * R) // 2
    for d, part_of in ((1, slice(4 * R, cut)), (3, slice(cut, H))):
        with scope(f"wait_xb#d={d}"):
            arrived(xg.at[d, 4 * R :], xb_rs.at[d - 1])
        send(xg.at[d, part_of], xg.at[2, part_of], xb_rs.at[1], dev(dy=d))
    send_columns(1)

    def send_rows(d, k0, k1):
        tiles = pl.ds(tile0(mod4(y + d)) + k0, k1 - k0)
        send(wd.at[tiles], wdb.at[y, k0:k1, c], d_rs.at[d - 1], dev(dy=d))

    with scope("wait_xza"):
        for d in (1, 3, 2):
            block = xz.at[d - 1, quarter_z]
            arrived(block, xza_rs.at[d - 1])
            for e in NEAR:
                send(block, block, xzc_rs, dev(dx=e))
    with scope("wait_xz"):
        for d, half in ((1, slice(4 * RZ, 2 * RZ + H // 2)), (3, slice(2 * RZ + H // 2, H))):
            near_z[d].wait_recv()
            send(xz.at[d - 1, half], xz.at[1, half], xz_rs.at[1], dev(dz=d))
    def columns_of(k):
        with scope(f"wait_w#k={k}"):
            for d in NEAR:
                arrived(wb.at[k, c, d], w_rs.at[k, d - 1])
                send(wb.at[k, c, d], wb.at[k, c, d], f_rs.at[k], dev(dc=1))

    def along(axis, d):
        return (dev(dz=d), mod4(z + d)) if axis == "z" else (dev(dy=d), mod4(y + d))

    def block_of(at, r0=0, r1=B):
        return rows(at * B + r0, r1 - r0)

    def multiply(u):
        k, cc = u // 2, lax.rem(c + u % 2, 2)
        if u % 2:
            with scope(f"wait_f#k={k}"):
                arrived(wb.at[k, cc], f_rs.at[k])
        acc = jnp.zeros((H, 2 * L), F32)
        for d in range(4):
            xs = xz[d - 1] if u >= 4 and d else xg[d]
            acc = acc + jnp.dot(xs, wb[k, cc, d], preferred_element_type=F32)
        part[u] = acc.astype(BF16)

    half = B // 2

    def start(u):
        _, axis, through = JOBS[u]
        if not through:
            for d in NEAR:
                to, at = along(axis, d)
                send(part.at[u, block_of(at)], rdir.at[u, d - 1], sum_rs.at[u], to)
            return
        far = along(axis, 2)[1]
        (up1, above), (dn1, below) = along(axis, 1), along(axis, 3)
        send(part.at[u, block_of(far, 0, half)], zr.at[u, 0], relay_rs.at[u, 0], up1)
        send(part.at[u, block_of(far, half, B)], zr.at[u, 1], relay_rs.at[u, 1], dn1)
        send(part.at[u, block_of(above, half, B)], rbuf.at[u, 0, half:], sum_rs.at[u], up1)
        send(part.at[u, block_of(below, 0, half)], rbuf.at[u, 1, :half], sum_rs.at[u], dn1)

    def add(u):
        _, axis, _ = JOBS[u]
        for side, d, a, b in ((0, 1, 0, half), (1, 3, half, B)):
            to, at = along(axis, d)
            with scope(f"wait_relay#u={u}"):
                arrived(zr.at[u, side], relay_rs.at[u, side])
            zs[u, side] = (part[u, block_of(at, a, b), :].astype(F32) + zr[u, side].astype(F32)).astype(BF16)
            send(zs.at[u, side], rbuf.at[u, side, a:b], sum_rs.at[u], to)

    def core_of(u):
        return lax.rem(c + u % 2, 2)

    def finish(u):
        _, axis, through = JOBS[u]
        came = rbuf if through else rdir
        with scope(f"wait_sum#u={u}"):
            arrived(came.at[u], sum_rs.at[u])
        total = part[u, block_of(along(axis, 0)[1]), :].astype(F32)
        for d in range(2 if through else 3):
            total = total + came[u, d].astype(F32)
        scale = inv if axis == "z" else inv_y
        gate, up = total[:, :L] * scale, total[:, L:] * scale
        hid = gate / (1.0 + jnp.exp(-gate)) * up
        if u < 2:
            hid = jnp.where(y == 3, jnp.zeros_like(hid), hid)
        if axis == "z":
            lanes = pl.ds(pl.multiple_of((u // 2 * 2 + core_of(u)) * L, L), L)
            hall[z, :, lanes] = hid.astype(BF16)
            block = hall.at[z, :, lanes]
        else:
            lanes = pl.ds(pl.multiple_of(core_of(u) * L, L), L)
            hz[z, :, lanes] = hid.astype(BF16)
            block = hz.at[z, :, lanes]
        if u < PASSED:
            send(block, block, shown_rs.at[u, 0], dev(dz=1))
            send(block, block, shown_rs.at[u, 1], dev(dz=3))
            return
        for d in NEAR:
            send(block, block, h_rs.at[u // 4], dev(dz=d))

    def pass_on(u):
        lanes = pl.ds(pl.multiple_of((u // 2 * 2 + core_of(u)) * L, L), L)
        for side, to, dz, a, b in ((0, 1, 3, 0, half), (1, 3, 1, half, B)):
            with scope(f"wait_shown#u={u}"):
                arrived(hall.at[mod4(z + dz), :, lanes], shown_rs.at[u, side])
            block = hall.at[mod4(z + dz), a:b, lanes]
            send(block, block, h_rs.at[0], dev(dz=to))

    for k in range(K):
        arrived(wb.at[k, c, 0], loc.at[k])
        send(wb.at[k, c, 0], wb.at[k, c, 0], f_rs.at[k], dev(dc=1))
    local_d.wait()
    send(wdb.at[y, :, c], wdb.at[y, :, c], df_rs, dev(dc=1))
    columns_of(0)
    with scope("wait_xc"):
        arrived(xg.at[1:, : 3 * R], xc_rs)
    with scope("wait_xb2"):
        arrived(xg.at[2, 4 * R :], xb_rs.at[1])
    multiply(0)
    start(0)
    columns_of(2)
    with scope("wait_sq"):
        arrived(sq_r, q_rs.at[0])
    for b in range(4):
        st2_s[b] = sq_s[b] + sq_r[0, b] + sq_r[1, b] + sq_r[2, b]
    for d in NEAR:
        send(st2_s.at[mod4(z + d)], sq2_r.at[d - 1], q_rs.at[1], dev(dz=d))
        send(st2_s.at[y], sq3_r.at[d - 1], q_rs.at[2], dev(dz=d))
    multiply(1)
    start(1)
    with scope("wait_xz2"):
        arrived(xz.at[1, 4 * RZ :], xz_rs.at[1])
    with scope("wait_xzc"):
        arrived(xz.at[:, : 3 * RZ], xzc_rs)
    multiply(4)
    start(4)
    multiply(5)
    start(5)
    for d in NEAR:
        send_rows(d, 0, K)
    add(0)
    columns_of(1)
    add(1)
    multiply(2)
    start(2)
    multiply(3)
    start(3)
    with scope("wait_sq2"):
        arrived(sq2_r, q_rs.at[1])
        arrived(sq3_r, q_rs.at[2])
    inv = as_columns(lax.rsqrt((st2_s[z] + sq2_r[0] + sq2_r[1] + sq2_r[2]) / D + EPS))
    inv_y = as_columns(lax.rsqrt((st2_s[y] + sq3_r[0] + sq3_r[1] + sq3_r[2]) / D + EPS))
    finish(0)
    finish(1)
    add(2)
    finish(4)
    add(3)
    finish(5)
    finish(2)
    pass_on(0)
    pass_on(1)
    with scope("wait_d2"):
        arrived(wdb.at[0, :, c], d_rs.at[1])
        send(wdb.at[mod4(y - 2), :, c], wdb.at[mod4(y - 2), :, c], df_rs, dev(dc=1))
    finish(3)
    with scope("wait_hz"):
        arrived(hz.at[:3], h_rs.at[1])
    last = slice(4 * L, 6 * L)
    for i, (r0, r1) in enumerate(HALVES):
        for d in NEAR:
            send(hz.at[mod4(y + d), r0:r1], hall.at[y, r0:r1, last], hy_rs.at[i], dev(dy=d))
    hall[y, :, last] = hz[y]
    with scope("wait_d"):
        for d in (1, 3):
            arrived(wdb.at[0, :, c], d_rs.at[d - 1])
            block = wdb.at[mod4(y - d), :, c]
            send(block, block, df_rs, dev(dc=1))
    with scope("wait_df"):
        arrived(wdb.at[:, :, c], df_rs)

    with scope("wait_h"):
        arrived(hall.at[:2, :, : 4 * L], h_rs.at[0])
    for yy in range(4):
        w = wdb[yy, :2].reshape(4 * L, W)
        begun[yy] = jnp.dot(hall[:, :, : 4 * L].reshape(H, 4 * L), w, preferred_element_type=F32).reshape(4, B, W)
    for i, (r0, r1) in enumerate(HALVES):
        with scope(f"wait_hy#i={i}"):
            arrived(hall.at[:3, r0:r1, last], hy_rs.at[i])
        mid = (r0 + r1) // 2
        a, b = slice(r0, mid), slice(mid, r1)
        for dy in (2, 1, 3, 0):
            yy = mod4(y + dy)
            hid = hall[:, r0:r1, 4 * L :].reshape(4 * (r1 - r0), 2 * L)
            acc = jnp.dot(hid, wdb[yy, 2].reshape(2 * L, W), preferred_element_type=F32)
            psend[yy, :, r0:r1] = (begun[yy, :, r0:r1] + acc.reshape(4, r1 - r0, W)).astype(BF16)
            if dy:
                send(psend.at[yy, :, a], p1.at[dy - 1, :, a], p_rs.at[i, 0], dev(dy=dy))
            for dx in NEAR:
                send(psend.at[yy, mod4(x + dx), b], p2.at[dx - 1, yy, b], p_rs.at[i, 1], dev(dx=dx))
    for i, (r0, r1) in enumerate(HALVES):
        mid = (r0 + r1) // 2
        a, b = slice(r0, mid), slice(mid, r1)
        with scope(f"wait_p1#i={i}"):
            arrived(p1.at[:, :, a], p_rs.at[i, 0])
        for xx in range(4):
            v = psend[y, xx, a].astype(F32)
            for d in range(3):
                v = v + p1[d, xx, a].astype(F32)
            s1[xx, a] = v.astype(BF16)
        for d in NEAR:
            send(s1.at[mod4(x + d), a], p3.at[d - 1, a], p_rs.at[i, 2], dev(dx=d))
        with scope(f"wait_p2#i={i}"):
            arrived(p2.at[:, :, b], p_rs.at[i, 1])
        for yy in range(4):
            v = psend[yy, x, b].astype(F32)
            for d in range(3):
                v = v + p2[d, yy, b].astype(F32)
            s2[yy, b] = v.astype(BF16)
        for d in NEAR:
            send(s2.at[mod4(y + d), b], p4.at[d - 1, b], p_rs.at[i, 3], dev(dy=d))
    pieces = []
    for i, (r0, r1) in enumerate(HALVES):
        mid = (r0 + r1) // 2
        a, b = slice(r0, mid), slice(mid, r1)
        with scope(f"wait_p3#i={i}"):
            arrived(p3.at[:, a], p_rs.at[i, 2])
        v1 = s1[x, a].astype(F32)
        for d in range(3):
            v1 = v1 + p3[d, a].astype(F32)
        with scope(f"wait_p4#i={i}"):
            arrived(p4.at[:, b], p_rs.at[i, 3])
        v2 = s2[y, b].astype(F32)
        for d in range(3):
            v2 = v2 + p4[d, b].astype(F32)
        piece = rows(c * H + x * B + r0, r1 - r0)
        pieces.append(0.5 * tok[rows(x * B + r0, r1 - r0), :].astype(F32) + jnp.concatenate([v1, v2], axis=0))
        out[piece, :] = pieces[i].astype(BF16)
        if i == 0:
            for d in NEAR:
                send(out.at[piece, :], out.at[piece, :], o_rs.at[i, d - 1], dev(dx=d))
    stream = jnp.concatenate(pieces, axis=0)
    mine = 2 * x + c
    st_all[mine, 0] = row_sums(stream)
    for dz, f, d, e in EVERYONE:
        send(st_all.at[mine, 0], st_all.at[mine, 4 * dz + f], t_rs, dev(dz=dz, dy=f, dx=d, dc=e))
    for d in NEAR:
        send(out.at[piece, :], out.at[piece, :], o_rs.at[1, d - 1], dev(dx=d))
    for i, (r0, r1) in enumerate(HALVES):
        with scope(f"wait_o#i={i}"):
            for d in (0, 1, 3, 2):
                block = out.at[rows(c * H + mod4(x - d) * B + r0, r1 - r0), :]
                if d:
                    arrived(block, o_rs.at[i, d - 1])
                send(block, block, of_rs, dev(dc=1))
    with scope("wait_of"):
        arrived(out.at[:H], of_rs)
    with scope("wait_st2"):
        arrived(sq_n.at[: len(EVERYONE)], t_rs)
    with scope("wait_sends"):
        for s in sends:
            s.wait_send()
    for xx in range(4):
        for cc in range(2):
            total = jnp.sum(st_all[2 * xx + cc], axis=0)
            factor = as_columns(lax.rsqrt(total / D + EPS))
            r = slice(cc * H + xx * B, cc * H + (xx + 1) * B)
            for h in range(2):
                lanes = slice(h * L, (h + 1) * L)
                out[r, lanes] = (out[r, lanes].astype(F32) * factor * ogain[:, lanes]).astype(BF16)


def body(tokens, norm_gain, gate_weight, up_weight, down_weight, out_gain):
    dma = pltpu.SemaphoreType.DMA
    hbm = pl.BlockSpec(memory_space=pltpu.HBM)
    operands = (
        tokens,
        norm_gain.reshape(1, W),
        gate_weight,
        up_weight,
        down_weight.reshape(11, L, W),
        out_gain.reshape(1, W),
    )
    return pl.pallas_call(
        kernel,
        out_shape=jax.ShapeDtypeStruct((T, W), BF16),
        in_specs=[hbm] * 6,
        out_specs=pl.BlockSpec(memory_space=pltpu.VMEM),
        scratch_shapes=[
            pltpu.VMEM((H, W), BF16),
            pltpu.VMEM((1, W), F32),
            pltpu.VMEM((W, 11 * L), BF16),
            pltpu.VMEM((W, 11 * L), BF16),
            pltpu.VMEM((11, L, W), BF16),
            pltpu.VMEM((1, W), F32),
            pltpu.VMEM((4, H, W), BF16),
            pltpu.VMEM((3, H, W), BF16),
            pltpu.VMEM((K, 2, 4, W, 2 * L), BF16),
            pltpu.VMEM((4, K, 2, L, W), BF16),
            pltpu.VMEM((2 * K, H, 2 * L), BF16),
            pltpu.VMEM((2 * K, 2, B // 2, 2 * L), BF16),
            pltpu.VMEM((2 * K, 2, B // 2, 2 * L), BF16),
            pltpu.VMEM((2 * K, 2, B, 2 * L), BF16),
            pltpu.VMEM((2 * K, 3, B, 2 * L), BF16),
            pltpu.VMEM((4, B, 2 * K * L), BF16),
            pltpu.VMEM((4, B, 2 * L), BF16),
            pltpu.VMEM((4, 4, B, W), F32),
            pltpu.VMEM((4, 4, B, W), BF16),
            pltpu.VMEM((3, 4, B, W), BF16),
            pltpu.VMEM((3, 4, B, W), BF16),
            pltpu.VMEM((4, B, W), BF16),
            pltpu.VMEM((4, B, W), BF16),
            pltpu.VMEM((3, B, W), BF16),
            pltpu.VMEM((3, B, W), BF16),
            pltpu.VMEM((4, 1, L), F32),
            pltpu.VMEM((3, 4, 1, L), F32),
            pltpu.VMEM((3, 1, L), F32),
            pltpu.VMEM((3, 1, L), F32),
            pltpu.VMEM((4, 1, L), F32),
            pltpu.VMEM((8, 16, 1, L), F32),
            pltpu.VMEM((128, 1, L), F32),
            dma,
            dma((6,)),
            dma((K + 1,)),
            dma((3,)), dma((3,)), dma, dma((3,)), dma((3,)), dma,
            dma((K, 3)), dma((K,)), dma((3,)), dma,
            dma((len(JOBS), 2)), dma((len(JOBS),)),
            dma((PASSED, 2)), dma((2,)), dma((2,)),
            dma((2, 4)), dma((3,)), dma,
            dma((2, 3)), dma,
        ],
        compiler_params=pltpu.CompilerParams(
            collective_id=0, has_side_effects=True, vmem_limit_bytes=40 * 1024 * 1024
        ),
    )(*[pltpu.with_memory_space_constraint(a, pltpu.HBM) for a in operands])


def solution(mesh):
    placed = (P(None, "ra"), P("ra"), P("ra", "cb"), P("ra", "cb"), P("cb", "ra"), P("ra"))
    return jax.shard_map(body, mesh=mesh, in_specs=placed, out_specs=P(None, "ra"), check_vma=False)
```

```python
import functools

import jax
import jax.numpy as jnp
from jax import lax
from jax.experimental import pallas as pl
from jax.experimental.pallas import tpu as pltpu
from jax.sharding import PartitionSpec as P

D = 4096
EPS = 1e-06
MESH = pl.DeviceIdType.MESH
scope = jax.named_scope
F32 = jnp.float32
BF16 = jnp.bfloat16
T = 1024
H = 512
B = 128
W = 256
L = 128
K = 3

R = 112
RZ = 32

S0 = 64
HALVES = ((0, S0), (S0, B))

JOBS = ((0, "z", True), (1, "z", True), (2, "z", True), (3, "z", True), (4, "y", False), (5, "y", False))

PASSED = 2

NEAR = (2, 1, 3)
EVERYONE = [(g, f, d, e) for g in range(4) for f in range(4) for d in range(4) for e in range(2)][1:]
EVERYONE.sort(key=lambda s: -sum(min(v, 4 - v) for v in s[:3]))


def mod4(v):
    return lax.rem(v + 4, 4)


def row_sums(v):
    sq = v * v
    hi = sq.astype(BF16)
    lo = (sq - hi.astype(F32)).astype(BF16)
    ones = jnp.ones((8, v.shape[1]), BF16)
    dims = (((1,), (1,)), ((), ()))
    out = lax.dot_general(ones, hi, dims, preferred_element_type=F32)
    return (out + lax.dot_general(ones, lo, dims, preferred_element_type=F32))[:1]


def as_columns(row):
    return jnp.transpose(jnp.broadcast_to(row, (L, L)), (1, 0))


def kernel(
    tok_h, gain_h, wg_h, wu_h, wd_h, ogain_h, out,
    tok, gain, wg, wu, wd, ogain, xg, xz, wb, wdb, part, zr, zs, rbuf, rdir, hall, hz, begun, psend, p1, p2, s1, s2, p3, p4,
    sq_s, sq_r, sq2_r, sq3_r, st2_s, st_all, sq_n,
    sent, head, loc, xa_rs, xb_rs, xc_rs, xz_rs, xza_rs, xzc_rs, w_rs, f_rs, d_rs, df_rs, relay_rs, sum_rs, shown_rs, h_rs, hy_rs,
    p_rs, q_rs, t_rs, o_rs, of_rs,
):
    ra, cb = lax.axis_index("ra"), lax.axis_index("cb")
    z, y, x, c = ra // 4, lax.rem(ra, 4), cb // 2, lax.rem(cb, 2)

    def dev(dz=0, dy=0, dx=0, dc=0):
        return (mod4(z + dz) * 4 + mod4(y + dy), mod4(x + dx) * 2 + lax.rem(c + dc, 2))

    def rows(start, size):
        return pl.ds(pl.multiple_of(start, 8), size)

    sends = []

    def send(src, dst, rs, to):
        cp = pltpu.make_async_remote_copy(
            src_ref=src, dst_ref=dst, send_sem=sent, recv_sem=rs, device_id=to, device_id_type=MESH
        )
        cp.start()
        sends.append(cp)
        return cp

    def arrived(ref, sem):
        pltpu.make_async_copy(ref, ref, sem).wait()

    def local(src, dst, sem):
        cp = pltpu.make_async_copy(src, dst, sem)
        cp.start()
        return cp

    partners = [dev(dz=d) for d in NEAR] + [dev(dy=d) for d in NEAR] + [dev(dx=d) for d in NEAR] + [dev(dc=1)]
    bar = pltpu.get_barrier_semaphore()
    for p in partners:
        pl.semaphore_signal(bar, inc=1, device_id=p, device_id_type=MESH)

    mine = rows(c * H, H)
    first = [local(tok_h.at[mine, :], tok, head.at[0]), local(gain_h, gain, head.at[0])]
    heads = [
        local(src, dst, head.at[1]) for src, dst in ((wg_h, wg), (wu_h, wu), (wd_h, wd), (ogain_h, ogain))
    ]

    def tile0(yy):
        return jnp.minimum(3 * yy, 8)

    def cols(yy, k):
        return pl.ds(pl.multiple_of((tile0(yy) + k) * L, L), L)

    for k in range(K):
        own = cols(y if k < 2 else z, k)
        local(wg_h.at[:, own], wb.at[k, c, 0, :, :L], loc.at[k])
        local(wu_h.at[:, own], wb.at[k, c, 0, :, L:], loc.at[k])
    local_d = local(wd_h.at[pl.ds(tile0(y), K)], wdb.at[y, :, c], loc.at[K])

    for h in first:
        h.wait()
    xg[0] = (tok[...].astype(F32) * gain[...]).astype(BF16)
    with scope("barrier"):
        pl.semaphore_wait(bar, len(partners))

    quarter = rows(x * R, R)
    for d in NEAR:
        send(xg.at[0, quarter], xg.at[d, quarter], xa_rs.at[d - 1], dev(dy=d))
    for d in (1, 3):
        send(xg.at[0, 4 * R :], xg.at[d, 4 * R :], xb_rs.at[d - 1], dev(dy=d))
    quarter_z = rows(x * RZ, RZ)
    for d in NEAR:
        send(xg.at[0, quarter_z], xz.at[d - 1, quarter_z], xza_rs, dev(dz=d))
    near_z = {d: send(xg.at[0, 4 * RZ :], xz.at[d - 1, 4 * RZ :], xz_rs.at[d - 1], dev(dz=d)) for d in (1, 3)}
    for h in heads:
        h.wait()

    def send_columns(k):
        for d in NEAR:
            own, to = (mod4(y + d), dev(dy=d)) if k < 2 else (mod4(z + d), dev(dz=d))
            send(wg.at[:, cols(own, k)], wb.at[k, c, d, :, :L], w_rs.at[k, d - 1], to)
            send(wu.at[:, cols(own, k)], wb.at[k, c, d, :, L:], w_rs.at[k, d - 1], to)

    send_columns(0)
    send_columns(2)
    sq = row_sums(tok[...].astype(F32))
    for b in range(4):
        sq_s[b] = sq[:, b * L : (b + 1) * L]
    for d in NEAR:
        send(sq_s, sq_r.at[d - 1], q_rs.at[0], dev(dy=d))
    for d in (1, 3, 2):
        with scope(f"wait_xa#d={d}"):
            arrived(xg.at[d, quarter], xa_rs.at[d - 1])
        for e in NEAR:
            send(xg.at[d, quarter], xg.at[d, quarter], xc_rs, dev(dx=e))
    cut = 4 * R + (H - 4 * R) // 2
    for d, part_of in ((1, slice(4 * R, cut)), (3, slice(cut, H))):
        with scope(f"wait_xb#d={d}"):
            arrived(xg.at[d, 4 * R :], xb_rs.at[d - 1])
        send(xg.at[d, part_of], xg.at[2, part_of], xb_rs.at[1], dev(dy=d))
    send_columns(1)

    def send_rows(d, k0, k1):
        tiles = pl.ds(tile0(mod4(y + d)) + k0, k1 - k0)
        send(wd.at[tiles], wdb.at[y, k0:k1, c], d_rs.at[d - 1], dev(dy=d))

    with scope("wait_xza"):
        arrived(xz.at[:, quarter_z], xza_rs)
        for e in NEAR:
            send(xz.at[:, quarter_z], xz.at[:, quarter_z], xzc_rs, dev(dx=e))
    with scope("wait_xz"):
        for d, half in ((1, slice(4 * RZ, 2 * RZ + H // 2)), (3, slice(2 * RZ + H // 2, H))):
            near_z[d].wait_recv()
            send(xz.at[d - 1, half], xz.at[1, half], xz_rs.at[1], dev(dz=d))
    def columns_of(k):
        with scope(f"wait_w#k={k}"):
            for d in NEAR:
                arrived(wb.at[k, c, d], w_rs.at[k, d - 1])
                send(wb.at[k, c, d], wb.at[k, c, d], f_rs.at[k], dev(dc=1))

    def along(axis, d):
        return (dev(dz=d), mod4(z + d)) if axis == "z" else (dev(dy=d), mod4(y + d))

    def block_of(at, r0=0, r1=B):
        return rows(at * B + r0, r1 - r0)

    def multiply(u):
        k, cc = u // 2, lax.rem(c + u % 2, 2)
        if u % 2:
            with scope(f"wait_f#k={k}"):
                arrived(wb.at[k, cc], f_rs.at[k])
        acc = jnp.zeros((H, 2 * L), F32)
        for d in range(4):
            xs = xz[d - 1] if u >= 4 and d else xg[d]
            acc = acc + jnp.dot(xs, wb[k, cc, d], preferred_element_type=F32)
        part[u] = acc.astype(BF16)

    half = B // 2

    def start(u):
        _, axis, through = JOBS[u]
        if not through:
            for d in NEAR:
                to, at = along(axis, d)
                send(part.at[u, block_of(at)], rdir.at[u, d - 1], sum_rs.at[u], to)
            return
        far = along(axis, 2)[1]
        (up1, above), (dn1, below) = along(axis, 1), along(axis, 3)
        send(part.at[u, block_of(far, 0, half)], zr.at[u, 0], relay_rs.at[u, 0], up1)
        send(part.at[u, block_of(far, half, B)], zr.at[u, 1], relay_rs.at[u, 1], dn1)
        send(part.at[u, block_of(above, half, B)], rbuf.at[u, 0, half:], sum_rs.at[u], up1)
        send(part.at[u, block_of(below, 0, half)], rbuf.at[u, 1, :half], sum_rs.at[u], dn1)

    def add(u):
        _, axis, _ = JOBS[u]
        for side, d, a, b in ((0, 1, 0, half), (1, 3, half, B)):
            to, at = along(axis, d)
            with scope(f"wait_relay#u={u}"):
                arrived(zr.at[u, side], relay_rs.at[u, side])
            zs[u, side] = (part[u, block_of(at, a, b), :].astype(F32) + zr[u, side].astype(F32)).astype(BF16)
            send(zs.at[u, side], rbuf.at[u, side, a:b], sum_rs.at[u], to)

    def core_of(u):
        return lax.rem(c + u % 2, 2)

    def finish(u):
        _, axis, through = JOBS[u]
        came = rbuf if through else rdir
        with scope(f"wait_sum#u={u}"):
            arrived(came.at[u], sum_rs.at[u])
        total = part[u, block_of(along(axis, 0)[1]), :].astype(F32)
        for d in range(2 if through else 3):
            total = total + came[u, d].astype(F32)
        scale = inv if axis == "z" else inv_y
        gate, up = total[:, :L] * scale, total[:, L:] * scale
        hid = gate / (1.0 + jnp.exp(-gate)) * up
        if u < 2:
            hid = jnp.where(y == 3, jnp.zeros_like(hid), hid)
        if axis == "z":
            lanes = pl.ds(pl.multiple_of((u // 2 * 2 + core_of(u)) * L, L), L)
            hall[z, :, lanes] = hid.astype(BF16)
            block = hall.at[z, :, lanes]
        else:
            lanes = pl.ds(pl.multiple_of(core_of(u) * L, L), L)
            hz[z, :, lanes] = hid.astype(BF16)
            block = hz.at[z, :, lanes]
        if u < PASSED:
            send(block, block, shown_rs.at[u, 0], dev(dz=1))
            send(block, block, shown_rs.at[u, 1], dev(dz=3))
            return
        for d in NEAR:
            send(block, block, h_rs.at[u // 4], dev(dz=d))

    def pass_on(u):
        lanes = pl.ds(pl.multiple_of((u // 2 * 2 + core_of(u)) * L, L), L)
        for side, to, dz, a, b in ((0, 1, 3, 0, half), (1, 3, 1, half, B)):
            with scope(f"wait_shown#u={u}"):
                arrived(hall.at[mod4(z + dz), :, lanes], shown_rs.at[u, side])
            block = hall.at[mod4(z + dz), a:b, lanes]
            send(block, block, h_rs.at[0], dev(dz=to))

    for k in range(K):
        arrived(wb.at[k, c, 0], loc.at[k])
        send(wb.at[k, c, 0], wb.at[k, c, 0], f_rs.at[k], dev(dc=1))
    local_d.wait()
    send(wdb.at[y, :, c], wdb.at[y, :, c], df_rs, dev(dc=1))
    columns_of(0)
    with scope("wait_xc"):
        arrived(xg.at[1:, : 3 * R], xc_rs)
    with scope("wait_xb2"):
        arrived(xg.at[2, 4 * R :], xb_rs.at[1])
    multiply(0)
    start(0)
    columns_of(2)
    with scope("wait_sq"):
        arrived(sq_r, q_rs.at[0])
    for b in range(4):
        st2_s[b] = sq_s[b] + sq_r[0, b] + sq_r[1, b] + sq_r[2, b]
    for d in NEAR:
        send(st2_s.at[mod4(z + d)], sq2_r.at[d - 1], q_rs.at[1], dev(dz=d))
        send(st2_s.at[y], sq3_r.at[d - 1], q_rs.at[2], dev(dz=d))
    multiply(1)
    start(1)
    with scope("wait_xz2"):
        arrived(xz.at[1, 4 * RZ :], xz_rs.at[1])
    with scope("wait_xzc"):
        arrived(xz.at[:, : 3 * RZ], xzc_rs)
    multiply(4)
    start(4)
    multiply(5)
    start(5)
    for d in NEAR:
        send_rows(d, 0, K)
    add(0)
    columns_of(1)
    add(1)
    multiply(2)
    start(2)
    multiply(3)
    start(3)
    with scope("wait_sq2"):
        arrived(sq2_r, q_rs.at[1])
        arrived(sq3_r, q_rs.at[2])
    inv = as_columns(lax.rsqrt((st2_s[z] + sq2_r[0] + sq2_r[1] + sq2_r[2]) / D + EPS))
    inv_y = as_columns(lax.rsqrt((st2_s[y] + sq3_r[0] + sq3_r[1] + sq3_r[2]) / D + EPS))
    finish(0)
    finish(1)
    add(2)
    finish(4)
    add(3)
    finish(5)
    finish(2)
    pass_on(0)
    pass_on(1)
    with scope("wait_d2"):
        arrived(wdb.at[0, :, c], d_rs.at[1])
        send(wdb.at[mod4(y - 2), :, c], wdb.at[mod4(y - 2), :, c], df_rs, dev(dc=1))
    finish(3)
    with scope("wait_hz"):
        arrived(hz.at[:3], h_rs.at[1])
    last = slice(4 * L, 6 * L)
    for i, (r0, r1) in enumerate(HALVES):
        for d in NEAR:
            send(hz.at[mod4(y + d), r0:r1], hall.at[y, r0:r1, last], hy_rs.at[i], dev(dy=d))
    hall[y, :, last] = hz[y]
    with scope("wait_d"):
        for d in (1, 3):
            arrived(wdb.at[0, :, c], d_rs.at[d - 1])
            block = wdb.at[mod4(y - d), :, c]
            send(block, block, df_rs, dev(dc=1))
    with scope("wait_df"):
        arrived(wdb.at[:, :, c], df_rs)

    with scope("wait_h"):
        arrived(hall.at[:2, :, : 4 * L], h_rs.at[0])
    for yy in range(4):
        w = wdb[yy, :2].reshape(4 * L, W)
        begun[yy] = jnp.dot(hall[:, :, : 4 * L].reshape(H, 4 * L), w, preferred_element_type=F32).reshape(4, B, W)
    for i, (r0, r1) in enumerate(HALVES):
        with scope(f"wait_hy#i={i}"):
            arrived(hall.at[:3, r0:r1, last], hy_rs.at[i])
        mid = (r0 + r1) // 2
        a, b = slice(r0, mid), slice(mid, r1)
        for dy in (2, 1, 3, 0):
            yy = mod4(y + dy)
            hid = hall[:, r0:r1, 4 * L :].reshape(4 * (r1 - r0), 2 * L)
            acc = jnp.dot(hid, wdb[yy, 2].reshape(2 * L, W), preferred_element_type=F32)
            psend[yy, :, r0:r1] = (begun[yy, :, r0:r1] + acc.reshape(4, r1 - r0, W)).astype(BF16)
            for dx in NEAR:
                send(psend.at[yy, mod4(x + dx), b], p2.at[dx - 1, yy, b], p_rs.at[i, 1], dev(dx=dx))
            if dy:
                send(psend.at[yy, :, a], p1.at[dy - 1, :, a], p_rs.at[i, 0], dev(dy=dy))
    for i, (r0, r1) in enumerate(HALVES):
        mid = (r0 + r1) // 2
        a, b = slice(r0, mid), slice(mid, r1)
        with scope(f"wait_p1#i={i}"):
            arrived(p1.at[:, :, a], p_rs.at[i, 0])
        for xx in range(4):
            v = psend[y, xx, a].astype(F32)
            for d in range(3):
                v = v + p1[d, xx, a].astype(F32)
            s1[xx, a] = v.astype(BF16)
        for d in NEAR:
            send(s1.at[mod4(x + d), a], p3.at[d - 1, a], p_rs.at[i, 2], dev(dx=d))
        with scope(f"wait_p2#i={i}"):
            arrived(p2.at[:, :, b], p_rs.at[i, 1])
        for yy in range(4):
            v = psend[yy, x, b].astype(F32)
            for d in range(3):
                v = v + p2[d, yy, b].astype(F32)
            s2[yy, b] = v.astype(BF16)
        for d in NEAR:
            send(s2.at[mod4(y + d), b], p4.at[d - 1, b], p_rs.at[i, 3], dev(dy=d))
    pieces = []
    for i, (r0, r1) in enumerate(HALVES):
        mid = (r0 + r1) // 2
        a, b = slice(r0, mid), slice(mid, r1)
        with scope(f"wait_p3#i={i}"):
            arrived(p3.at[:, a], p_rs.at[i, 2])
        v1 = s1[x, a].astype(F32)
        for d in range(3):
            v1 = v1 + p3[d, a].astype(F32)
        with scope(f"wait_p4#i={i}"):
            arrived(p4.at[:, b], p_rs.at[i, 3])
        v2 = s2[y, b].astype(F32)
        for d in range(3):
            v2 = v2 + p4[d, b].astype(F32)
        piece = rows(c * H + x * B + r0, r1 - r0)
        pieces.append(0.5 * tok[rows(x * B + r0, r1 - r0), :].astype(F32) + jnp.concatenate([v1, v2], axis=0))
        out[piece, :] = pieces[i].astype(BF16)
        if i == 0:
            for d in NEAR:
                send(out.at[piece, :], out.at[piece, :], o_rs.at[i, d - 1], dev(dx=d))
    stream = jnp.concatenate(pieces, axis=0)
    mine = 2 * x + c
    st_all[mine, 0] = row_sums(stream)
    for dz, f, d, e in EVERYONE:
        send(st_all.at[mine, 0], st_all.at[mine, 4 * dz + f], t_rs, dev(dz=dz, dy=f, dx=d, dc=e))
    for d in NEAR:
        send(out.at[piece, :], out.at[piece, :], o_rs.at[1, d - 1], dev(dx=d))
    for i, (r0, r1) in enumerate(HALVES):
        with scope(f"wait_o#i={i}"):
            for d in (0, 1, 3, 2):
                block = out.at[rows(c * H + mod4(x - d) * B + r0, r1 - r0), :]
                if d:
                    arrived(block, o_rs.at[i, d - 1])
                send(block, block, of_rs, dev(dc=1))
    with scope("wait_of"):
        arrived(out.at[:H], of_rs)
    with scope("wait_st2"):
        arrived(sq_n.at[: len(EVERYONE)], t_rs)
    with scope("wait_sends"):
        for s in sends:
            s.wait_send()
    for xx in range(4):
        for cc in range(2):
            total = jnp.sum(st_all[2 * xx + cc], axis=0)
            factor = as_columns(lax.rsqrt(total / D + EPS))
            r = slice(cc * H + xx * B, cc * H + (xx + 1) * B)
            for h in range(2):
                lanes = slice(h * L, (h + 1) * L)
                out[r, lanes] = (out[r, lanes].astype(F32) * factor * ogain[:, lanes]).astype(BF16)


def body(tokens, norm_gain, gate_weight, up_weight, down_weight, out_gain):
    dma = pltpu.SemaphoreType.DMA
    hbm = pl.BlockSpec(memory_space=pltpu.HBM)
    operands = (
        tokens,
        norm_gain.reshape(1, W),
        gate_weight,
        up_weight,
        down_weight.reshape(11, L, W),
        out_gain.reshape(1, W),
    )
    return pl.pallas_call(
        kernel,
        out_shape=jax.ShapeDtypeStruct((T, W), BF16),
        in_specs=[hbm] * 6,
        out_specs=pl.BlockSpec(memory_space=pltpu.VMEM),
        scratch_shapes=[
            pltpu.VMEM((H, W), BF16),
            pltpu.VMEM((1, W), F32),
            pltpu.VMEM((W, 11 * L), BF16),
            pltpu.VMEM((W, 11 * L), BF16),
            pltpu.VMEM((11, L, W), BF16),
            pltpu.VMEM((1, W), F32),
            pltpu.VMEM((4, H, W), BF16),
            pltpu.VMEM((3, H, W), BF16),
            pltpu.VMEM((K, 2, 4, W, 2 * L), BF16),
            pltpu.VMEM((4, K, 2, L, W), BF16),
            pltpu.VMEM((2 * K, H, 2 * L), BF16),
            pltpu.VMEM((2 * K, 2, B // 2, 2 * L), BF16),
            pltpu.VMEM((2 * K, 2, B // 2, 2 * L), BF16),
            pltpu.VMEM((2 * K, 2, B, 2 * L), BF16),
            pltpu.VMEM((2 * K, 3, B, 2 * L), BF16),
            pltpu.VMEM((4, B, 2 * K * L), BF16),
            pltpu.VMEM((4, B, 2 * L), BF16),
            pltpu.VMEM((4, 4, B, W), F32),
            pltpu.VMEM((4, 4, B, W), BF16),
            pltpu.VMEM((3, 4, B, W), BF16),
            pltpu.VMEM((3, 4, B, W), BF16),
            pltpu.VMEM((4, B, W), BF16),
            pltpu.VMEM((4, B, W), BF16),
            pltpu.VMEM((3, B, W), BF16),
            pltpu.VMEM((3, B, W), BF16),
            pltpu.VMEM((4, 1, L), F32),
            pltpu.VMEM((3, 4, 1, L), F32),
            pltpu.VMEM((3, 1, L), F32),
            pltpu.VMEM((3, 1, L), F32),
            pltpu.VMEM((4, 1, L), F32),
            pltpu.VMEM((8, 16, 1, L), F32),
            pltpu.VMEM((128, 1, L), F32),
            dma,
            dma((2,)),
            dma((K + 1,)),
            dma((3,)), dma((3,)), dma, dma((3,)), dma, dma,
            dma((K, 3)), dma((K,)), dma((3,)), dma,
            dma((4, 2)), dma((len(JOBS),)),
            dma((PASSED, 2)), dma((2,)), dma((2,)),
            dma((2, 4)), dma((3,)), dma,
            dma((2, 3)), dma,
        ],
        compiler_params=pltpu.CompilerParams(
            collective_id=0, has_side_effects=True, vmem_limit_bytes=40 * 1024 * 1024
        ),
    )(*[pltpu.with_memory_space_constraint(a, pltpu.HBM) for a in operands])


def solution(mesh):
    placed = (P(None, "ra"), P("ra"), P("ra", "cb"), P("ra", "cb"), P("cb", "ra"), P("ra"))
    return jax.shard_map(body, mesh=mesh, in_specs=placed, out_specs=P(None, "ra"), check_vma=False)
```

```python
import functools

import jax
import jax.numpy as jnp
from jax import lax
from jax.experimental import pallas as pl
from jax.experimental.pallas import tpu as pltpu
from jax.sharding import PartitionSpec as P

D = 4096
EPS = 1e-06
MESH = pl.DeviceIdType.MESH
scope = jax.named_scope
F32 = jnp.float32
BF16 = jnp.bfloat16
T = 1024
H = 512
B = 128
W = 256
L = 128
K = 3

R = 112
RZ = 32

S0 = 64
HALVES = ((0, S0), (S0, B))

JOBS = ((0, "z", True), (1, "z", True), (2, "z", True), (3, "z", True), (4, "y", False), (5, "y", False))

PASSED = 2

NEAR = (2, 1, 3)
EVERYONE = [(g, f, d, e) for g in range(4) for f in range(4) for d in range(4) for e in range(2)][1:]
EVERYONE.sort(key=lambda s: -sum(min(v, 4 - v) for v in s[:3]))


def mod4(v):
    return lax.rem(v + 4, 4)


def row_sums(v):
    sq = v * v
    hi = sq.astype(BF16)
    lo = (sq - hi.astype(F32)).astype(BF16)
    ones = jnp.ones((8, v.shape[1]), BF16)
    dims = (((1,), (1,)), ((), ()))
    out = lax.dot_general(ones, hi, dims, preferred_element_type=F32)
    return (out + lax.dot_general(ones, lo, dims, preferred_element_type=F32))[:1]


def as_columns(row):
    return jnp.transpose(jnp.broadcast_to(row, (L, L)), (1, 0))


def kernel(
    tok_h, gain_h, wg_h, wu_h, wd_h, ogain_h, out, scale,
    tok, gain, wg, wu, wd, ogain, xg, xz, wb, wdb, part, zr, zs, rbuf, rdir, hall, hz, begun, psend, p1, p2, s1, s2, p3, p4,
    sq_s, sq_r, sq2_r, sq3_r, st2_s, st_all, sq_n,
    sent, head, loc, xa_rs, xb_rs, xc_rs, xz_rs, xza_rs, xzc_rs, w_rs, f_rs, d_rs, df_rs, relay_rs, sum_rs, shown_rs, h_rs, hy_rs,
    p_rs, q_rs, t_rs, o_rs, of_rs,
):
    ra, cb = lax.axis_index("ra"), lax.axis_index("cb")
    z, y, x, c = ra // 4, lax.rem(ra, 4), cb // 2, lax.rem(cb, 2)

    def dev(dz=0, dy=0, dx=0, dc=0):
        return (mod4(z + dz) * 4 + mod4(y + dy), mod4(x + dx) * 2 + lax.rem(c + dc, 2))

    def rows(start, size):
        return pl.ds(pl.multiple_of(start, 8), size)

    sends = []

    def send(src, dst, rs, to):
        cp = pltpu.make_async_remote_copy(
            src_ref=src, dst_ref=dst, send_sem=sent, recv_sem=rs, device_id=to, device_id_type=MESH
        )
        cp.start()
        sends.append(cp)
        return cp

    def arrived(ref, sem):
        pltpu.make_async_copy(ref, ref, sem).wait()

    def local(src, dst, sem):
        cp = pltpu.make_async_copy(src, dst, sem)
        cp.start()
        return cp

    partners = [dev(dz=d) for d in NEAR] + [dev(dy=d) for d in NEAR] + [dev(dx=d) for d in NEAR] + [dev(dc=1)]
    bar = pltpu.get_barrier_semaphore()
    for p in partners:
        pl.semaphore_signal(bar, inc=1, device_id=p, device_id_type=MESH)

    mine = rows(c * H, H)
    first = [local(tok_h.at[mine, :], tok, head.at[0]), local(gain_h, gain, head.at[0])]
    heads = [
        local(src, dst, head.at[1]) for src, dst in ((wg_h, wg), (wu_h, wu), (wd_h, wd), (ogain_h, ogain))
    ]

    def tile0(yy):
        return jnp.minimum(3 * yy, 8)

    def cols(yy, k):
        return pl.ds(pl.multiple_of((tile0(yy) + k) * L, L), L)

    for k in range(K):
        own = cols(y if k < 2 else z, k)
        local(wg_h.at[:, own], wb.at[k, c, 0, :, :L], loc.at[k])
        local(wu_h.at[:, own], wb.at[k, c, 0, :, L:], loc.at[k])
    local_d = local(wd_h.at[pl.ds(tile0(y), K)], wdb.at[y, :, c], loc.at[K])

    for h in first:
        h.wait()
    xg[0] = (tok[...].astype(F32) * gain[...]).astype(BF16)
    with scope("barrier"):
        pl.semaphore_wait(bar, len(partners))

    quarter = rows(x * R, R)
    for d in NEAR:
        send(xg.at[0, quarter], xg.at[d, quarter], xa_rs.at[d - 1], dev(dy=d))
    for d in (1, 3):
        send(xg.at[0, 4 * R :], xg.at[d, 4 * R :], xb_rs.at[d - 1], dev(dy=d))
    quarter_z = rows(x * RZ, RZ)
    for d in NEAR:
        send(xg.at[0, quarter_z], xz.at[d - 1, quarter_z], xza_rs, dev(dz=d))
    near_z = {d: send(xg.at[0, 4 * RZ :], xz.at[d - 1, 4 * RZ :], xz_rs.at[d - 1], dev(dz=d)) for d in (1, 3)}
    for h in heads:
        h.wait()

    def send_columns(k):
        for d in NEAR:
            own, to = (mod4(y + d), dev(dy=d)) if k < 2 else (mod4(z + d), dev(dz=d))
            send(wg.at[:, cols(own, k)], wb.at[k, c, d, :, :L], w_rs.at[k, d - 1], to)
            send(wu.at[:, cols(own, k)], wb.at[k, c, d, :, L:], w_rs.at[k, d - 1], to)

    send_columns(0)
    send_columns(2)
    sq = row_sums(tok[...].astype(F32))
    for b in range(4):
        sq_s[b] = sq[:, b * L : (b + 1) * L]
    for d in NEAR:
        send(sq_s, sq_r.at[d - 1], q_rs.at[0], dev(dy=d))
    for d in (1, 3, 2):
        with scope(f"wait_xa#d={d}"):
            arrived(xg.at[d, quarter], xa_rs.at[d - 1])
        for e in NEAR:
            send(xg.at[d, quarter], xg.at[d, quarter], xc_rs, dev(dx=e))
    cut = 4 * R + (H - 4 * R) // 2
    for d, part_of in ((1, slice(4 * R, cut)), (3, slice(cut, H))):
        with scope(f"wait_xb#d={d}"):
            arrived(xg.at[d, 4 * R :], xb_rs.at[d - 1])
        send(xg.at[d, part_of], xg.at[2, part_of], xb_rs.at[1], dev(dy=d))
    send_columns(1)

    def send_rows(d, k0, k1):
        tiles = pl.ds(tile0(mod4(y + d)) + k0, k1 - k0)
        send(wd.at[tiles], wdb.at[y, k0:k1, c], d_rs.at[d - 1], dev(dy=d))

    with scope("wait_xza"):
        arrived(xz.at[:, quarter_z], xza_rs)
        for e in NEAR:
            send(xz.at[:, quarter_z], xz.at[:, quarter_z], xzc_rs, dev(dx=e))
    with scope("wait_xz"):
        for d, half in ((1, slice(4 * RZ, 2 * RZ + H // 2)), (3, slice(2 * RZ + H // 2, H))):
            near_z[d].wait_recv()
            send(xz.at[d - 1, half], xz.at[1, half], xz_rs.at[1], dev(dz=d))
    def columns_of(k):
        with scope(f"wait_w#k={k}"):
            for d in NEAR:
                arrived(wb.at[k, c, d], w_rs.at[k, d - 1])
                send(wb.at[k, c, d], wb.at[k, c, d], f_rs.at[k], dev(dc=1))

    def along(axis, d):
        return (dev(dz=d), mod4(z + d)) if axis == "z" else (dev(dy=d), mod4(y + d))

    def block_of(at, r0=0, r1=B):
        return rows(at * B + r0, r1 - r0)

    def multiply(u):
        k, cc = u // 2, lax.rem(c + u % 2, 2)
        if u % 2:
            with scope(f"wait_f#k={k}"):
                arrived(wb.at[k, cc], f_rs.at[k])
        acc = jnp.zeros((H, 2 * L), F32)
        for d in range(4):
            xs = xz[d - 1] if u >= 4 and d else xg[d]
            acc = acc + jnp.dot(xs, wb[k, cc, d], preferred_element_type=F32)
        part[u] = acc.astype(BF16)

    half = B // 2

    def start(u):
        _, axis, through = JOBS[u]
        if not through:
            for d in NEAR:
                to, at = along(axis, d)
                send(part.at[u, block_of(at)], rdir.at[u, d - 1], sum_rs.at[u], to)
            return
        far = along(axis, 2)[1]
        (up1, above), (dn1, below) = along(axis, 1), along(axis, 3)
        send(part.at[u, block_of(far, 0, half)], zr.at[u, 0], relay_rs.at[u, 0], up1)
        send(part.at[u, block_of(far, half, B)], zr.at[u, 1], relay_rs.at[u, 1], dn1)
        send(part.at[u, block_of(above, half, B)], rbuf.at[u, 0, half:], sum_rs.at[u], up1)
        send(part.at[u, block_of(below, 0, half)], rbuf.at[u, 1, :half], sum_rs.at[u], dn1)

    def add(u):
        _, axis, _ = JOBS[u]
        for side, d, a, b in ((0, 1, 0, half), (1, 3, half, B)):
            to, at = along(axis, d)
            with scope(f"wait_relay#u={u}"):
                arrived(zr.at[u, side], relay_rs.at[u, side])
            zs[u, side] = (part[u, block_of(at, a, b), :].astype(F32) + zr[u, side].astype(F32)).astype(BF16)
            send(zs.at[u, side], rbuf.at[u, side, a:b], sum_rs.at[u], to)

    def core_of(u):
        return lax.rem(c + u % 2, 2)

    def finish(u):
        _, axis, through = JOBS[u]
        came = rbuf if through else rdir
        with scope(f"wait_sum#u={u}"):
            arrived(came.at[u], sum_rs.at[u])
        total = part[u, block_of(along(axis, 0)[1]), :].astype(F32)
        for d in range(2 if through else 3):
            total = total + came[u, d].astype(F32)
        scale = inv if axis == "z" else inv_y
        gate, up = total[:, :L] * scale, total[:, L:] * scale
        hid = gate / (1.0 + jnp.exp(-gate)) * up
        if u < 2:
            hid = jnp.where(y == 3, jnp.zeros_like(hid), hid)
        if axis == "z":
            lanes = pl.ds(pl.multiple_of((u // 2 * 2 + core_of(u)) * L, L), L)
            hall[z, :, lanes] = hid.astype(BF16)
            block = hall.at[z, :, lanes]
        else:
            lanes = pl.ds(pl.multiple_of(core_of(u) * L, L), L)
            hz[z, :, lanes] = hid.astype(BF16)
            block = hz.at[z, :, lanes]
        if u < PASSED:
            send(block, block, shown_rs.at[u, 0], dev(dz=1))
            send(block, block, shown_rs.at[u, 1], dev(dz=3))
            return
        for d in NEAR:
            send(block, block, h_rs.at[u // 4], dev(dz=d))

    def pass_on(u):
        lanes = pl.ds(pl.multiple_of((u // 2 * 2 + core_of(u)) * L, L), L)
        for side, to, dz, a, b in ((0, 1, 3, 0, half), (1, 3, 1, half, B)):
            with scope(f"wait_shown#u={u}"):
                arrived(hall.at[mod4(z + dz), :, lanes], shown_rs.at[u, side])
            block = hall.at[mod4(z + dz), a:b, lanes]
            send(block, block, h_rs.at[0], dev(dz=to))

    for k in range(K):
        arrived(wb.at[k, c, 0], loc.at[k])
        send(wb.at[k, c, 0], wb.at[k, c, 0], f_rs.at[k], dev(dc=1))
    local_d.wait()
    send(wdb.at[y, :, c], wdb.at[y, :, c], df_rs, dev(dc=1))
    columns_of(0)
    with scope("wait_xc"):
        arrived(xg.at[1:, : 3 * R], xc_rs)
    with scope("wait_xb2"):
        arrived(xg.at[2, 4 * R :], xb_rs.at[1])
    multiply(0)
    start(0)
    columns_of(2)
    with scope("wait_sq"):
        arrived(sq_r, q_rs.at[0])
    for b in range(4):
        st2_s[b] = sq_s[b] + sq_r[0, b] + sq_r[1, b] + sq_r[2, b]
    for d in NEAR:
        send(st2_s.at[mod4(z + d)], sq2_r.at[d - 1], q_rs.at[1], dev(dz=d))
        send(st2_s.at[y], sq3_r.at[d - 1], q_rs.at[2], dev(dz=d))
    multiply(1)
    start(1)
    with scope("wait_xz2"):
        arrived(xz.at[1, 4 * RZ :], xz_rs.at[1])
    with scope("wait_xzc"):
        arrived(xz.at[:, : 3 * RZ], xzc_rs)
    multiply(4)
    start(4)
    multiply(5)
    start(5)
    for d in NEAR:
        send_rows(d, 0, K)
    add(0)
    columns_of(1)
    add(1)
    multiply(2)
    start(2)
    multiply(3)
    start(3)
    with scope("wait_sq2"):
        arrived(sq2_r, q_rs.at[1])
        arrived(sq3_r, q_rs.at[2])
    inv = as_columns(lax.rsqrt((st2_s[z] + sq2_r[0] + sq2_r[1] + sq2_r[2]) / D + EPS))
    inv_y = as_columns(lax.rsqrt((st2_s[y] + sq3_r[0] + sq3_r[1] + sq3_r[2]) / D + EPS))
    finish(0)
    finish(1)
    add(2)
    finish(4)
    add(3)
    finish(5)
    finish(2)
    pass_on(0)
    pass_on(1)
    with scope("wait_d2"):
        arrived(wdb.at[0, :, c], d_rs.at[1])
        send(wdb.at[mod4(y - 2), :, c], wdb.at[mod4(y - 2), :, c], df_rs, dev(dc=1))
    finish(3)
    with scope("wait_hz"):
        arrived(hz.at[:3], h_rs.at[1])
    last = slice(4 * L, 6 * L)
    for i, (r0, r1) in enumerate(HALVES):
        for d in NEAR:
            send(hz.at[mod4(y + d), r0:r1], hall.at[y, r0:r1, last], hy_rs.at[i], dev(dy=d))
    hall[y, :, last] = hz[y]
    with scope("wait_d"):
        for d in (1, 3):
            arrived(wdb.at[0, :, c], d_rs.at[d - 1])
            block = wdb.at[mod4(y - d), :, c]
            send(block, block, df_rs, dev(dc=1))
    with scope("wait_df"):
        arrived(wdb.at[:, :, c], df_rs)

    with scope("wait_h"):
        arrived(hall.at[:2, :, : 4 * L], h_rs.at[0])
    for yy in range(4):
        w = wdb[yy, :2].reshape(4 * L, W)
        begun[yy] = jnp.dot(hall[:, :, : 4 * L].reshape(H, 4 * L), w, preferred_element_type=F32).reshape(4, B, W)
    for i, (r0, r1) in enumerate(HALVES):
        with scope(f"wait_hy#i={i}"):
            arrived(hall.at[:3, r0:r1, last], hy_rs.at[i])
        mid = (r0 + r1) // 2
        a, b = slice(r0, mid), slice(mid, r1)
        for dy in (2, 1, 3, 0):
            yy = mod4(y + dy)
            hid = hall[:, r0:r1, 4 * L :].reshape(4 * (r1 - r0), 2 * L)
            acc = jnp.dot(hid, wdb[yy, 2].reshape(2 * L, W), preferred_element_type=F32)
            psend[yy, :, r0:r1] = (begun[yy, :, r0:r1] + acc.reshape(4, r1 - r0, W)).astype(BF16)
            for dx in NEAR:
                send(psend.at[yy, mod4(x + dx), b], p2.at[dx - 1, yy, b], p_rs.at[i, 1], dev(dx=dx))
            if dy:
                send(psend.at[yy, :, a], p1.at[dy - 1, :, a], p_rs.at[i, 0], dev(dy=dy))
    for i, (r0, r1) in enumerate(HALVES):
        mid = (r0 + r1) // 2
        a, b = slice(r0, mid), slice(mid, r1)
        with scope(f"wait_p1#i={i}"):
            arrived(p1.at[:, :, a], p_rs.at[i, 0])
        for xx in range(4):
            v = psend[y, xx, a].astype(F32)
            for d in range(3):
                v = v + p1[d, xx, a].astype(F32)
            s1[xx, a] = v.astype(BF16)
        for d in NEAR:
            send(s1.at[mod4(x + d), a], p3.at[d - 1, a], p_rs.at[i, 2], dev(dx=d))
        with scope(f"wait_p2#i={i}"):
            arrived(p2.at[:, :, b], p_rs.at[i, 1])
        for yy in range(4):
            v = psend[yy, x, b].astype(F32)
            for d in range(3):
                v = v + p2[d, yy, b].astype(F32)
            s2[yy, b] = v.astype(BF16)
        for d in NEAR:
            send(s2.at[mod4(y + d), b], p4.at[d - 1, b], p_rs.at[i, 3], dev(dy=d))
    pieces = []
    for i, (r0, r1) in enumerate(HALVES):
        mid = (r0 + r1) // 2
        a, b = slice(r0, mid), slice(mid, r1)
        with scope(f"wait_p3#i={i}"):
            arrived(p3.at[:, a], p_rs.at[i, 2])
        v1 = s1[x, a].astype(F32)
        for d in range(3):
            v1 = v1 + p3[d, a].astype(F32)
        with scope(f"wait_p4#i={i}"):
            arrived(p4.at[:, b], p_rs.at[i, 3])
        v2 = s2[y, b].astype(F32)
        for d in range(3):
            v2 = v2 + p4[d, b].astype(F32)
        piece = rows(c * H + x * B + r0, r1 - r0)
        pieces.append(0.5 * tok[rows(x * B + r0, r1 - r0), :].astype(F32) + jnp.concatenate([v1, v2], axis=0))
        out[piece, :] = pieces[i].astype(BF16)
        if i == 0:
            for d in NEAR:
                send(out.at[piece, :], out.at[piece, :], o_rs.at[i, d - 1], dev(dx=d))
    stream = jnp.concatenate(pieces, axis=0)
    mine = 2 * x + c
    st_all[mine, 0] = row_sums(stream)
    for dz, f, d, e in EVERYONE:
        send(st_all.at[mine, 0], st_all.at[mine, 4 * dz + f], t_rs, dev(dz=dz, dy=f, dx=d, dc=e))
    for d in NEAR:
        send(out.at[piece, :], out.at[piece, :], o_rs.at[1, d - 1], dev(dx=d))
    for i, (r0, r1) in enumerate(HALVES):
        with scope(f"wait_o#i={i}"):
            for d in (0, 1, 3, 2):
                block = out.at[rows(c * H + mod4(x - d) * B + r0, r1 - r0), :]
                if d:
                    arrived(block, o_rs.at[i, d - 1])
                send(block, block, of_rs, dev(dc=1))
    with scope("wait_of"):
        arrived(out.at[:H], of_rs)
    with scope("wait_st2"):
        arrived(sq_n.at[: len(EVERYONE)], t_rs)
    with scope("wait_sends"):
        for s in sends:
            s.wait_send()
    for xx in range(4):
        for cc in range(2):
            total = jnp.sum(st_all[2 * xx + cc], axis=0)
            factor = as_columns(lax.rsqrt(total / D + EPS))
            r = slice(cc * H + xx * B, cc * H + (xx + 1) * B)
            for h in range(2):
                lanes = slice(h * L, (h + 1) * L)
                scale[r, lanes] = factor * ogain[:, lanes]


def body(tokens, norm_gain, gate_weight, up_weight, down_weight, out_gain):
    dma = pltpu.SemaphoreType.DMA
    hbm = pl.BlockSpec(memory_space=pltpu.HBM)
    operands = (
        tokens,
        norm_gain.reshape(1, W),
        gate_weight,
        up_weight,
        down_weight.reshape(11, L, W),
        out_gain.reshape(1, W),
    )
    stream, scale = pl.pallas_call(
        kernel,
        out_shape=(jax.ShapeDtypeStruct((T, W), BF16), jax.ShapeDtypeStruct((T, W), F32)),
        in_specs=[hbm] * 6,
        out_specs=(pl.BlockSpec(memory_space=pltpu.VMEM),) * 2,
        scratch_shapes=[
            pltpu.VMEM((H, W), BF16),
            pltpu.VMEM((1, W), F32),
            pltpu.VMEM((W, 11 * L), BF16),
            pltpu.VMEM((W, 11 * L), BF16),
            pltpu.VMEM((11, L, W), BF16),
            pltpu.VMEM((1, W), F32),
            pltpu.VMEM((4, H, W), BF16),
            pltpu.VMEM((3, H, W), BF16),
            pltpu.VMEM((K, 2, 4, W, 2 * L), BF16),
            pltpu.VMEM((4, K, 2, L, W), BF16),
            pltpu.VMEM((2 * K, H, 2 * L), BF16),
            pltpu.VMEM((2 * K, 2, B // 2, 2 * L), BF16),
            pltpu.VMEM((2 * K, 2, B // 2, 2 * L), BF16),
            pltpu.VMEM((2 * K, 2, B, 2 * L), BF16),
            pltpu.VMEM((2 * K, 3, B, 2 * L), BF16),
            pltpu.VMEM((4, B, 2 * K * L), BF16),
            pltpu.VMEM((4, B, 2 * L), BF16),
            pltpu.VMEM((4, 4, B, W), F32),
            pltpu.VMEM((4, 4, B, W), BF16),
            pltpu.VMEM((3, 4, B, W), BF16),
            pltpu.VMEM((3, 4, B, W), BF16),
            pltpu.VMEM((4, B, W), BF16),
            pltpu.VMEM((4, B, W), BF16),
            pltpu.VMEM((3, B, W), BF16),
            pltpu.VMEM((3, B, W), BF16),
            pltpu.VMEM((4, 1, L), F32),
            pltpu.VMEM((3, 4, 1, L), F32),
            pltpu.VMEM((3, 1, L), F32),
            pltpu.VMEM((3, 1, L), F32),
            pltpu.VMEM((4, 1, L), F32),
            pltpu.VMEM((8, 16, 1, L), F32),
            pltpu.VMEM((128, 1, L), F32),
            dma,
            dma((2,)),
            dma((K + 1,)),
            dma((3,)), dma((3,)), dma, dma((3,)), dma, dma,
            dma((K, 3)), dma((K,)), dma((3,)), dma,
            dma((4, 2)), dma((len(JOBS),)),
            dma((PASSED, 2)), dma((2,)), dma((2,)),
            dma((2, 4)), dma((3,)), dma,
            dma((2, 3)), dma,
        ],
        compiler_params=pltpu.CompilerParams(
            collective_id=0, has_side_effects=True, vmem_limit_bytes=40 * 1024 * 1024
        ),
    )(*[pltpu.with_memory_space_constraint(a, pltpu.HBM) for a in operands])
    return (stream.astype(F32) * scale).astype(BF16)


def solution(mesh):
    placed = (P(None, "ra"), P("ra"), P("ra", "cb"), P("ra", "cb"), P("cb", "ra"), P("ra"))
    return jax.shard_map(body, mesh=mesh, in_specs=placed, out_specs=P(None, "ra"), check_vma=False)
```

```python
import functools

import jax
import jax.numpy as jnp
from jax import lax
from jax.experimental import pallas as pl
from jax.experimental.pallas import tpu as pltpu
from jax.sharding import PartitionSpec as P

D = 4096
EPS = 1e-06
MESH = pl.DeviceIdType.MESH
scope = jax.named_scope
F32 = jnp.float32
BF16 = jnp.bfloat16
T = 1024
H = 512
B = 128
W = 256
L = 128
K = 3

R = 104
RZ = 32

S0 = 64
HALVES = ((0, S0), (S0, B))

JOBS = ((0, "z", True), (1, "z", True), (2, "z", True), (3, "z", True), (4, "y", False), (5, "y", False))

PASSED = 2

NEAR = (2, 1, 3)
EVERYONE = [(g, f, d, e) for g in range(4) for f in range(4) for d in range(4) for e in range(2)][1:]
EVERYONE.sort(key=lambda s: -sum(min(v, 4 - v) for v in s[:3]))


def mod4(v):
    return lax.rem(v + 4, 4)


def row_sums(v):
    sq = v * v
    hi = sq.astype(BF16)
    lo = (sq - hi.astype(F32)).astype(BF16)
    ones = jnp.ones((8, v.shape[1]), BF16)
    dims = (((1,), (1,)), ((), ()))
    out = lax.dot_general(ones, hi, dims, preferred_element_type=F32)
    return (out + lax.dot_general(ones, lo, dims, preferred_element_type=F32))[:1]


def as_columns(row):
    return jnp.transpose(jnp.broadcast_to(row, (L, L)), (1, 0))


def kernel(
    tok_h, gain_h, wg_h, wu_h, wd_h, ogain_h, out,
    tok, gain, wg, wu, wd, ogain, xg, xz, wb, wdb, part, zr, zs, rbuf, rdir, hall, hz, begun, psend, p1, p2, s1, s2, p3, p4,
    sq_s, sq_r, sq2_r, sq3_r, st2_s, st_all, sq_n,
    sent, head, loc, xa_rs, xb_rs, xc_rs, xz_rs, xza_rs, xzc_rs, w_rs, f_rs, d_rs, df_rs, relay_rs, sum_rs, shown_rs, h_rs, hy_rs,
    p_rs, q_rs, t_rs, o_rs, of_rs,
):
    ra, cb = lax.axis_index("ra"), lax.axis_index("cb")
    z, y, x, c = ra // 4, lax.rem(ra, 4), cb // 2, lax.rem(cb, 2)

    def dev(dz=0, dy=0, dx=0, dc=0):
        return (mod4(z + dz) * 4 + mod4(y + dy), mod4(x + dx) * 2 + lax.rem(c + dc, 2))

    def rows(start, size):
        return pl.ds(pl.multiple_of(start, 8), size)

    sends = []

    def send(src, dst, rs, to):
        cp = pltpu.make_async_remote_copy(
            src_ref=src, dst_ref=dst, send_sem=sent, recv_sem=rs, device_id=to, device_id_type=MESH
        )
        cp.start()
        sends.append(cp)
        return cp

    def arrived(ref, sem):
        pltpu.make_async_copy(ref, ref, sem).wait()

    def local(src, dst, sem):
        cp = pltpu.make_async_copy(src, dst, sem)
        cp.start()
        return cp

    partners = [dev(dz=d) for d in NEAR] + [dev(dy=d) for d in NEAR] + [dev(dx=d) for d in NEAR] + [dev(dc=1)]
    bar = pltpu.get_barrier_semaphore()
    for p in partners:
        pl.semaphore_signal(bar, inc=1, device_id=p, device_id_type=MESH)

    mine = rows(c * H, H)
    first = [local(tok_h.at[mine, :], tok, head.at[0]), local(gain_h, gain, head.at[0])]
    heads = [
        local(src, dst, head.at[1]) for src, dst in ((wg_h, wg), (wu_h, wu), (wd_h, wd), (ogain_h, ogain))
    ]

    def tile0(yy):
        return jnp.minimum(3 * yy, 8)

    def cols(yy, k):
        return pl.ds(pl.multiple_of((tile0(yy) + k) * L, L), L)

    for k in range(K):
        own = cols(y if k < 2 else z, k)
        local(wg_h.at[:, own], wb.at[k, c, 0, :, :L], loc.at[k])
        local(wu_h.at[:, own], wb.at[k, c, 0, :, L:], loc.at[k])
    local_d = local(wd_h.at[pl.ds(tile0(y), K)], wdb.at[y, :, c], loc.at[K])

    for h in first:
        h.wait()
    xg[0] = (tok[...].astype(F32) * gain[...]).astype(BF16)
    with scope("barrier"):
        pl.semaphore_wait(bar, len(partners))

    quarter = rows(x * R, R)
    for d in NEAR:
        send(xg.at[0, quarter], xg.at[d, quarter], xa_rs.at[d - 1], dev(dy=d))
    for d in (1, 3):
        send(xg.at[0, 4 * R :], xg.at[d, 4 * R :], xb_rs.at[d - 1], dev(dy=d))
    quarter_z = rows(x * RZ, RZ)
    for d in NEAR:
        send(xg.at[0, quarter_z], xz.at[d - 1, quarter_z], xza_rs, dev(dz=d))
    near_z = {d: send(xg.at[0, 4 * RZ :], xz.at[d - 1, 4 * RZ :], xz_rs.at[d - 1], dev(dz=d)) for d in (1, 3)}
    for h in heads:
        h.wait()

    def send_columns(k):
        for d in NEAR:
            own, to = (mod4(y + d), dev(dy=d)) if k < 2 else (mod4(z + d), dev(dz=d))
            send(wg.at[:, cols(own, k)], wb.at[k, c, d, :, :L], w_rs.at[k, d - 1], to)
            send(wu.at[:, cols(own, k)], wb.at[k, c, d, :, L:], w_rs.at[k, d - 1], to)

    send_columns(0)
    send_columns(2)
    sq = row_sums(tok[...].astype(F32))
    for b in range(4):
        sq_s[b] = sq[:, b * L : (b + 1) * L]
    for d in NEAR:
        send(sq_s, sq_r.at[d - 1], q_rs.at[0], dev(dy=d))
    for d in (1, 3, 2):
        with scope(f"wait_xa#d={d}"):
            arrived(xg.at[d, quarter], xa_rs.at[d - 1])
        for e in NEAR:
            send(xg.at[d, quarter], xg.at[d, quarter], xc_rs, dev(dx=e))
    cut = 4 * R + (H - 4 * R) // 2
    for d, part_of in ((1, slice(4 * R, cut)), (3, slice(cut, H))):
        with scope(f"wait_xb#d={d}"):
            arrived(xg.at[d, 4 * R :], xb_rs.at[d - 1])
        send(xg.at[d, part_of], xg.at[2, part_of], xb_rs.at[1], dev(dy=d))
    send_columns(1)

    def send_rows(d, k0, k1):
        tiles = pl.ds(tile0(mod4(y + d)) + k0, k1 - k0)
        send(wd.at[tiles], wdb.at[y, k0:k1, c], d_rs.at[d - 1], dev(dy=d))

    with scope("wait_xza"):
        arrived(xz.at[:, quarter_z], xza_rs)
        for e in NEAR:
            send(xz.at[:, quarter_z], xz.at[:, quarter_z], xzc_rs, dev(dx=e))
    with scope("wait_xz"):
        for d, half in ((1, slice(4 * RZ, 2 * RZ + H // 2)), (3, slice(2 * RZ + H // 2, H))):
            near_z[d].wait_recv()
            send(xz.at[d - 1, half], xz.at[1, half], xz_rs.at[1], dev(dz=d))
    def columns_of(k):
        with scope(f"wait_w#k={k}"):
            for d in NEAR:
                arrived(wb.at[k, c, d], w_rs.at[k, d - 1])
                send(wb.at[k, c, d], wb.at[k, c, d], f_rs.at[k], dev(dc=1))

    def along(axis, d):
        return (dev(dz=d), mod4(z + d)) if axis == "z" else (dev(dy=d), mod4(y + d))

    def block_of(at, r0=0, r1=B):
        return rows(at * B + r0, r1 - r0)

    def multiply(u):
        k, cc = u // 2, lax.rem(c + u % 2, 2)
        if u % 2:
            with scope(f"wait_f#k={k}"):
                arrived(wb.at[k, cc], f_rs.at[k])
        acc = jnp.zeros((H, 2 * L), F32)
        for d in range(4):
            xs = xz[d - 1] if u >= 4 and d else xg[d]
            acc = acc + jnp.dot(xs, wb[k, cc, d], preferred_element_type=F32)
        part[u] = acc.astype(BF16)

    half = B // 2

    def start(u):
        _, axis, through = JOBS[u]
        if not through:
            for d in NEAR:
                to, at = along(axis, d)
                send(part.at[u, block_of(at)], rdir.at[u, d - 1], sum_rs.at[u], to)
            return
        far = along(axis, 2)[1]
        (up1, above), (dn1, below) = along(axis, 1), along(axis, 3)
        send(part.at[u, block_of(far, 0, half)], zr.at[u, 0], relay_rs.at[u, 0], up1)
        send(part.at[u, block_of(far, half, B)], zr.at[u, 1], relay_rs.at[u, 1], dn1)
        send(part.at[u, block_of(above, half, B)], rbuf.at[u, 0, half:], sum_rs.at[u], up1)
        send(part.at[u, block_of(below, 0, half)], rbuf.at[u, 1, :half], sum_rs.at[u], dn1)

    def add(u):
        _, axis, _ = JOBS[u]
        for side, d, a, b in ((0, 1, 0, half), (1, 3, half, B)):
            to, at = along(axis, d)
            with scope(f"wait_relay#u={u}"):
                arrived(zr.at[u, side], relay_rs.at[u, side])
            zs[u, side] = (part[u, block_of(at, a, b), :].astype(F32) + zr[u, side].astype(F32)).astype(BF16)
            send(zs.at[u, side], rbuf.at[u, side, a:b], sum_rs.at[u], to)

    def core_of(u):
        return lax.rem(c + u % 2, 2)

    def finish(u):
        _, axis, through = JOBS[u]
        came = rbuf if through else rdir
        with scope(f"wait_sum#u={u}"):
            arrived(came.at[u], sum_rs.at[u])
        total = part[u, block_of(along(axis, 0)[1]), :].astype(F32)
        for d in range(2 if through else 3):
            total = total + came[u, d].astype(F32)
        scale = inv if axis == "z" else inv_y
        gate, up = total[:, :L] * scale, total[:, L:] * scale
        hid = gate / (1.0 + jnp.exp(-gate)) * up
        if u < 2:
            hid = jnp.where(y == 3, jnp.zeros_like(hid), hid)
        if axis == "z":
            lanes = pl.ds(pl.multiple_of((u // 2 * 2 + core_of(u)) * L, L), L)
            hall[z, :, lanes] = hid.astype(BF16)
            block = hall.at[z, :, lanes]
        else:
            lanes = pl.ds(pl.multiple_of(core_of(u) * L, L), L)
            hz[z, :, lanes] = hid.astype(BF16)
            block = hz.at[z, :, lanes]
        if u < PASSED:
            send(block, block, shown_rs.at[u, 0], dev(dz=1))
            send(block, block, shown_rs.at[u, 1], dev(dz=3))
            return
        for d in NEAR:
            send(block, block, h_rs.at[u // 4], dev(dz=d))

    def pass_on(u):
        lanes = pl.ds(pl.multiple_of((u // 2 * 2 + core_of(u)) * L, L), L)
        for side, to, dz, a, b in ((0, 1, 3, 0, half), (1, 3, 1, half, B)):
            with scope(f"wait_shown#u={u}"):
                arrived(hall.at[mod4(z + dz), :, lanes], shown_rs.at[u, side])
            block = hall.at[mod4(z + dz), a:b, lanes]
            send(block, block, h_rs.at[0], dev(dz=to))

    for k in range(K):
        arrived(wb.at[k, c, 0], loc.at[k])
        send(wb.at[k, c, 0], wb.at[k, c, 0], f_rs.at[k], dev(dc=1))
    local_d.wait()
    send(wdb.at[y, :, c], wdb.at[y, :, c], df_rs, dev(dc=1))
    columns_of(0)
    with scope("wait_xc"):
        arrived(xg.at[1:, : 3 * R], xc_rs)
    with scope("wait_xb2"):
        arrived(xg.at[2, 4 * R :], xb_rs.at[1])
    multiply(0)
    start(0)
    columns_of(2)
    with scope("wait_sq"):
        arrived(sq_r, q_rs.at[0])
    for b in range(4):
        st2_s[b] = sq_s[b] + sq_r[0, b] + sq_r[1, b] + sq_r[2, b]
    for d in NEAR:
        send(st2_s.at[mod4(z + d)], sq2_r.at[d - 1], q_rs.at[1], dev(dz=d))
        send(st2_s.at[y], sq3_r.at[d - 1], q_rs.at[2], dev(dz=d))
    multiply(1)
    start(1)
    with scope("wait_xz2"):
        arrived(xz.at[1, 4 * RZ :], xz_rs.at[1])
    with scope("wait_xzc"):
        arrived(xz.at[:, : 3 * RZ], xzc_rs)
    multiply(4)
    start(4)
    multiply(5)
    start(5)
    for d in NEAR:
        send_rows(d, 0, K)
    add(0)
    columns_of(1)
    add(1)
    multiply(2)
    start(2)
    multiply(3)
    start(3)
    with scope("wait_sq2"):
        arrived(sq2_r, q_rs.at[1])
        arrived(sq3_r, q_rs.at[2])
    inv = as_columns(lax.rsqrt((st2_s[z] + sq2_r[0] + sq2_r[1] + sq2_r[2]) / D + EPS))
    inv_y = as_columns(lax.rsqrt((st2_s[y] + sq3_r[0] + sq3_r[1] + sq3_r[2]) / D + EPS))
    finish(0)
    finish(1)
    add(2)
    finish(4)
    add(3)
    finish(5)
    finish(2)
    pass_on(0)
    pass_on(1)
    with scope("wait_d2"):
        arrived(wdb.at[0, :, c], d_rs.at[1])
        send(wdb.at[mod4(y - 2), :, c], wdb.at[mod4(y - 2), :, c], df_rs, dev(dc=1))
    finish(3)
    with scope("wait_hz"):
        arrived(hz.at[:3], h_rs.at[1])
    last = slice(4 * L, 6 * L)
    for i, (r0, r1) in enumerate(HALVES):
        for d in NEAR:
            send(hz.at[mod4(y + d), r0:r1], hall.at[y, r0:r1, last], hy_rs.at[i], dev(dy=d))
    hall[y, :, last] = hz[y]
    with scope("wait_d"):
        for d in (1, 3):
            arrived(wdb.at[0, :, c], d_rs.at[d - 1])
            block = wdb.at[mod4(y - d), :, c]
            send(block, block, df_rs, dev(dc=1))
    with scope("wait_df"):
        arrived(wdb.at[:, :, c], df_rs)

    with scope("wait_h"):
        arrived(hall.at[:2, :, : 4 * L], h_rs.at[0])
    for yy in range(4):
        w = wdb[yy, :2].reshape(4 * L, W)
        begun[yy] = jnp.dot(hall[:, :, : 4 * L].reshape(H, 4 * L), w, preferred_element_type=F32).reshape(4, B, W)
    for i, (r0, r1) in enumerate(HALVES):
        with scope(f"wait_hy#i={i}"):
            arrived(hall.at[:3, r0:r1, last], hy_rs.at[i])
        mid = (r0 + r1) // 2
        a, b = slice(r0, mid), slice(mid, r1)
        for dy in (2, 1, 3, 0):
            yy = mod4(y + dy)
            hid = hall[:, r0:r1, 4 * L :].reshape(4 * (r1 - r0), 2 * L)
            acc = jnp.dot(hid, wdb[yy, 2].reshape(2 * L, W), preferred_element_type=F32)
            psend[yy, :, r0:r1] = (begun[yy, :, r0:r1] + acc.reshape(4, r1 - r0, W)).astype(BF16)
            for dx in NEAR:
                send(psend.at[yy, mod4(x + dx), b], p2.at[dx - 1, yy, b], p_rs.at[i, 1], dev(dx=dx))
            if dy:
                send(psend.at[yy, :, a], p1.at[dy - 1, :, a], p_rs.at[i, 0], dev(dy=dy))
    for i, (r0, r1) in enumerate(HALVES):
        mid = (r0 + r1) // 2
        a, b = slice(r0, mid), slice(mid, r1)
        with scope(f"wait_p1#i={i}"):
            arrived(p1.at[:, :, a], p_rs.at[i, 0])
        for xx in range(4):
            v = psend[y, xx, a].astype(F32)
            for d in range(3):
                v = v + p1[d, xx, a].astype(F32)
            s1[xx, a] = v.astype(BF16)
        for d in NEAR:
            send(s1.at[mod4(x + d), a], p3.at[d - 1, a], p_rs.at[i, 2], dev(dx=d))
        with scope(f"wait_p2#i={i}"):
            arrived(p2.at[:, :, b], p_rs.at[i, 1])
        for yy in range(4):
            v = psend[yy, x, b].astype(F32)
            for d in range(3):
                v = v + p2[d, yy, b].astype(F32)
            s2[yy, b] = v.astype(BF16)
        for d in NEAR:
            send(s2.at[mod4(y + d), b], p4.at[d - 1, b], p_rs.at[i, 3], dev(dy=d))
    pieces = []
    for i, (r0, r1) in enumerate(HALVES):
        mid = (r0 + r1) // 2
        a, b = slice(r0, mid), slice(mid, r1)
        with scope(f"wait_p3#i={i}"):
            arrived(p3.at[:, a], p_rs.at[i, 2])
        v1 = s1[x, a].astype(F32)
        for d in range(3):
            v1 = v1 + p3[d, a].astype(F32)
        with scope(f"wait_p4#i={i}"):
            arrived(p4.at[:, b], p_rs.at[i, 3])
        v2 = s2[y, b].astype(F32)
        for d in range(3):
            v2 = v2 + p4[d, b].astype(F32)
        piece = rows(c * H + x * B + r0, r1 - r0)
        pieces.append(0.5 * tok[rows(x * B + r0, r1 - r0), :].astype(F32) + jnp.concatenate([v1, v2], axis=0))
        out[piece, :] = pieces[i].astype(BF16)
        if i == 0:
            for d in NEAR:
                send(out.at[piece, :], out.at[piece, :], o_rs.at[i, d - 1], dev(dx=d))
    stream = jnp.concatenate(pieces, axis=0)
    mine = 2 * x + c
    st_all[mine, 0] = row_sums(stream)
    for dz, f, d, e in EVERYONE:
        send(st_all.at[mine, 0], st_all.at[mine, 4 * dz + f], t_rs, dev(dz=dz, dy=f, dx=d, dc=e))
    for d in NEAR:
        send(out.at[piece, :], out.at[piece, :], o_rs.at[1, d - 1], dev(dx=d))
    for i, (r0, r1) in enumerate(HALVES):
        with scope(f"wait_o#i={i}"):
            for d in (0, 1, 3, 2):
                block = out.at[rows(c * H + mod4(x - d) * B + r0, r1 - r0), :]
                if d:
                    arrived(block, o_rs.at[i, d - 1])
                send(block, block, of_rs, dev(dc=1))
    with scope("wait_of"):
        arrived(out.at[:H], of_rs)
    with scope("wait_st2"):
        arrived(sq_n.at[: len(EVERYONE)], t_rs)
    with scope("wait_sends"):
        for s in sends:
            s.wait_send()
    for xx in range(4):
        for cc in range(2):
            total = jnp.sum(st_all[2 * xx + cc], axis=0)
            factor = as_columns(lax.rsqrt(total / D + EPS))
            r = slice(cc * H + xx * B, cc * H + (xx + 1) * B)
            for h in range(2):
                lanes = slice(h * L, (h + 1) * L)
                out[r, lanes] = (out[r, lanes].astype(F32) * factor * ogain[:, lanes]).astype(BF16)


def body(tokens, norm_gain, gate_weight, up_weight, down_weight, out_gain):
    dma = pltpu.SemaphoreType.DMA
    hbm = pl.BlockSpec(memory_space=pltpu.HBM)
    operands = (
        tokens,
        norm_gain.reshape(1, W),
        gate_weight,
        up_weight,
        down_weight.reshape(11, L, W),
        out_gain.reshape(1, W),
    )
    return pl.pallas_call(
        kernel,
        out_shape=jax.ShapeDtypeStruct((T, W), BF16),
        in_specs=[hbm] * 6,
        out_specs=pl.BlockSpec(memory_space=pltpu.VMEM),
        scratch_shapes=[
            pltpu.VMEM((H, W), BF16),
            pltpu.VMEM((1, W), F32),
            pltpu.VMEM((W, 11 * L), BF16),
            pltpu.VMEM((W, 11 * L), BF16),
            pltpu.VMEM((11, L, W), BF16),
            pltpu.VMEM((1, W), F32),
            pltpu.VMEM((4, H, W), BF16),
            pltpu.VMEM((3, H, W), BF16),
            pltpu.VMEM((K, 2, 4, W, 2 * L), BF16),
            pltpu.VMEM((4, K, 2, L, W), BF16),
            pltpu.VMEM((2 * K, H, 2 * L), BF16),
            pltpu.VMEM((2 * K, 2, B // 2, 2 * L), BF16),
            pltpu.VMEM((2 * K, 2, B // 2, 2 * L), BF16),
            pltpu.VMEM((2 * K, 2, B, 2 * L), BF16),
            pltpu.VMEM((2 * K, 3, B, 2 * L), BF16),
            pltpu.VMEM((4, B, 2 * K * L), BF16),
            pltpu.VMEM((4, B, 2 * L), BF16),
            pltpu.VMEM((4, 4, B, W), F32),
            pltpu.VMEM((4, 4, B, W), BF16),
            pltpu.VMEM((3, 4, B, W), BF16),
            pltpu.VMEM((3, 4, B, W), BF16),
            pltpu.VMEM((4, B, W), BF16),
            pltpu.VMEM((4, B, W), BF16),
            pltpu.VMEM((3, B, W), BF16),
            pltpu.VMEM((3, B, W), BF16),
            pltpu.VMEM((4, 1, L), F32),
            pltpu.VMEM((3, 4, 1, L), F32),
            pltpu.VMEM((3, 1, L), F32),
            pltpu.VMEM((3, 1, L), F32),
            pltpu.VMEM((4, 1, L), F32),
            pltpu.VMEM((8, 16, 1, L), F32),
            pltpu.VMEM((128, 1, L), F32),
            dma,
            dma((2,)),
            dma((K + 1,)),
            dma((3,)), dma((3,)), dma, dma((3,)), dma, dma,
            dma((K, 3)), dma((K,)), dma((3,)), dma,
            dma((4, 2)), dma((len(JOBS),)),
            dma((PASSED, 2)), dma((2,)), dma((2,)),
            dma((2, 4)), dma((3,)), dma,
            dma((2, 3)), dma,
        ],
        compiler_params=pltpu.CompilerParams(
            collective_id=0, has_side_effects=True, vmem_limit_bytes=40 * 1024 * 1024
        ),
    )(*[pltpu.with_memory_space_constraint(a, pltpu.HBM) for a in operands])


def solution(mesh):
    placed = (P(None, "ra"), P("ra"), P("ra", "cb"), P("ra", "cb"), P("cb", "ra"), P("ra"))
    return jax.shard_map(body, mesh=mesh, in_specs=placed, out_specs=P(None, "ra"), check_vma=False)
```
